32 devices in a mesh: rep: 2 (over core), fs: 8 (over z, y), tp: 2 (over x).
Axes of the slice: x: 2, y: 2, z: 4, core: 2. Of those that a mesh axis runs over, the one named last changes fastest.
Arguments:
- tokens: bfloat16 [8192, 2048], P(('rep', 'fs')), may hold values from -6 to 6
- recurrence_branch_weight: bfloat16 [2048, 2048], P('fs', 'tp'), may hold values from -0.125 to 0.125
- gate_branch_weight: bfloat16 [2048, 2048], P('fs', 'tp'), may hold values from -0.125 to 0.125
- convolution_kernel: bfloat16 [4, 2048], P(None, 'tp'), may hold values from -3 to 3
- recurrence_gate_blockwise: bfloat16 [8, 256, 256], P('tp'), may hold values from -0.375 to 0.375
- input_gate_blockwise: bfloat16 [8, 256, 256], P('tp'), may hold values from -0.375 to 0.375
- channel_decay_param: float32 [2048], P('tp')
- token_decay_shift: float32 [8192, 2048], P(('rep', 'fs'), 'tp'), may hold values from -1 to 0
- recurrence_output_weight: bfloat16 [2048, 2048], P('tp', 'fs'), may hold values from -0.5 to 0.5
- first_norm_gain: float32 [2048], replicated, may hold values from 0.1 to 1.9
- feedforward_gate_weight: bfloat16 [2048, 5120], P('fs', 'tp'), may hold values from -0.125 to 0.125
- feedforward_up_weight: bfloat16 [2048, 5120], P('fs', 'tp'), may hold values from -0.125 to 0.125
- feedforward_down_weight: bfloat16 [5120, 2048], P('tp', 'fs'), may hold values from -0.15625 to 0.15625
- second_norm_gain: float32 [2048], replicated, may hold values from 0.1 to 1.9
Outputs:
- layer_out: bfloat16 [8192, 2048], P(('rep', 'fs', 'tp'))
The draws below stay inside these ranges and needn't reach their ends.
All inputs are finite; a program needn't handle non-finite values.
Results may differ from the reference program's by a relative error of at most 0.02.
Values may be sent and summed in bfloat16 or wider, within the bound.
A program may use at most 128 MiB of HBM per device.

```python
import math
import jax
import jax.numpy as jnp
from jax import lax

MODEL_WIDTH = 2048
FF = 5120
LRU_BLOCKS = 8
BLOCK = 256
CONV = 4
SEQUENCE_TOKENS = 512
RECURRENT_WIDTH = 2048
ROWS_ALL = 8192
N_TP = 2


def draw_channel_decay_param(key, part):
    key_flag = jax.random.fold_in(key, 11)
    key_slow = jax.random.fold_in(key, 12)
    key_fast = jax.random.fold_in(key, 13)
    quick = jax.random.randint(key_flag, (RECURRENT_WIDTH,), 0, 2) == 1
    slow_value = math.log(4.0 * SEQUENCE_TOKENS) + jax.random.uniform(key_slow, (RECURRENT_WIDTH,), jnp.float32, 0.0, 1.5)
    fast_value = math.log(4.0 * min(50.0, SEQUENCE_TOKENS / 4.0)) + jax.random.uniform(key_fast, (RECURRENT_WIDTH,), jnp.float32, -0.5, 0.5)
    return jnp.where(quick, fast_value, slow_value).astype(jnp.float32)


def draw_token_decay_shift(key, part):
    key_where = jax.random.fold_in(key, 21)
    key_depth = jax.random.fold_in(key, 22)
    struck = jax.random.randint(key_where, (ROWS_ALL, 1), 0, SEQUENCE_TOKENS) < 3
    depth = jax.random.uniform(key_depth, (ROWS_ALL, RECURRENT_WIDTH), jnp.float32, 0.22, 0.69)
    return jnp.where(struck, -depth, 0.0).astype(jnp.float32)


def block_levels(key, extent, cuts, low, top_value):
    level = 1.0
    for axis_at, parts in cuts:
        heights = jax.random.uniform(jax.random.fold_in(jax.random.fold_in(key, 6), axis_at), (parts,), jnp.float32, low / len(cuts), top_value / len(cuts))
        level = level * jnp.repeat(jnp.exp(heights), extent[axis_at] // parts).reshape((-1,) + (1,) * (len(extent) - 1 - axis_at))
    return level


def scatter_about(rng, shape, spread, bound, pieces=(), held_as=jnp.bfloat16):
    array = jax.random.normal(rng, shape, jnp.float32) * spread
    if len(pieces) > 0:
        array = block_levels(rng, shape, pieces, -0.22, 0.18) * array
    return jnp.clip(array, min=-bound, max=bound).astype(held_as)


def setup_inputs(seed: int = 0) -> dict:
    arg_keys = jax.random.split(jax.random.key(seed), 15)
    return {
        "tokens": scatter_about(arg_keys[0], (ROWS_ALL, MODEL_WIDTH), 1.0, 6.0, ((0, 16),)),
        "recurrence_branch_weight": scatter_about(arg_keys[1], (MODEL_WIDTH, RECURRENT_WIDTH), MODEL_WIDTH ** -0.5, 0.125, ((0, 8), (1, 2))),
        "gate_branch_weight": scatter_about(arg_keys[2], (MODEL_WIDTH, RECURRENT_WIDTH), MODEL_WIDTH ** -0.5, 0.125, ((0, 8), (1, 2))),
        "convolution_kernel": scatter_about(arg_keys[3], (CONV, RECURRENT_WIDTH), 0.5, 3.0, ((1, 2),)),
        "recurrence_gate_blockwise": scatter_about(arg_keys[4], (LRU_BLOCKS, BLOCK, BLOCK), BLOCK ** -0.5, 0.375, ((0, 2),)),
        "input_gate_blockwise": scatter_about(arg_keys[5], (LRU_BLOCKS, BLOCK, BLOCK), BLOCK ** -0.5, 0.375, ((0, 2),)),
        "channel_decay_param": draw_channel_decay_param(jax.random.fold_in(arg_keys[14], 71), 0),
        "token_decay_shift": draw_token_decay_shift(jax.random.fold_in(arg_keys[14], 71), 0),
        "recurrence_output_weight": scatter_about(arg_keys[8], (RECURRENT_WIDTH, MODEL_WIDTH), (RECURRENT_WIDTH // 16) ** -0.5, 0.5, ((0, 2), (1, 8))),
        "first_norm_gain": jnp.clip(1.0 + 0.18 * jax.random.normal(arg_keys[9], (MODEL_WIDTH,), jnp.float32), 0.1, 1.9),
        "feedforward_gate_weight": scatter_about(arg_keys[10], (MODEL_WIDTH, FF), MODEL_WIDTH ** -0.5, 0.125, ((0, 8), (1, 2))),
        "feedforward_up_weight": scatter_about(arg_keys[11], (MODEL_WIDTH, FF), MODEL_WIDTH ** -0.5, 0.125, ((0, 8), (1, 2))),
        "feedforward_down_weight": scatter_about(arg_keys[12], (FF, MODEL_WIDTH), (FF // 4) ** -0.5, 0.15625, ((0, 2), (1, 8))),
        "second_norm_gain": jnp.clip(1.0 + 0.18 * jax.random.normal(arg_keys[13], (MODEL_WIDTH,), jnp.float32), 0.1, 1.9),
    }


residual_scale = 1.4142135623730951

def layer_norm(values, gain):
    center = values - lax.optimization_barrier(jnp.mean(values, axis=-1, keepdims=True))
    variance = lax.optimization_barrier(jnp.mean(center * center, axis=-1, keepdims=True))
    return center * lax.rsqrt(variance + 1e-05) * gain

def grouped_product(left, right):
    width = left.shape[1] // N_TP
    total = jnp.zeros((left.shape[0], right.shape[1]), jnp.float32)
    for group in range(N_TP):
        term = jnp.dot(left[:, group * width:(group + 1) * width], right[group * width:(group + 1) * width], preferred_element_type=jnp.float32)
        term = lax.optimization_barrier(term.astype(jnp.bfloat16))
        total = total + term.astype(jnp.float32)
    return total

def combine(earlier, later):
    return (earlier[0] * later[0], later[0] * earlier[1] + later[1])

def single_sequence_layer(tokens, decay_added, recurrence_branch_weight, gate_branch_weight, convolution_kernel, recurrence_gate_blockwise, input_gate_blockwise, channel_decay_param, recurrence_output_weight, first_norm_gain, feedforward_gate_weight, feedforward_up_weight, feedforward_down_weight, second_norm_gain):
    length = tokens.shape[0]
    value_in = jnp.dot(tokens, recurrence_branch_weight, preferred_element_type=jnp.float32).astype(jnp.bfloat16)
    gate_in = jnp.dot(tokens, gate_branch_weight, preferred_element_type=jnp.float32).astype(jnp.bfloat16)
    padded = jnp.concatenate([jnp.zeros((CONV - 1, RECURRENT_WIDTH), jnp.float32), value_in.astype(jnp.float32)], axis=0)
    conv = jnp.zeros((length, RECURRENT_WIDTH), jnp.float32)
    for tap in range(CONV):
        conv = conv + padded[tap:tap + length] * convolution_kernel[tap].astype(jnp.float32)
    conv = conv.astype(jnp.bfloat16)
    blocked = conv.astype(jnp.float32).reshape(length, LRU_BLOCKS, BLOCK)
    recurrence_gate_value = jax.nn.sigmoid(jnp.einsum('rnk,nkj->rnj', blocked, recurrence_gate_blockwise.astype(jnp.float32)).reshape(length, RECURRENT_WIDTH))
    inlet = jax.nn.sigmoid(jnp.einsum('rnk,nkj->rnj', blocked, input_gate_blockwise.astype(jnp.float32)).reshape(length, RECURRENT_WIDTH))
    log_decay_factor = -8.0 * recurrence_gate_value * jax.nn.softplus(-channel_decay_param) + decay_added
    decay = jnp.exp(log_decay_factor)
    drive = jnp.sqrt(-jnp.expm1(2.0 * log_decay_factor)) * inlet * conv.astype(jnp.float32)
    _, state = lax.associative_scan(combine, (decay, drive), axis=0)
    branch = (state * jax.nn.gelu(gate_in.astype(jnp.float32))).astype(jnp.bfloat16)
    mix = grouped_product(branch, recurrence_output_weight)
    normed = layer_norm(residual_scale * tokens.astype(jnp.float32) + mix, first_norm_gain).astype(jnp.bfloat16)
    gate = jnp.dot(normed, feedforward_gate_weight, preferred_element_type=jnp.float32)
    upward = jnp.dot(normed, feedforward_up_weight, preferred_element_type=jnp.float32)
    hidden = (jax.nn.silu(gate) * upward).astype(jnp.bfloat16)
    ffn = grouped_product(hidden, feedforward_down_weight)
    return layer_norm(residual_scale * normed.astype(jnp.float32) + ffn, second_norm_gain).astype(jnp.bfloat16)

def reference(tokens, recurrence_branch_weight, gate_branch_weight, convolution_kernel, recurrence_gate_blockwise, input_gate_blockwise, channel_decay_param, token_decay_shift, recurrence_output_weight, first_norm_gain, feedforward_gate_weight, feedforward_up_weight, feedforward_down_weight, second_norm_gain):
    token_count = tokens.shape[0] // SEQUENCE_TOKENS

    def apply_layer(pair):
        return single_sequence_layer(pair[0], pair[1], recurrence_branch_weight, gate_branch_weight, convolution_kernel, recurrence_gate_blockwise, input_gate_blockwise, channel_decay_param, recurrence_output_weight, first_norm_gain, feedforward_gate_weight, feedforward_up_weight, feedforward_down_weight, second_norm_gain)
    layer_result = lax.map(apply_layer, (tokens.reshape(token_count, SEQUENCE_TOKENS, MODEL_WIDTH), token_decay_shift.reshape(token_count, SEQUENCE_TOKENS, RECURRENT_WIDTH)))
    return layer_result.reshape(token_count * SEQUENCE_TOKENS, MODEL_WIDTH)
```

```python
import functools

import jax
import jax.numpy as jnp
from jax import lax
from jax.experimental import pallas as pl
from jax.experimental.pallas import tpu as pltpu
from jax.sharding import PartitionSpec as P

residual_scale = 1.4142135623730951

VMEM_BYTES = 60 * 1024 * 1024
LAYER_VMEM_BYTES = 67043328
MESH = pl.DeviceIdType.MESH


def layer_norm(values, gain):
    center = values - jnp.mean(values, axis=-1, keepdims=True)
    variance = jnp.mean(center * center, axis=-1, keepdims=True)
    return center * lax.rsqrt(variance + 1e-05) * gain


def scalars(owners, swapped):
    return jnp.stack([jnp.asarray(v, jnp.int32) for v in [swapped, *owners]])


def split_product(meta, left_ref, part_refs):
    total = None
    for at, part in enumerate(part_refs):
        depth = part.shape[0]
        columns = pl.ds(pl.multiple_of(meta[1 + at] * depth, depth), depth)
        term = jnp.dot(left_ref[:, columns], part[...], preferred_element_type=jnp.float32)
        total = term if total is None else total + term
    return total


def shifted(values, step, fill):
    rows = lax.broadcasted_iota(jnp.int32, values.shape, 0)
    return jnp.where(rows < step, fill, pltpu.roll(values, step, 0))


def sigmoid(values):
    return 1.0 / (1.0 + jnp.exp(-values))


def recur_core(value_in, gate_in, taps, rate_block, inlet_block, plus, shift):
    value_in = value_in.astype(jnp.bfloat16).astype(jnp.float32)
    gate_in = gate_in.astype(jnp.bfloat16).astype(jnp.float32)
    taps = taps.astype(jnp.float32)
    depth = taps.shape[0]
    conv = None
    for tap in range(depth):
        lag = depth - 1 - tap
        moved = value_in if lag == 0 else shifted(value_in, lag, 0.0)
        term = moved * taps[tap : tap + 1, :]
        conv = term if conv is None else conv + term
    conv = conv.astype(jnp.bfloat16)
    rate = sigmoid(jnp.dot(conv, rate_block, preferred_element_type=jnp.float32))
    inlet = sigmoid(jnp.dot(conv, inlet_block, preferred_element_type=jnp.float32))
    log_decay = -8.0 * rate * plus + shift
    decay = jnp.exp(log_decay)
    twice = 2.0 * log_decay
    series = jnp.ones_like(twice)
    for order in range(8, 1, -1):
        series = 1.0 + twice * series * (1.0 / order)
    lost = jnp.where(twice > -0.3, -twice * series, 1.0 - jnp.exp(twice))
    state = jnp.sqrt(lost) * inlet * conv.astype(jnp.float32)
    step = 1
    while step < state.shape[0]:
        state = state + decay * shifted(state, step, 0.0)
        if 2 * step < state.shape[0]:
            decay = decay * shifted(decay, step, 1.0)
        step *= 2
    gelu = 0.5 * gate_in * (
        1.0 + jnp.tanh(0.7978845608028654 * (gate_in + 0.044715 * gate_in * gate_in * gate_in))
    )
    return (state * gelu).astype(jnp.bfloat16)


LINE, OTHER, SIDE, CORE = 0, 1, 2, 3


def layer_kernel(
    tok_hbm,
    in_hbm,
    gate_hbm,
    taps_ref,
    rate_ref,
    inlet_ref,
    plus_ref,
    shift_hbm,
    out_hbm,
    first_gain_ref,
    ffgate_hbm,
    ffup_hbm,
    down_hbm,
    second_gain_ref,
    out_ref,
    buf_a,
    buf_b,
    buf_c,
    buf_d,
    tok,
    shift,
    branch,
    terms,
    came,
    normed,
    hidden,
    load_sem,
    send_sem,
    recv_sem,
    terms_send,
    terms_recv,
    norm_send,
    norm_recv,
):
    core, fs, tp = lax.axis_index("rep"), lax.axis_index("fs"), lax.axis_index("tp")
    z, y = fs // 2, fs % 2
    zs = [z, z + 1 - 2 * (z % 2), 2 - z // 2, 3 - 3 * (z // 2)]
    middle = z * (3 - z) == 2
    first_core, second_core = core == 0, core == 1
    second_middle = jnp.logical_and(second_core, middle)
    first_or_end = jnp.logical_or(first_core, jnp.logical_not(middle))
    far = 3 - z
    own_at = [k * 2 + y for k in zs]
    side_at = [k * 2 + 1 - y for k in zs]
    me = own_at[0]
    targets = {
        LINE: (core, own_at[1], tp),
        OTHER: (core, far * 2 + y, tp),
        SIDE: (core, side_at[0], tp),
        CORE: (1 - core, me, tp),
    }
    across = (core, me, 1 - tp)
    width = in_hbm.shape[0]
    ff_half = buf_c.shape[3]
    columns = buf_b.shape[2]
    mix_depth, down_depth = buf_b.shape[1], buf_d.shape[1]
    share = out_ref.shape[0]
    tile = min(256, ff_half)
    own_row = pl.multiple_of(tp * share, share)
    sent = []

    def piece(pack, at, half):
        if pack == 0:
            return buf_a.at[half, pl.ds(pl.multiple_of(at * width, width), width), :]
        if pack == 1:
            rows = mix_depth // 2
            return buf_b.at[at, pl.ds(pl.multiple_of(half * rows, rows), rows), :]
        if pack < 4:
            return buf_c.at[pack - 2, half, pl.ds(pl.multiple_of(at * width, width), width), :]
        rows = down_depth // 4
        return buf_d.at[at, pl.ds(pl.multiple_of((half * 2 + pack - 4) * rows, rows), rows), :]

    def copy(pack, at, way, half=core):
        return pltpu.make_async_remote_copy(
            src_ref=piece(pack, at, half),
            dst_ref=piece(pack, at, half),
            send_sem=send_sem.at[pack, at, way],
            recv_sem=recv_sem.at[pack, half, at],
            device_id=targets[way],
            device_id_type=MESH,
        )

    def under(condition, action):
        if condition is None:
            action()
        else:
            pl.when(condition)(action)

    def send(pack, at, way, condition=None):
        sent.append((pack, at, way, condition))
        under(condition, lambda: copy(pack, at, way).start())

    def arrived(pack, at):
        copy(pack, at, CORE).wait_recv()

    def handed(pack, at):
        copy(pack, at, CORE, 1 - core).wait_recv()

    def send_own(pack):
        send(pack, me, LINE)
        send(pack, me, OTHER, middle)
        send(pack, me, SIDE)

    def from_side(pack):
        at = side_at[0]
        arrived(pack, at)
        send(pack, at, LINE, second_core)
        send(pack, at, OTHER, second_middle)
        send(pack, at, CORE)

    def from_line(pack, k):
        at = own_at[k]
        arrived(pack, at)
        send(pack, at, OTHER if k == 1 else LINE, middle)
        if k == 3:
            send(pack, at, SIDE)
        elif k == 2:
            send(pack, at, SIDE, first_or_end)
        else:
            send(pack, at, SIDE, first_core)
        send(pack, at, CORE)

    def from_far_side(pack, k):
        at = side_at[k]
        arrived(pack, at)
        send(pack, at, CORE)

    def events(pack):
        return [
            lambda: from_side(pack),
            lambda: from_line(pack, 1),
            lambda: from_line(pack, 2),
            lambda: from_far_side(pack, 1),
            lambda: from_line(pack, 3),
            lambda: from_far_side(pack, 2),
            lambda: from_far_side(pack, 3),
        ]

    order = [me, side_at[0], own_at[1], own_at[2], side_at[1], own_at[3], side_at[2], side_at[3]]

    def all_handed(pack):
        for at in order[1:]:
            handed(pack, at)

    def run(actions):
        for action in actions:
            action()

    def at_step(step, plan):
        for when, actions in enumerate(plan):
            if actions:
                pl.when(step == when)(functools.partial(run, actions))

    c_cols = lambda half: pl.ds(half * ff_half, ff_half)
    loads = {
        "a0": (in_hbm, piece(0, me, 0)),
        "a1": (gate_hbm, piece(0, me, 1)),
        "b": (out_hbm, buf_b.at[me]),
        "tok": (tok_hbm, tok),
        "c0": (ffgate_hbm.at[:, c_cols(0)], piece(2, me, 0)),
        "c1": (ffup_hbm.at[:, c_cols(0)], piece(2, me, 1)),
        "c2": (ffgate_hbm.at[:, c_cols(1)], piece(3, me, 0)),
        "c3": (ffup_hbm.at[:, c_cols(1)], piece(3, me, 1)),
        "d": (down_hbm, buf_d.at[me]),
        "shift": (shift_hbm, shift),
    }
    loads = {
        name: pltpu.make_async_copy(source, target, load_sem.at[at])
        for at, (name, (source, target)) in enumerate(loads.items())
    }
    for load in loads.values():
        load.start()

    barrier = pltpu.get_barrier_semaphore()
    for target in [targets[LINE], targets[SIDE], targets[CORE], across]:
        pl.semaphore_signal(barrier, inc=1, device_id=target, device_id_type=MESH)

    @pl.when(middle)
    def _():
        pl.semaphore_signal(barrier, inc=1, device_id=targets[OTHER], device_id_type=MESH)

    pl.semaphore_wait(barrier, 4 + z * (3 - z) // 2)

    loads["a0"].wait()
    loads["a1"].wait()
    send_own(0)
    loads["b"].wait()
    send_own(1)
    run(events(0)[:5])
    for name in ("c0", "c1"):
        loads[name].wait()
    send_own(2)
    run(events(0)[5:])
    all_handed(0)
    loads["tok"].wait()
    loads["shift"].wait()

    block = rate_ref.shape[1]

    def recur_step(i, plan):
        cols = pl.ds(pl.multiple_of(i * block, block), block)
        value_in = jnp.dot(tok[...], buf_a[0, :, cols], preferred_element_type=jnp.float32)
        gate_in = jnp.dot(tok[...], buf_a[1, :, cols], preferred_element_type=jnp.float32)
        branch[:, cols] = recur_core(
            value_in, gate_in, taps_ref[:, cols], rate_ref[i], inlet_ref[i], plus_ref[:, cols], shift[:, cols]
        )
        at_step(i, plan)

    ev = events(1)
    plan = [ev[:2], ev[2:4], ev[4:5], ev[5:]]
    lax.fori_loop(0, rate_ref.shape[0], lambda i, _: recur_step(i, plan), None)
    for name in ("c2", "c3"):
        loads[name].wait()
    send_own(3)
    all_handed(1)

    def terms_copy(phase, at):
        return pltpu.make_async_remote_copy(
            src_ref=terms.at[1 - tp, at],
            dst_ref=came.at[phase, at],
            send_sem=terms_send.at[phase, at],
            recv_sem=terms_recv.at[phase, at],
            device_id=across,
            device_id_type=MESH,
        )

    def keep(product, at):
        product = product.astype(jnp.bfloat16)
        for row in range(2):
            terms[row, at] = product[row * share : (row + 1) * share]

    parts = buf_b.shape[0]

    def mix_step(s, _):
        keep(jnp.dot(branch[...], buf_b[s], preferred_element_type=jnp.float32), s)
        pl.when(s > 0)(lambda: terms_copy(0, s - 1).start())

    lax.fori_loop(0, parts, mix_step, None)
    ev = events(2)
    run(ev[:1])
    terms_copy(0, parts - 1).start()
    run(ev[1:2])
    for s in range(parts):
        terms_copy(0, s).wait_recv()

    rows = 64

    def norm_rows(i, phase, residual, gain_ref):
        piece_rows = pl.ds(pl.multiple_of(i * rows, rows), rows)
        value = jnp.concatenate(
            [
                terms[tp, s, piece_rows, :].astype(jnp.float32) + came[phase, s, piece_rows, :].astype(jnp.float32)
                for s in range(parts)
            ],
            axis=1,
        )
        return layer_norm(residual_scale * residual.astype(jnp.float32) + value, gain_ref[...]).astype(jnp.bfloat16)

    def own_rows(i):
        return pl.ds(pl.multiple_of(own_row + i * rows, rows), rows)

    def norm_copy(i):
        return pltpu.make_async_remote_copy(
            src_ref=normed.at[own_rows(i), :],
            dst_ref=normed.at[own_rows(i), :],
            send_sem=norm_send.at[i],
            recv_sem=norm_recv.at[i],
            device_id=across,
            device_id_type=MESH,
        )

    def first_norm(i, _):
        normed[own_rows(i), :] = norm_rows(i, 0, tok[own_rows(i), :], first_gain_ref)
        pl.when(i > 0)(lambda: norm_copy(i - 1).start())

    tiles = share // rows
    lax.fori_loop(0, tiles, first_norm, None)
    run(ev[2:3])
    norm_copy(tiles - 1).start()
    run(ev[3:5])
    loads["d"].wait()
    send_own(4)
    run(ev[5:])
    for i in range(tiles):
        norm_copy(i).wait_recv()
    all_handed(2)

    def hidden_step(j, half, plan):
        cols = pl.ds(pl.multiple_of(j * tile, tile), tile)
        gate = jnp.dot(normed[...], buf_c[half, 0, :, cols], preferred_element_type=jnp.float32)
        upward = jnp.dot(normed[...], buf_c[half, 1, :, cols], preferred_element_type=jnp.float32)
        to = pl.ds(pl.multiple_of(half * ff_half + j * tile, tile), tile)
        hidden[:, to] = (gate * sigmoid(gate) * upward).astype(jnp.bfloat16)
        at_step(j, plan)

    steps = ff_half // tile
    ev = events(3)
    plan = [ev[:2], ev[2:3], ev[3:4], ev[4:5], []]
    lax.fori_loop(0, steps, lambda j, _: hidden_step(j, 0, plan), None)
    send_own(5)
    run(ev[5:])
    all_handed(3)
    ev = events(4)
    plan = [ev[:2], ev[2:3], ev[3:5], ev[5:6], []]
    lax.fori_loop(0, steps, lambda j, _: hidden_step(j, 1, plan), None)
    run(ev[6:])

    for s in range(parts):
        terms_copy(0, s).wait_send()

    ev = events(5)

    def pick(j):
        at = order[0]
        for turn in range(1, parts):
            at = jnp.where(j == turn, order[turn], at)
        return at

    def down_step(j, _):
        at_step(j, [[]] + [[e] for e in ev])
        at = pick(j)
        @pl.when(j > 0)
        def _():
            handed(4, at)
            handed(5, at)
        keep(jnp.dot(hidden[...], buf_d[at], preferred_element_type=jnp.float32), at)
        pl.when(j > 0)(lambda: terms_copy(1, pick(j - 1)).start())

    lax.fori_loop(0, parts, down_step, None)
    for pack, at, way, condition in sent:
        under(condition, lambda: copy(pack, at, way).wait_send())
    terms_copy(1, order[-1]).start()
    for s in order:
        terms_copy(1, s).wait_recv()

    def second_norm(i, _):
        here = pl.ds(pl.multiple_of(i * rows, rows), rows)
        out_ref[here, :] = norm_rows(i, 1, normed[own_rows(i), :], second_gain_ref)

    lax.fori_loop(0, tiles, second_norm, None)
    for i in range(tiles):
        norm_copy(i).wait_send()
    for s in range(parts):
        terms_copy(1, s).wait_send()


def whole_layer(
    tokens,
    recurrence_branch_weight,
    gate_branch_weight,
    convolution_kernel,
    recurrence_gate_blockwise,
    input_gate_blockwise,
    channel_decay_param,
    token_decay_shift,
    recurrence_output_weight,
    first_norm_gain,
    feedforward_gate_weight,
    feedforward_up_weight,
    feedforward_down_weight,
    second_norm_gain,
):
    length, model = tokens.shape
    parts = lax.axis_size("fs")
    share = length // lax.axis_size("tp")
    depth, channels = recurrence_branch_weight.shape
    units = feedforward_gate_weight.shape[1]
    columns = recurrence_output_weight.shape[1]
    hbm = pl.BlockSpec(memory_space=pl.ANY)
    vmem = pl.BlockSpec(memory_space=pltpu.VMEM)
    half = jnp.bfloat16
    return pl.pallas_call(
        layer_kernel,
        in_specs=[hbm, hbm, hbm, vmem, vmem, vmem, vmem, hbm, hbm, vmem, hbm, hbm, hbm, vmem],
        out_specs=vmem,
        out_shape=jax.ShapeDtypeStruct((share, model), half),
        scratch_shapes=[
            pltpu.VMEM((2, depth * parts, channels), half),
            pltpu.VMEM((parts, channels, columns), half),
            pltpu.VMEM((2, 2, depth * parts, units // 2), half),
            pltpu.VMEM((parts, units, columns), half),
            pltpu.VMEM((length, model), half),
            pltpu.VMEM((length, channels), jnp.float32),
            pltpu.VMEM((length, channels), half),
            pltpu.VMEM((2, parts, share, columns), half),
            pltpu.VMEM((2, parts, share, columns), half),
            pltpu.VMEM((length, model), half),
            pltpu.VMEM((length, units), half),
            pltpu.SemaphoreType.DMA((10,)),
            pltpu.SemaphoreType.DMA((6, parts, 4)),
            pltpu.SemaphoreType.DMA((6, 2, parts)),
            pltpu.SemaphoreType.DMA((2, parts)),
            pltpu.SemaphoreType.DMA((2, parts)),
            pltpu.SemaphoreType.DMA((share // 64,)),
            pltpu.SemaphoreType.DMA((share // 64,)),
        ],
        cost_estimate=pl.CostEstimate(
            flops=2 * length * model * (2 * channels + 2 * units) + 2 * length * model * (channels + units),
            bytes_accessed=2 * model * (3 * channels + 3 * units),
            transcendentals=0,
        ),
        compiler_params=pltpu.CompilerParams(
            vmem_limit_bytes=LAYER_VMEM_BYTES, collective_id=0, has_side_effects=True
        ),
    )(
        tokens,
        recurrence_branch_weight,
        gate_branch_weight,
        convolution_kernel,
        recurrence_gate_blockwise,
        input_gate_blockwise,
        jax.nn.softplus(-channel_decay_param)[None, :],
        token_decay_shift,
        recurrence_output_weight,
        first_norm_gain[None, :],
        feedforward_gate_weight,
        feedforward_up_weight,
        feedforward_down_weight,
        second_norm_gain[None, :],
    )


def recurrence_kernel(count, meta, x_ref, taps_ref, rate_ref, inlet_ref, plus_ref, shift_ref, *refs):
    mine, other, out_ref = refs[:count], refs[count : 2 * count], refs[-1]
    first = split_product(meta, x_ref, mine)
    second = split_product(meta, x_ref, other)
    out_ref[...] = recur_core(
        first, second, taps_ref[...], rate_ref[0], inlet_ref[0], plus_ref[...], shift_ref[...]
    )


def recurrence(tokens, mine, other, meta, taps, rate_blocks, inlet_blocks, plus, shift):
    length, width = tokens.shape
    block = rate_blocks.shape[1]
    blocks = rate_blocks.shape[0]
    parts = [pl.BlockSpec((p.shape[0], block), lambda i: (0, i)) for p in [*mine, *other]]
    column = lambda rows: pl.BlockSpec((rows, block), lambda i: (0, i))
    square = pl.BlockSpec((1, block, block), lambda i: (i, 0, 0))
    return pl.pallas_call(
        functools.partial(recurrence_kernel, len(mine)),
        grid=(blocks,),
        in_specs=[
            pl.BlockSpec(memory_space=pltpu.SMEM),
            pl.BlockSpec((length, width), lambda i: (0, 0)),
            column(taps.shape[0]),
            square,
            square,
            column(1),
            column(length),
            *parts,
        ],
        out_specs=column(length),
        out_shape=jax.ShapeDtypeStruct((length, block * blocks), jnp.bfloat16),
        cost_estimate=pl.CostEstimate(
            flops=4 * length * width * block * blocks,
            bytes_accessed=4 * width * block * blocks + 8 * length * block * blocks,
            transcendentals=0,
        ),
        compiler_params=pltpu.CompilerParams(vmem_limit_bytes=VMEM_BYTES),
    )(meta, tokens, taps, rate_blocks, inlet_blocks, plus, shift, *mine, *other)


def hidden_kernel(count, meta, x_ref, *refs):
    mine, other, out_ref = refs[:count], refs[count : 2 * count], refs[-1]
    first = split_product(meta, x_ref, mine)
    second = split_product(meta, x_ref, other)
    swapped = meta[0] == 1
    gate = jnp.where(swapped, second, first)
    upward = jnp.where(swapped, first, second)
    out_ref[...] = (gate * sigmoid(gate) * upward).astype(jnp.bfloat16)


def hidden_units(normed, mine, other, meta):
    length, width = normed.shape
    units = mine[0].shape[1]
    tile = next(t for t in (512, 640, 256, 128, units) if units % t == 0)
    return pl.pallas_call(
        functools.partial(hidden_kernel, len(mine)),
        grid=(units // tile,),
        in_specs=[
            pl.BlockSpec(memory_space=pltpu.SMEM),
            pl.BlockSpec((length, width), lambda i: (0, 0)),
            *[pl.BlockSpec((p.shape[0], tile), lambda i: (0, i)) for p in [*mine, *other]],
        ],
        out_specs=pl.BlockSpec((length, tile), lambda i: (0, i)),
        out_shape=jax.ShapeDtypeStruct((length, units), jnp.bfloat16),
        cost_estimate=pl.CostEstimate(
            flops=4 * length * width * units, bytes_accessed=4 * width * units, transcendentals=0
        ),
        compiler_params=pltpu.CompilerParams(vmem_limit_bytes=VMEM_BYTES),
    )(meta, normed, *mine, *other)


def outward_kernel(count, meta, left_ref, *refs):
    mine, other, out_ref = refs[:count], refs[count : 2 * count], refs[-1]
    half = mine[0].shape[0]
    near = pl.ds(pl.multiple_of(meta[0] * half, 128), half)
    far = pl.ds(pl.multiple_of((1 - meta[0]) * half, 128), half)
    start = 0
    for at in range(count):
        total = jnp.dot(left_ref[:, near], mine[at][...], preferred_element_type=jnp.float32)
        total += jnp.dot(left_ref[:, far], other[at][...], preferred_element_type=jnp.float32)
        columns = mine[at].shape[1]
        out_ref[:, start : start + columns] = total.astype(jnp.bfloat16)
        start += columns


def outward(left, mine, other, meta):
    length, depth = left.shape
    width = sum(p.shape[1] for p in mine)
    rows = min(length, 256)
    whole = [pl.BlockSpec(p.shape, lambda i: (0, 0)) for p in [*mine, *other]]
    return pl.pallas_call(
        functools.partial(outward_kernel, len(mine)),
        grid=(length // rows,),
        in_specs=[
            pl.BlockSpec(memory_space=pltpu.SMEM),
            pl.BlockSpec((rows, depth), lambda i: (i, 0)),
            *whole,
        ],
        out_specs=pl.BlockSpec((rows, width), lambda i: (i, 0)),
        out_shape=jax.ShapeDtypeStruct((length, width), jnp.bfloat16),
        cost_estimate=pl.CostEstimate(
            flops=2 * length * width * depth, bytes_accessed=2 * width * depth, transcendentals=0
        ),
        compiler_params=pltpu.CompilerParams(vmem_limit_bytes=VMEM_BYTES),
    )(meta, left, *mine, *other)


def gathered_layer(
    tokens,
    recurrence_branch_weight,
    gate_branch_weight,
    convolution_kernel,
    recurrence_gate_blockwise,
    input_gate_blockwise,
    channel_decay_param,
    token_decay_shift,
    recurrence_output_weight,
    first_norm_gain,
    feedforward_gate_weight,
    feedforward_up_weight,
    feedforward_down_weight,
    second_norm_gain,
):
    share = tokens.shape[0] // lax.axis_size("tp")
    offset = lax.axis_index("tp") * share
    rows_of = lambda weight: [lax.all_gather(weight, "fs", axis=0, tiled=True)]

    def halves_of(weight):
        half = weight.shape[0] // 2
        return [[lax.all_gather(part, "fs", axis=1, tiled=True)] for part in (weight[:half], weight[half:])]

    meta = scalars([jnp.int32(0)], jnp.int32(0))
    branch = recurrence(
        tokens,
        rows_of(recurrence_branch_weight),
        rows_of(gate_branch_weight),
        meta,
        convolution_kernel,
        recurrence_gate_blockwise,
        input_gate_blockwise,
        jax.nn.softplus(-channel_decay_param)[None, :],
        token_decay_shift,
    )

    def grouped(left, weight):
        terms = outward(left, *halves_of(weight), meta)
        return lax.psum_scatter(terms, "tp", scatter_dimension=0, tiled=True).astype(jnp.float32)

    mix = grouped(branch, recurrence_output_weight)
    own_tokens = lax.dynamic_slice_in_dim(tokens, offset, share, 0)
    normed = layer_norm(
        residual_scale * own_tokens.astype(jnp.float32) + mix, first_norm_gain
    ).astype(jnp.bfloat16)
    rows = lax.all_gather(normed, "tp", axis=0, tiled=True)
    hidden = hidden_units(rows, rows_of(feedforward_gate_weight), rows_of(feedforward_up_weight), meta)
    ffn = grouped(hidden, feedforward_down_weight)
    return layer_norm(residual_scale * normed.astype(jnp.float32) + ffn, second_norm_gain).astype(
        jnp.bfloat16
    )


def solution(mesh):
    sizes = mesh.shape
    one_kernel = sizes["rep"] == 2 and sizes["tp"] == 2 and sizes["fs"] == 8
    return jax.shard_map(
        whole_layer if one_kernel else gathered_layer,
        mesh=mesh,
        in_specs=(
            P(("rep", "fs"), None),
            P("fs", "tp"),
            P("fs", "tp"),
            P(None, "tp"),
            P("tp", None, None),
            P("tp", None, None),
            P("tp"),
            P(("rep", "fs"), "tp"),
            P("tp", "fs"),
            P(),
            P("fs", "tp"),
            P("fs", "tp"),
            P("tp", "fs"),
            P(),
        ),
        out_specs=P(("rep", "fs", "tp"), None),
        check_vma=False,
    )
```

```python
import functools

import jax
import jax.numpy as jnp
from jax import lax
from jax.experimental import pallas as pl
from jax.experimental.pallas import tpu as pltpu
from jax.sharding import PartitionSpec as P

residual_scale = 1.4142135623730951

VMEM_BYTES = 60 * 1024 * 1024
LAYER_VMEM_BYTES = 67043328
MESH = pl.DeviceIdType.MESH


def layer_norm(values, gain):
    center = values - jnp.mean(values, axis=-1, keepdims=True)
    variance = jnp.mean(center * center, axis=-1, keepdims=True)
    return center * lax.rsqrt(variance + 1e-05) * gain


def scalars(owners, swapped):
    return jnp.stack([jnp.asarray(v, jnp.int32) for v in [swapped, *owners]])


def split_product(meta, left_ref, part_refs):
    total = None
    for at, part in enumerate(part_refs):
        depth = part.shape[0]
        columns = pl.ds(pl.multiple_of(meta[1 + at] * depth, depth), depth)
        term = jnp.dot(left_ref[:, columns], part[...], preferred_element_type=jnp.float32)
        total = term if total is None else total + term
    return total


def shifted(values, step, fill):
    rows = lax.broadcasted_iota(jnp.int32, values.shape, 0)
    return jnp.where(rows < step, fill, pltpu.roll(values, step, 0))


def sigmoid(values):
    return 1.0 / (1.0 + jnp.exp(-values))


def recur_core(value_in, gate_in, taps, rate_block, inlet_block, plus, shift):
    value_in = value_in.astype(jnp.bfloat16).astype(jnp.float32)
    gate_in = gate_in.astype(jnp.bfloat16).astype(jnp.float32)
    taps = taps.astype(jnp.float32)
    depth = taps.shape[0]
    conv = None
    for tap in range(depth):
        lag = depth - 1 - tap
        moved = value_in if lag == 0 else shifted(value_in, lag, 0.0)
        term = moved * taps[tap : tap + 1, :]
        conv = term if conv is None else conv + term
    conv = conv.astype(jnp.bfloat16)
    rate = sigmoid(jnp.dot(conv, rate_block, preferred_element_type=jnp.float32))
    inlet = sigmoid(jnp.dot(conv, inlet_block, preferred_element_type=jnp.float32))
    log_decay = -8.0 * rate * plus + shift
    decay = jnp.exp(log_decay)
    twice = 2.0 * log_decay
    series = jnp.ones_like(twice)
    for order in range(8, 1, -1):
        series = 1.0 + twice * series * (1.0 / order)
    lost = jnp.where(twice > -0.3, -twice * series, 1.0 - jnp.exp(twice))
    state = jnp.sqrt(lost) * inlet * conv.astype(jnp.float32)
    step = 1
    while step < state.shape[0]:
        state = state + decay * shifted(state, step, 0.0)
        if 2 * step < state.shape[0]:
            decay = decay * shifted(decay, step, 1.0)
        step *= 2
    gelu = 0.5 * gate_in * (
        1.0 + jnp.tanh(0.7978845608028654 * (gate_in + 0.044715 * gate_in * gate_in * gate_in))
    )
    return (state * gelu).astype(jnp.bfloat16)


LINE, OTHER, SIDE, CORE = 0, 1, 2, 3
OWN, OWN_SIDE, FROM_SIDE, FROM_LINE, ON_SIDE, FROM_FAR_SIDE = range(6)
PACKS = ((0, 0, 1), (1, 0, 1), (2, 0, 1), (3, 0, 1), (4, 0, 2), (4, 1, 2))
PLANS = (
    (
        (100, 110, 0, 10, 401, 130, 402, 403),
        (503, 412, 303, 200, 312, 210, 20, 501, 413, 30, 150, 502, 431, 411, 313, 302, 421, 120, 512),
        (50, 311, 511, 513, 301), (432,), (), (), (331, 322), (), (321,), (422,), (220, 40, 451), (230, 423), (),
        (521,), (433, 341), (523,), (351, 522, 333, 140), (441,), (323, 533, 532), (), (), (332,), (), (531, 442),
        (), (), (250, 452), (342,), (352,), (240, 443, 551, 541), (343,), (543,), (353, 453, 552), (542,), (553,),
        (),
    ),
    (

        (130, 100, 0, 10, 301, 20, 200, 403, 110, 401, 503, 402, 302, 421, 120, 412, 303, 312, 501, 150, 502, 210, 411),
        (413,), (313, 50), (311, 512, 40, 513, 511, 432), (), (), (), (), (322, 30), (140,), (331,), (422,),
        (451, 230), (332,), (), (), (), (220, 321, 323, 522, 423, 521), (531,), (351, 441), (532, 431),
        (523, 333, 433, 533), (442, 250), (), (240,), (), (342, 452), (), (), (352,), (), (551, 552),
        (341, 443, 343, 541), (353, 542, 453, 543), (), (553,),
    ),
    (
        (0, 100, 110, 401, 301, 311, 10, 302, 403, 130, 303, 402), (313, 312, 501, 210, 503, 30, 150),
        (200, 412, 20, 411, 502, 50), (120, 413), (512, 513, 511), (432,), (332,), (), (422,), (322,), (331,),
        (140, 321), (451,), (230, 323, 431, 423), (), (), (351,), (341, 421),
        (523, 522, 220, 333, 441, 531, 40, 250, 532, 521), (433,), (), (), (533,), (342,), (352, 452), (),
        (343, 240, 442), (), (443, 551), (), (543, 552, 541), (542, 353, 453), (553,), (), (), (),
    ),
    (
        (100, 401, 0, 10, 110, 302, 311, 402, 312, 301, 303, 403, 501, 413, 200, 20, 30, 503, 502, 150), (), (411,),
        (), (210, 313, 332, 50, 412, 321, 130, 513, 511), (), (120,), (), (512,), (422, 322, 40, 331), (323,),
        (230, 451, 140, 423), (), (), (), (220,), (521,), (421, 432, 433, 523), (522,), (441, 531), (), (333,),
        (351, 342, 532), (), (250, 352), (533,), (), (341, 431, 443, 442), (551, 240), (), (343, 552), (), (),
        (543, 353, 453, 542), (), (452, 541, 553),
    ),
)


def layer_kernel(
    tok_hbm,
    in_hbm,
    gate_hbm,
    taps_ref,
    rate_hbm,
    inlet_hbm,
    param_ref,
    shift_hbm,
    out_hbm,
    first_gain_ref,
    ffgate_hbm,
    ffup_hbm,
    down_hbm,
    second_gain_ref,
    out_ref,
    buf_a,
    buf_b,
    buf_c,
    buf_d,
    tok,
    rate_blocks,
    inlet_blocks,
    shift,
    branch,
    terms,
    came,
    normed,
    hidden,
    load_sem,
    send_sem,
    recv_sem,
    terms_send,
    terms_recv,
    norm_send,
    norm_recv,
):
    core, fs, tp = lax.axis_index("rep"), lax.axis_index("fs"), lax.axis_index("tp")
    z, y = fs // 2, fs % 2
    zs = [z, z + 1 - 2 * (z % 2), 2 - z // 2, 3 - 3 * (z // 2)]
    middle = z * (3 - z) == 2
    role = core + z * (3 - z)
    roles = [role == at for at in range(4)]
    spots = [[k * 2 + y for k in zs], [k * 2 + 1 - y for k in zs]]
    me = spots[0][0]
    targets = {
        LINE: (core, spots[0][1], tp),
        OTHER: (core, (3 - z) * 2 + y, tp),
        SIDE: (core, spots[1][0], tp),
        CORE: (1 - core, me, tp),
    }
    across = (core, me, 1 - tp)
    width = in_hbm.shape[0]
    parts = buf_b.shape[0]
    ff_half = buf_c.shape[3]
    mix_depth, down_depth = buf_b.shape[1], buf_d.shape[1]
    share = out_ref.shape[0]
    block = rate_blocks.shape[1]
    blocks = rate_blocks.shape[0]
    tile = min(256, ff_half)
    tiles = ff_half // tile
    rows = min(64, share)
    row_tiles = share // rows
    own_row = pl.multiple_of(tp * share, share)

    def run_of(base, part, count):
        return pl.ds(pl.multiple_of(base + part * count, count), count)

    def piece(pack, at, half):
        weight, part, count = PACKS[pack]
        if weight == 0:
            return buf_a.at[half, run_of(at * width, part, width // count), :]
        if weight == 1:
            return buf_b.at[at, run_of(half * (mix_depth // 2), part, mix_depth // 2 // count), :]
        if weight < 4:
            return buf_c.at[weight - 2, half, run_of(at * width, part, width // count), :]
        return buf_d.at[at, run_of(half * (down_depth // 2), part, down_depth // 2 // count), :]

    def copy(pack, at, way, half=core):
        return pltpu.make_async_remote_copy(
            src_ref=piece(pack, at, half),
            dst_ref=piece(pack, at, half),
            send_sem=send_sem.at[pack, at, way],
            recv_sem=recv_sem.at[pack, half, at],
            device_id=targets[way],
            device_id_type=MESH,
        )

    c_cols = lambda half: pl.ds(half * ff_half, ff_half)
    own_rows_of = lambda ref, *at: ref.at[(*at, pl.ds(pl.multiple_of(me * width, width), width), slice(None))]
    loads = [
        [(in_hbm, own_rows_of(buf_a, 0)), (gate_hbm, own_rows_of(buf_a, 1))],
        [(out_hbm, buf_b.at[me])],
        [(ffgate_hbm.at[:, c_cols(0)], own_rows_of(buf_c, 0, 0)), (ffup_hbm.at[:, c_cols(0)], own_rows_of(buf_c, 0, 1))],
        [(ffgate_hbm.at[:, c_cols(1)], own_rows_of(buf_c, 1, 0)), (ffup_hbm.at[:, c_cols(1)], own_rows_of(buf_c, 1, 1))],
        [(down_hbm, buf_d.at[me])],
        [(tok_hbm, tok), (shift_hbm, shift), (rate_hbm, rate_blocks), (inlet_hbm, inlet_blocks)],
    ]
    count = 0
    for group in loads:
        for at, (source, target) in enumerate(group):
            group[at] = pltpu.make_async_copy(source, target, load_sem.at[count])
            count += 1

    steps = ["recur"] * blocks + ["mix"] * parts + ["terms"] + ["norm"] * row_tiles + ["rows"]
    steps += ["hidden0"] * tiles + ["hidden1"] * tiles + ["down"] * parts
    begins = {name: steps.index(name) for name in dict.fromkeys(steps)}
    turn_of = [(0, 0), (0, 1), (1, 0), (2, 0), (1, 1), (3, 0), (2, 1), (3, 1)]
    needs = {begins["recur"]: 0, begins["mix"]: 1, begins["hidden0"]: 2, begins["hidden1"]: 3}
    packs_of = [[p for p, (w, _, _) in enumerate(PACKS) if w == weight] for weight in range(5)]

    def actions(plan, in_middle, second):
        loaded, waited, sends, gaps = set(), set(), [], []

        def load(weight, out):
            if weight not in loaded:
                loaded.add(weight)
                out.append(("load", weight))

        def arrive(pack, k, side, out):
            if (k, side) == (0, 0):
                load(PACKS[pack][0], out)
            elif (pack, k, side) not in waited:
                waited.add((pack, k, side))
                out.append(("arrive", pack, k, side))

        def send(pack, k, side, way, out):
            arrive(pack, k, side, out)
            out.append(("send", pack, k, side, way))
            sends.append((pack, k, side, way, len(gaps)))

        for step, codes in enumerate(plan):
            out = []
            for code in codes:
                kind, pack, k = code // 100, code // 10 % 10, code % 10
                if kind == OWN:
                    send(pack, 0, 0, LINE, out)
                    if in_middle:
                        send(pack, 0, 0, OTHER, out)
                elif kind == OWN_SIDE:
                    send(pack, 0, 0, SIDE, out)
                elif kind == FROM_SIDE:
                    arrive(pack, 0, 1, out)
                    if second:
                        send(pack, 0, 1, LINE, out)
                        if in_middle:
                            send(pack, 0, 1, OTHER, out)
                    send(pack, 0, 1, CORE, out)
                elif kind == FROM_LINE:
                    if in_middle:
                        send(pack, k, 0, OTHER if k == 1 else LINE, out)
                    send(pack, k, 0, CORE, out)
                elif kind == ON_SIDE:
                    if k == 3 or not second or (k == 2 and not in_middle):
                        send(pack, k, 0, SIDE, out)
                else:
                    send(pack, k, 1, CORE, out)
            if step in needs:
                weight = needs[step]
                load(weight, out)
                if step == 0:
                    load(5, out)
                for pack in packs_of[weight]:
                    for turn in turn_of[1:]:
                        arrive(pack, *turn, out)
                        out.append(("handed", pack, *turn))
            if begins["down"] <= step:
                turn = turn_of[step - begins["down"]]
                for pack in packs_of[4]:
                    arrive(pack, *turn, out)
                    if turn != (0, 0):
                        out.append(("handed", pack, *turn))
            gaps.append(out)
        return gaps, sends

    programs = [actions(plan, at >= 2, at % 2 == 1) for at, plan in enumerate(PLANS)]

    def act(todo):
        for kind, *rest in todo:
            if kind == "load":
                for one in loads[rest[0]]:
                    one.wait()
                continue
            at = spots[rest[2]][rest[1]]
            if kind == "arrive":
                copy(rest[0], at, CORE).wait_recv()
            elif kind == "handed":
                copy(rest[0], at, CORE, 1 - core).wait_recv()
            elif kind == "send":
                copy(rest[0], at, rest[3]).start()
            else:
                copy(rest[0], at, rest[3]).wait_send()

    def ahead_of(step, index=None):
        for mine, (gaps, _) in zip(roles, programs):
            if gaps[step]:
                asked = mine if index is None else jnp.logical_and(mine, index == step - begins[steps[step]])
                pl.when(asked)(functools.partial(act, gaps[step]))

    def loop(name, length, body):
        def whole(index, _):
            for step in range(begins[name], begins[name] + length):
                ahead_of(step, index)
            body(index)

        lax.fori_loop(0, length, whole, None)

    drained = [set() for _ in programs]

    def drain(weights, before):
        for mine, (_, sends), gone in zip(roles, programs, drained):
            now = [one for one in sends if PACKS[one[0]][0] in weights and one[-1] < before and one not in gone]
            gone.update(now)
            pl.when(mine)(functools.partial(act, [("sent", *one) for one in now]))

    for group in loads:
        for one in group:
            one.start()
    barrier = pltpu.get_barrier_semaphore()
    for target in [targets[LINE], targets[SIDE], targets[CORE], across]:
        pl.semaphore_signal(barrier, inc=1, device_id=target, device_id_type=MESH)

    @pl.when(middle)
    def _():
        pl.semaphore_signal(barrier, inc=1, device_id=targets[OTHER], device_id_type=MESH)

    pl.semaphore_wait(barrier, 4 + z * (3 - z) // 2)

    def recur_step(i):
        cols = pl.ds(pl.multiple_of(i * block, block), block)
        value_in = jnp.dot(tok[...], buf_a[0, :, cols], preferred_element_type=jnp.float32)
        gate_in = jnp.dot(tok[...], buf_a[1, :, cols], preferred_element_type=jnp.float32)
        param = -param_ref[:, cols]
        plus = jnp.maximum(param, 0.0) + jnp.log1p(jnp.exp(-jnp.abs(param)))
        branch[:, cols] = recur_core(
            value_in, gate_in, taps_ref[:, cols], rate_blocks[i], inlet_blocks[i], plus, shift[:, cols]
        )

    loop("recur", blocks, recur_step)

    def terms_copy(phase, at):
        return pltpu.make_async_remote_copy(
            src_ref=terms.at[1 - tp, at],
            dst_ref=came.at[phase, at],
            send_sem=terms_send.at[phase, at],
            recv_sem=terms_recv.at[phase, at],
            device_id=across,
            device_id_type=MESH,
        )

    def keep(product, at):
        product = product.astype(jnp.bfloat16)
        for row in range(2):
            terms[row, at] = product[row * share : (row + 1) * share]

    def mix_step(s):
        keep(jnp.dot(branch[...], buf_b[s], preferred_element_type=jnp.float32), s)
        pl.when(s > 0)(lambda: terms_copy(0, s - 1).start())

    loop("mix", parts, mix_step)
    drain([0], begins["recur"] + 1)
    terms_copy(0, parts - 1).start()
    ahead_of(begins["terms"])
    for s in range(parts):
        terms_copy(0, s).wait_recv()

    def norm_rows(i, phase, residual, gain_ref):
        here = pl.ds(pl.multiple_of(i * rows, rows), rows)
        value = jnp.concatenate(
            [
                terms[tp, s, here, :].astype(jnp.float32) + came[phase, s, here, :].astype(jnp.float32)
                for s in range(parts)
            ],
            axis=1,
        )
        return layer_norm(residual_scale * residual.astype(jnp.float32) + value, gain_ref[...]).astype(jnp.bfloat16)

    def own_rows(i):
        return pl.ds(pl.multiple_of(own_row + i * rows, rows), rows)

    def norm_copy(i):
        return pltpu.make_async_remote_copy(
            src_ref=normed.at[own_rows(i), :],
            dst_ref=normed.at[own_rows(i), :],
            send_sem=norm_send.at[i],
            recv_sem=norm_recv.at[i],
            device_id=across,
            device_id_type=MESH,
        )

    def first_norm(i):
        normed[own_rows(i), :] = norm_rows(i, 0, tok[own_rows(i), :], first_gain_ref)
        pl.when(i > 0)(lambda: norm_copy(i - 1).start())

    loop("norm", row_tiles, first_norm)
    drain([1], begins["terms"])
    for s in range(parts):
        terms_copy(0, s).wait_send()
    norm_copy(row_tiles - 1).start()
    ahead_of(begins["rows"])
    for i in range(row_tiles):
        norm_copy(i).wait_recv()

    def hidden_step(j, half):
        cols = pl.ds(pl.multiple_of(j * tile, tile), tile)
        gate = jnp.dot(normed[...], buf_c[half, 0, :, cols], preferred_element_type=jnp.float32)
        upward = jnp.dot(normed[...], buf_c[half, 1, :, cols], preferred_element_type=jnp.float32)
        to = pl.ds(pl.multiple_of(half * ff_half + j * tile, tile), tile)
        hidden[:, to] = (gate * sigmoid(gate) * upward).astype(jnp.bfloat16)

    loop("hidden0", tiles, lambda j: hidden_step(j, 0))
    loop("hidden1", tiles, lambda j: hidden_step(j, 1))

    order = [spots[side][k] for k, side in turn_of]

    def pick(j):
        at = order[0]
        for turn in range(1, parts):
            at = jnp.where(j == turn, order[turn], at)
        return at

    def down_step(j):
        at = pick(j)
        keep(jnp.dot(hidden[...], buf_d[at], preferred_element_type=jnp.float32), at)
        pl.when(j > 0)(lambda: terms_copy(1, pick(j - 1)).start())

    loop("down", parts, down_step)
    drain(range(3), len(steps))
    terms_copy(1, order[-1]).start()
    drain(range(5), len(steps))
    for i in range(row_tiles):
        norm_copy(i).wait_send()
    for s in order:
        terms_copy(1, s).wait_recv()

    def second_norm(i, _):
        here = pl.ds(pl.multiple_of(i * rows, rows), rows)
        out_ref[here, :] = norm_rows(i, 1, normed[own_rows(i), :], second_gain_ref)

    lax.fori_loop(0, row_tiles, second_norm, None)
    for s in range(parts):
        terms_copy(1, s).wait_send()


def whole_layer(
    tokens,
    recurrence_branch_weight,
    gate_branch_weight,
    convolution_kernel,
    recurrence_gate_blockwise,
    input_gate_blockwise,
    channel_decay_param,
    token_decay_shift,
    recurrence_output_weight,
    first_norm_gain,
    feedforward_gate_weight,
    feedforward_up_weight,
    feedforward_down_weight,
    second_norm_gain,
):
    length, model = tokens.shape
    parts = lax.axis_size("fs")
    share = length // lax.axis_size("tp")
    depth, channels = recurrence_branch_weight.shape
    units = feedforward_gate_weight.shape[1]
    columns = recurrence_output_weight.shape[1]
    hbm = pl.BlockSpec(memory_space=pl.ANY)
    vmem = pl.BlockSpec(memory_space=pltpu.VMEM)
    half = jnp.bfloat16
    packs = len(PACKS)
    row_tiles = share // min(64, share)
    return pl.pallas_call(
        layer_kernel,
        in_specs=[hbm, hbm, hbm, vmem, hbm, hbm, vmem, hbm, hbm, vmem, hbm, hbm, hbm, vmem],
        out_specs=vmem,
        out_shape=jax.ShapeDtypeStruct((share, model), half),
        scratch_shapes=[
            pltpu.VMEM((2, depth * parts, channels), half),
            pltpu.VMEM((parts, channels, columns), half),
            pltpu.VMEM((2, 2, depth * parts, units // 2), half),
            pltpu.VMEM((parts, units, columns), half),
            pltpu.VMEM((length, model), half),
            pltpu.VMEM(recurrence_gate_blockwise.shape, half),
            pltpu.VMEM(input_gate_blockwise.shape, half),
            pltpu.VMEM((length, channels), jnp.float32),
            pltpu.VMEM((length, channels), half),
            pltpu.VMEM((2, parts, share, columns), half),
            pltpu.VMEM((2, parts, share, columns), half),
            pltpu.VMEM((length, model), half),
            pltpu.VMEM((length, units), half),
            pltpu.SemaphoreType.DMA((12,)),
            pltpu.SemaphoreType.DMA((packs, parts, 4)),
            pltpu.SemaphoreType.DMA((packs, 2, parts)),
            pltpu.SemaphoreType.DMA((2, parts)),
            pltpu.SemaphoreType.DMA((2, parts)),
            pltpu.SemaphoreType.DMA((row_tiles,)),
            pltpu.SemaphoreType.DMA((row_tiles,)),
        ],
        cost_estimate=pl.CostEstimate(
            flops=2 * length * model * (2 * channels + 2 * units) + 2 * length * model * (channels + units),
            bytes_accessed=2 * model * (3 * channels + 3 * units),
            transcendentals=0,
        ),
        compiler_params=pltpu.CompilerParams(
            vmem_limit_bytes=LAYER_VMEM_BYTES, collective_id=0, has_side_effects=True
        ),
    )(
        tokens,
        recurrence_branch_weight,
        gate_branch_weight,
        convolution_kernel,
        recurrence_gate_blockwise,
        input_gate_blockwise,
        channel_decay_param[None, :],
        token_decay_shift,
        recurrence_output_weight,
        first_norm_gain[None, :],
        feedforward_gate_weight,
        feedforward_up_weight,
        feedforward_down_weight,
        second_norm_gain[None, :],
    )


def recurrence_kernel(count, meta, x_ref, taps_ref, rate_ref, inlet_ref, plus_ref, shift_ref, *refs):
    mine, other, out_ref = refs[:count], refs[count : 2 * count], refs[-1]
    first = split_product(meta, x_ref, mine)
    second = split_product(meta, x_ref, other)
    out_ref[...] = recur_core(
        first, second, taps_ref[...], rate_ref[0], inlet_ref[0], plus_ref[...], shift_ref[...]
    )


def recurrence(tokens, mine, other, meta, taps, rate_blocks, inlet_blocks, plus, shift):
    length, width = tokens.shape
    block = rate_blocks.shape[1]
    blocks = rate_blocks.shape[0]
    parts = [pl.BlockSpec((p.shape[0], block), lambda i: (0, i)) for p in [*mine, *other]]
    column = lambda rows: pl.BlockSpec((rows, block), lambda i: (0, i))
    square = pl.BlockSpec((1, block, block), lambda i: (i, 0, 0))
    return pl.pallas_call(
        functools.partial(recurrence_kernel, len(mine)),
        grid=(blocks,),
        in_specs=[
            pl.BlockSpec(memory_space=pltpu.SMEM),
            pl.BlockSpec((length, width), lambda i: (0, 0)),
            column(taps.shape[0]),
            square,
            square,
            column(1),
            column(length),
            *parts,
        ],
        out_specs=column(length),
        out_shape=jax.ShapeDtypeStruct((length, block * blocks), jnp.bfloat16),
        cost_estimate=pl.CostEstimate(
            flops=4 * length * width * block * blocks,
            bytes_accessed=4 * width * block * blocks + 8 * length * block * blocks,
            transcendentals=0,
        ),
        compiler_params=pltpu.CompilerParams(vmem_limit_bytes=VMEM_BYTES),
    )(meta, tokens, taps, rate_blocks, inlet_blocks, plus, shift, *mine, *other)


def hidden_kernel(count, meta, x_ref, *refs):
    mine, other, out_ref = refs[:count], refs[count : 2 * count], refs[-1]
    first = split_product(meta, x_ref, mine)
    second = split_product(meta, x_ref, other)
    swapped = meta[0] == 1
    gate = jnp.where(swapped, second, first)
    upward = jnp.where(swapped, first, second)
    out_ref[...] = (gate * sigmoid(gate) * upward).astype(jnp.bfloat16)


def hidden_units(normed, mine, other, meta):
    length, width = normed.shape
    units = mine[0].shape[1]
    tile = next(t for t in (512, 640, 256, 128, units) if units % t == 0)
    return pl.pallas_call(
        functools.partial(hidden_kernel, len(mine)),
        grid=(units // tile,),
        in_specs=[
            pl.BlockSpec(memory_space=pltpu.SMEM),
            pl.BlockSpec((length, width), lambda i: (0, 0)),
            *[pl.BlockSpec((p.shape[0], tile), lambda i: (0, i)) for p in [*mine, *other]],
        ],
        out_specs=pl.BlockSpec((length, tile), lambda i: (0, i)),
        out_shape=jax.ShapeDtypeStruct((length, units), jnp.bfloat16),
        cost_estimate=pl.CostEstimate(
            flops=4 * length * width * units, bytes_accessed=4 * width * units, transcendentals=0
        ),
        compiler_params=pltpu.CompilerParams(vmem_limit_bytes=VMEM_BYTES),
    )(meta, normed, *mine, *other)


def outward_kernel(count, meta, left_ref, *refs):
    mine, other, out_ref = refs[:count], refs[count : 2 * count], refs[-1]
    half = mine[0].shape[0]
    near = pl.ds(pl.multiple_of(meta[0] * half, 128), half)
    far = pl.ds(pl.multiple_of((1 - meta[0]) * half, 128), half)
    start = 0
    for at in range(count):
        total = jnp.dot(left_ref[:, near], mine[at][...], preferred_element_type=jnp.float32)
        total += jnp.dot(left_ref[:, far], other[at][...], preferred_element_type=jnp.float32)
        columns = mine[at].shape[1]
        out_ref[:, start : start + columns] = total.astype(jnp.bfloat16)
        start += columns


def outward(left, mine, other, meta):
    length, depth = left.shape
    width = sum(p.shape[1] for p in mine)
    rows = min(length, 256)
    whole = [pl.BlockSpec(p.shape, lambda i: (0, 0)) for p in [*mine, *other]]
    return pl.pallas_call(
        functools.partial(outward_kernel, len(mine)),
        grid=(length // rows,),
        in_specs=[
            pl.BlockSpec(memory_space=pltpu.SMEM),
            pl.BlockSpec((rows, depth), lambda i: (i, 0)),
            *whole,
        ],
        out_specs=pl.BlockSpec((rows, width), lambda i: (i, 0)),
        out_shape=jax.ShapeDtypeStruct((length, width), jnp.bfloat16),
        cost_estimate=pl.CostEstimate(
            flops=2 * length * width * depth, bytes_accessed=2 * width * depth, transcendentals=0
        ),
        compiler_params=pltpu.CompilerParams(vmem_limit_bytes=VMEM_BYTES),
    )(meta, left, *mine, *other)


def gathered_layer(
    tokens,
    recurrence_branch_weight,
    gate_branch_weight,
    convolution_kernel,
    recurrence_gate_blockwise,
    input_gate_blockwise,
    channel_decay_param,
    token_decay_shift,
    recurrence_output_weight,
    first_norm_gain,
    feedforward_gate_weight,
    feedforward_up_weight,
    feedforward_down_weight,
    second_norm_gain,
):
    share = tokens.shape[0] // lax.axis_size("tp")
    offset = lax.axis_index("tp") * share
    rows_of = lambda weight: [lax.all_gather(weight, "fs", axis=0, tiled=True)]

    def halves_of(weight):
        half = weight.shape[0] // 2
        return [[lax.all_gather(part, "fs", axis=1, tiled=True)] for part in (weight[:half], weight[half:])]

    meta = scalars([jnp.int32(0)], jnp.int32(0))
    branch = recurrence(
        tokens,
        rows_of(recurrence_branch_weight),
        rows_of(gate_branch_weight),
        meta,
        convolution_kernel,
        recurrence_gate_blockwise,
        input_gate_blockwise,
        jax.nn.softplus(-channel_decay_param)[None, :],
        token_decay_shift,
    )

    def grouped(left, weight):
        terms = outward(left, *halves_of(weight), meta)
        return lax.psum_scatter(terms, "tp", scatter_dimension=0, tiled=True).astype(jnp.float32)

    mix = grouped(branch, recurrence_output_weight)
    own_tokens = lax.dynamic_slice_in_dim(tokens, offset, share, 0)
    normed = layer_norm(
        residual_scale * own_tokens.astype(jnp.float32) + mix, first_norm_gain
    ).astype(jnp.bfloat16)
    rows = lax.all_gather(normed, "tp", axis=0, tiled=True)
    hidden = hidden_units(rows, rows_of(feedforward_gate_weight), rows_of(feedforward_up_weight), meta)
    ffn = grouped(hidden, feedforward_down_weight)
    return layer_norm(residual_scale * normed.astype(jnp.float32) + ffn, second_norm_gain).astype(
        jnp.bfloat16
    )


def solution(mesh):
    sizes = mesh.shape
    one_kernel = sizes["rep"] == 2 and sizes["tp"] == 2 and sizes["fs"] == 8
    return jax.shard_map(
        whole_layer if one_kernel else gathered_layer,
        mesh=mesh,
        in_specs=(
            P(("rep", "fs"), None),
            P("fs", "tp"),
            P("fs", "tp"),
            P(None, "tp"),
            P("tp", None, None),
            P("tp", None, None),
            P("tp"),
            P(("rep", "fs"), "tp"),
            P("tp", "fs"),
            P(),
            P("fs", "tp"),
            P("fs", "tp"),
            P("tp", "fs"),
            P(),
        ),
        out_specs=P(("rep", "fs", "tp"), None),
        check_vma=False,
    )
```

```python
import functools

import jax
import jax.numpy as jnp
from jax import lax
from jax.experimental import pallas as pl
from jax.experimental.pallas import tpu as pltpu
from jax.sharding import PartitionSpec as P

residual_scale = 1.4142135623730951

VMEM_BYTES = 60 * 1024 * 1024
LAYER_VMEM_BYTES = 67043328
MESH = pl.DeviceIdType.MESH


def layer_norm(values, gain):
    center = values - jnp.mean(values, axis=-1, keepdims=True)
    variance = jnp.mean(center * center, axis=-1, keepdims=True)
    return center * lax.rsqrt(variance + 1e-05) * gain


def scalars(owners, swapped):
    return jnp.stack([jnp.asarray(v, jnp.int32) for v in [swapped, *owners]])


def split_product(meta, left_ref, part_refs):
    total = None
    for at, part in enumerate(part_refs):
        depth = part.shape[0]
        columns = pl.ds(pl.multiple_of(meta[1 + at] * depth, depth), depth)
        term = jnp.dot(left_ref[:, columns], part[...], preferred_element_type=jnp.float32)
        total = term if total is None else total + term
    return total


def shifted(values, step, fill):
    rows = lax.broadcasted_iota(jnp.int32, values.shape, 0)
    return jnp.where(rows < step, fill, pltpu.roll(values, step, 0))


def sigmoid(values):
    return 1.0 / (1.0 + jnp.exp(-values))


def recur_core(value_in, gate_in, taps, rate_block, inlet_block, plus, shift):
    value_in = value_in.astype(jnp.bfloat16).astype(jnp.float32)
    gate_in = gate_in.astype(jnp.bfloat16).astype(jnp.float32)
    taps = taps.astype(jnp.float32)
    depth = taps.shape[0]
    conv = None
    for tap in range(depth):
        lag = depth - 1 - tap
        moved = value_in if lag == 0 else shifted(value_in, lag, 0.0)
        term = moved * taps[tap : tap + 1, :]
        conv = term if conv is None else conv + term
    conv = conv.astype(jnp.bfloat16)
    rate = sigmoid(jnp.dot(conv, rate_block, preferred_element_type=jnp.float32))
    inlet = sigmoid(jnp.dot(conv, inlet_block, preferred_element_type=jnp.float32))
    log_decay = -8.0 * rate * plus + shift
    decay = jnp.exp(log_decay)
    twice = 2.0 * log_decay
    series = jnp.ones_like(twice)
    for order in range(8, 1, -1):
        series = 1.0 + twice * series * (1.0 / order)
    lost = jnp.where(twice > -0.3, -twice * series, 1.0 - jnp.exp(twice))
    state = jnp.sqrt(lost) * inlet * conv.astype(jnp.float32)
    step = 1
    while step < state.shape[0]:
        state = state + decay * shifted(state, step, 0.0)
        if 2 * step < state.shape[0]:
            decay = decay * shifted(decay, step, 1.0)
        step *= 2
    gelu = 0.5 * gate_in * (
        1.0 + jnp.tanh(0.7978845608028654 * (gate_in + 0.044715 * gate_in * gate_in * gate_in))
    )
    return (state * gelu).astype(jnp.bfloat16)


LINE, OTHER, SIDE, CORE = 0, 1, 2, 3
INPUTS = 7
OWN, OWN_SIDE, FROM_SIDE, FROM_LINE, ON_SIDE, FROM_FAR_SIDE = range(6)
A_PARTS = 1
PACKS = ((0, 0, 1), (2, 0, 1), (3, 0, 1), (4, 0, 1), (5, 0, 2), (5, 1, 2), (6, 0, 1))
ALONG = ((1, 1), (1, 1), (0, 0), (1, 1), (0, 0), (1, 1), (1, 1))
PLANS = (
    (
        (110, 331, 130, 10, 160, 421, 0, 402, 100, 200, 20, 403, 502, 531, 301, 522, 333, 210, 60, 311),
        (501, 503, 302, 50, 431), (30, 230, 451, 412, 303), (413, 401), (513, 312, 512, 511, 120), (40,), (140,), (),
        (), (341,), (), (332,), (441, 260, 313), (351,), (), (150,), (), (), (), (), (523, 461), (342,), (442, 453),
        (), (), (452, 240), (553, 343, 541), (), (), (443, 321), (542,), (), (551,), (361, 352, 411), (), (), (533,),
        (353,), (), (), (), (250, 323, 462, 552, 543), (220, 362), (), (363,), (), (), (562, 423, 532, 322), (433,),
        (521, 463, 561), (), (563,), (), (), (422, 432),
    ),
    (

        (522, 110, 100, 0, 130, 160, 60, 331, 333, 10, 50, 20, 210, 200, 531, 301, 402, 230, 30, 421, 40, 502, 501, 302, 401, 403, 451, 503, 413, 303, 311, 412, 120, 512, 313, 312, 513, 511, 361),
        (260,), (), (), (140, 441), (523,), (), (442,), (), (341, 150), (), (), (), (453,), (), (), (452,),
        (431, 332, 461), (), (323, 443), (), (), (411, 553, 240, 343, 352, 321, 250, 322, 541, 342), (), (), (), (),
        (), (), (542,), (), (463,), (), (462, 351, 423, 533, 353), (), (521, 432, 551), (), (552,), (543,), (), (),
        (362, 363), (), (), (), (532,), (), (), (433,), (), (), (), (422, 561, 563), (562,), (220,),
    ),
    (
        (140, 0, 150, 10, 311, 302, 301, 110, 100, 403, 303, 210, 200, 451, 20, 413, 402), (130, 501, 503),
        (502, 511, 240, 312, 512, 313), (120, 40), (), (), (351,), (), (50,), (422, 421, 331, 513), (442,),
        (342, 321, 401), (30,), (353,), (), (230, 341, 160), (60,), (433, 521, 531), (332,), (),
        (423, 333, 250, 361, 352), (323, 523), (441, 533, 343, 453, 443, 522, 220, 532), (), (322, 362), (561,),
        (542,), (541, 260), (), (), (), (), (), (363, 461, 463, 552), (), (), (), (), (), (431,), (562, 543), (), (),
        (553, 551), (), (), (), (), (), (411,), (), (), (), (412,), (432, 452, 563, 462),
    ),
    (

        (100, 130, 0, 302, 110, 150, 200, 301, 10, 120, 403, 502, 303, 311, 401, 413, 313, 501, 160, 60, 503, 511, 140, 441, 402, 210, 312, 321, 512, 451, 20),
        (513, 40, 362), (), (50,), (), (422, 421, 351), (), (), (), (342, 442, 30), (353, 240), (), (220,),
        (521, 352, 331), (), (332,), (531, 341, 423), (461,), (), (230, 522, 322, 323, 361, 433, 443, 523, 333),
        (343, 533, 532, 250, 542, 453), (363,), (), (561, 553, 543, 541), (551, 552), (), (), (), (260,), (), (),
        (463,), (431,), (), (), (), (563, 562), (), (), (), (), (), (), (411,), (), (), (), (), (412,), (), (), (),
        (), (), (452, 462, 432),
    ),
)


def layer_kernel(
    tok_hbm,
    in_hbm,
    gate_hbm,
    taps_ref,
    rate_hbm,
    inlet_hbm,
    param_ref,
    shift_hbm,
    out_hbm,
    first_gain_ref,
    ffgate_hbm,
    ffup_hbm,
    down_hbm,
    second_gain_ref,
    out_ref,
    buf_a,
    buf_b,
    buf_e,
    buf_f,
    buf_c,
    buf_d,
    tok,
    rate_blocks,
    inlet_blocks,
    shift,
    branch,
    terms,
    came,
    normed,
    hidden,
    load_sem,
    send_sem,
    recv_sem,
    terms_send,
    terms_recv,
    norm_send,
    norm_recv,
    far_send,
    far_recv,
    back_send,
    back_recv,
    free_sem,
):
    core, fs, tp = lax.axis_index("rep"), lax.axis_index("fs"), lax.axis_index("tp")
    z, y = fs // 2, fs % 2
    zs = [z, z + 1 - 2 * (z % 2), 2 - z // 2, 3 - 3 * (z // 2)]
    middle = z * (3 - z) == 2
    role = core + z * (3 - z)
    roles = [role == at for at in range(4)]
    outer = jnp.logical_not(middle)
    spots = [[k * 2 + y for k in zs], [k * 2 + 1 - y for k in zs]]
    me = spots[0][0]
    targets = {
        LINE: (core, spots[0][1], tp),
        OTHER: (core, (3 - z) * 2 + y, tp),
        SIDE: (core, spots[1][0], tp),
        CORE: (1 - core, me, tp),
    }
    across = (core, me, 1 - tp)
    width = in_hbm.shape[0]
    parts = buf_b.shape[0]
    first_units, other_units = buf_e.shape[2], buf_c.shape[2]
    a_columns = buf_a.shape[3]
    mix_depth = buf_b.shape[1]
    share = out_ref.shape[0]
    block = rate_blocks.shape[1]
    blocks = rate_blocks.shape[0]
    tile = min(256, first_units)
    first_tiles, other_tiles = first_units // tile, other_units // tile
    rows = min(64, share)
    row_tiles = share // rows
    own_row = pl.multiple_of(tp * share, share)

    def run_of(base, part, count):
        return pl.ds(pl.multiple_of(base + part * count, count), count)

    def piece(pack, at, half):
        weight, part, count = PACKS[pack]
        by_row = run_of(at * width, part, width // count)
        by_depth = lambda depth: run_of(half * (depth // 2), part, depth // 2 // count)
        if weight < 2:
            return buf_a.at[weight, half, by_row, :]
        if weight == 2:
            return buf_b.at[at, by_depth(mix_depth), :]
        if weight == 3:
            return buf_e.at[half, by_row, :]
        if weight == 4:
            return buf_f.at[at, by_depth(first_units), :]
        if weight == 5:
            return buf_c.at[half, by_row, :]
        return buf_d.at[at, by_depth(other_units), :]

    def copy(pack, at, way, half=core):
        return pltpu.make_async_remote_copy(
            src_ref=piece(pack, at, half),
            dst_ref=piece(pack, at, half),
            send_sem=send_sem.at[pack, at, way],
            recv_sem=recv_sem.at[pack, half, at],
            device_id=targets[way],
            device_id_type=MESH,
        )

    own_rows_of = lambda ref, *at: ref.at[(*at, pl.ds(pl.multiple_of(me * width, width), width), slice(None))]
    a_part = lambda part: [
        (ref.at[:, pl.ds(part * a_columns, a_columns)], own_rows_of(buf_a, part, half))
        for half, ref in enumerate((in_hbm, gate_hbm))
    ]
    units_of = lambda start, count, buf: [
        (ref.at[:, pl.ds(start, count)], own_rows_of(buf, half)) for half, ref in enumerate((ffgate_hbm, ffup_hbm))
    ]
    loads = [
        a_part(0),
        a_part(1) if A_PARTS == 2 else [],
        [(out_hbm, buf_b.at[me])],
        units_of(0, first_units, buf_e),
        [(down_hbm.at[pl.ds(0, first_units), :], buf_f.at[me])],
        units_of(first_units, other_units, buf_c),
        [(down_hbm.at[pl.ds(first_units, other_units), :], buf_d.at[me])],
        [(tok_hbm, tok), (shift_hbm, shift), (rate_hbm, rate_blocks), (inlet_hbm, inlet_blocks)],
    ]
    count = 0
    for group in loads:
        for at, (source, target) in enumerate(group):
            group[at] = pltpu.make_async_copy(source, target, load_sem.at[count])
            count += 1

    steps = ["recur"] * blocks + ["mix"] * parts + ["terms"] + ["norm"] * row_tiles + ["rows"] * row_tiles
    steps += ["first"] * first_tiles + ["far"] * parts + ["back"] * parts
    steps += ["hidden"] * other_tiles + ["down"] * parts
    begins = {name: steps.index(name) for name in dict.fromkeys(steps)}
    turn_of = [(0, 0), (0, 1), (1, 0), (2, 0), (1, 1), (3, 0), (2, 1), (3, 1)]
    needs = {begins["recur"]: 0, begins["mix"]: 2, begins["first"]: 3, begins["far"]: 4, begins["hidden"]: 5}
    if A_PARTS == 2:
        needs[begins["recur"] + blocks // 2] = 1
    packs_of = [[p for p, (w, _, _) in enumerate(PACKS) if w == weight] for weight in range(INPUTS)]

    def actions(plan, in_middle, second):
        loaded, waited, sends, gaps = set(), set(), [], []

        def load(weight, out):
            if weight not in loaded:
                loaded.add(weight)
                out.append(("load", weight))

        def arrive(pack, k, side, out):
            if (k, side) == (0, 0):
                load(PACKS[pack][0], out)
            elif (pack, k, side) not in waited:
                waited.add((pack, k, side))
                out.append(("arrive", pack, k, side))

        def send(pack, k, side, way, out):
            arrive(pack, k, side, out)
            out.append(("send", pack, k, side, way))
            sends.append((pack, k, side, way, len(gaps)))

        for step, codes in enumerate(plan):
            out = []
            for code in codes:
                kind, pack, k = code // 100, code // 10 % 10, code % 10
                first = PACKS[pack][0] in (3, 4)
                along = ALONG[pack][second]
                if kind == OWN:
                    if not (first and in_middle):
                        send(pack, 0, 0, LINE, out)
                    if in_middle:
                        send(pack, 0, 0, OTHER, out)
                elif kind == OWN_SIDE:
                    if not first or in_middle or along:
                        send(pack, 0, 0, SIDE, out)
                elif kind == FROM_SIDE:
                    if along:
                        if not (first and in_middle):
                            send(pack, 0, 1, LINE, out)
                        if in_middle:
                            send(pack, 0, 1, OTHER, out)
                    if not first or in_middle:
                        send(pack, 0, 1, CORE, out)
                elif first and not in_middle:
                    pass
                elif kind == FROM_LINE:
                    if in_middle and (k == 1 or not first):
                        send(pack, k, 0, OTHER if k == 1 else LINE, out)
                    send(pack, k, 0, CORE, out)
                elif kind == ON_SIDE:
                    if k == 3 or not along or (k == 2 and not in_middle):
                        send(pack, k, 0, SIDE, out)
                else:
                    send(pack, k, 1, CORE, out)
            if step in needs:
                weight = needs[step]
                load(weight, out)
                if step == 0:
                    load(INPUTS, out)
                for pack in packs_of[weight] if in_middle or weight not in (3, 4) else []:
                    for turn in turn_of[1:]:
                        arrive(pack, *turn, out)
                        out.append(("handed", pack, *turn))
            if begins["down"] <= step:
                turn = turn_of[step - begins["down"]]
                for pack in packs_of[6]:
                    arrive(pack, *turn, out)
                    if turn != (0, 0):
                        out.append(("handed", pack, *turn))
            gaps.append(out)
        return gaps, sends

    programs = [actions(plan, at >= 2, at % 2) for at, plan in enumerate(PLANS)]

    def act(todo):
        for kind, *rest in todo:
            if kind == "load":
                for one in loads[rest[0]]:
                    one.wait()
                continue
            at = spots[rest[2]][rest[1]]
            if kind == "arrive":
                copy(rest[0], at, CORE).wait_recv()
            elif kind == "handed":
                copy(rest[0], at, CORE, 1 - core).wait_recv()
            elif kind == "send":
                copy(rest[0], at, rest[3]).start()
            else:
                copy(rest[0], at, rest[3]).wait_send()

    def ahead_of(step, index=None):
        for mine, (gaps, _) in zip(roles, programs):
            if gaps[step]:
                asked = mine if index is None else jnp.logical_and(mine, index == step - begins[steps[step]])
                pl.when(asked)(functools.partial(act, gaps[step]))

    def loop(name, length, body):
        def whole(index, _):
            for step in range(begins[name], begins[name] + length):
                ahead_of(step, index)
            body(index)

        lax.fori_loop(0, length, whole, None)

    drained = [set() for _ in programs]

    def drain(weights, before):
        for mine, (_, sends), gone in zip(roles, programs, drained):
            now = [one for one in sends if PACKS[one[0]][0] in weights and one[-1] < before and one not in gone]
            gone.update(now)
            pl.when(mine)(functools.partial(act, [("sent", *one) for one in now]))

    for group in loads:
        for one in group:
            one.start()
    barrier = pltpu.get_barrier_semaphore()
    for target in [targets[LINE], targets[SIDE], targets[CORE], across]:
        pl.semaphore_signal(barrier, inc=1, device_id=target, device_id_type=MESH)

    @pl.when(middle)
    def _():
        pl.semaphore_signal(barrier, inc=1, device_id=targets[OTHER], device_id_type=MESH)

    pl.semaphore_wait(barrier, 4 + z * (3 - z) // 2)

    def recur_step(i):
        cols = pl.ds(pl.multiple_of(i * block, block), block)
        part, place = (i * block) // a_columns, pl.ds(pl.multiple_of(i * block % a_columns, block), block)
        value_in = jnp.dot(tok[...], buf_a[part, 0, :, place], preferred_element_type=jnp.float32)
        gate_in = jnp.dot(tok[...], buf_a[part, 1, :, place], preferred_element_type=jnp.float32)
        param = -param_ref[:, cols]
        plus = jnp.maximum(param, 0.0) + jnp.log1p(jnp.exp(-jnp.abs(param)))
        branch[:, cols] = recur_core(
            value_in, gate_in, taps_ref[:, cols], rate_blocks[i], inlet_blocks[i], plus, shift[:, cols]
        )

    loop("recur", blocks, recur_step)

    def terms_copy(phase, at):
        return pltpu.make_async_remote_copy(
            src_ref=terms.at[1 - tp, at],
            dst_ref=came.at[phase % 2, at],
            send_sem=terms_send.at[phase, at],
            recv_sem=terms_recv.at[phase, at],
            device_id=across,
            device_id_type=MESH,
        )

    def keep(product, at):
        product = product.astype(jnp.bfloat16)
        for row in range(2):
            terms[row, at] = product[row * share : (row + 1) * share]

    def mix_step(s):
        keep(jnp.dot(branch[...], buf_b[s], preferred_element_type=jnp.float32), s)
        pl.when(s > 0)(lambda: terms_copy(0, s - 1).start())

    loop("mix", parts, mix_step)
    drain([0, 1], begins["recur"] + 1)
    terms_copy(0, parts - 1).start()
    ahead_of(begins["terms"])
    for s in range(parts):
        terms_copy(0, s).wait_recv()

    def norm_rows(i, phase, residual, gain_ref):
        here = pl.ds(pl.multiple_of(i * rows, rows), rows)

        def total(s):
            value = terms[tp, s, here, :].astype(jnp.float32) + came[phase, s, here, :].astype(jnp.float32)
            return value if phase == 0 else value + jnp.where(outer, came[0, s, here, :].astype(jnp.float32), 0.0)

        value = jnp.concatenate([total(s) for s in range(parts)], axis=1)
        return layer_norm(residual_scale * residual.astype(jnp.float32) + value, gain_ref[...]).astype(jnp.bfloat16)

    def own_rows(i):
        return pl.ds(pl.multiple_of(own_row + i * rows, rows), rows)

    def norm_copy(i):
        return pltpu.make_async_remote_copy(
            src_ref=normed.at[own_rows(i), :],
            dst_ref=normed.at[own_rows(i), :],
            send_sem=norm_send.at[i],
            recv_sem=norm_recv.at[i],
            device_id=across,
            device_id_type=MESH,
        )

    def far_copy(half, i):
        here = pl.ds(pl.multiple_of(half * share + i * rows, rows), rows)
        return pltpu.make_async_remote_copy(
            src_ref=normed.at[here, :],
            dst_ref=tok.at[here, :],
            send_sem=far_send.at[half, i],
            recv_sem=far_recv.at[half, i],
            device_id=targets[LINE],
            device_id_type=MESH,
        )

    def pass_on(i):
        norm_copy(i).start()
        pl.when(outer)(lambda: far_copy(tp, i).start())

    def first_norm(i):
        normed[own_rows(i), :] = norm_rows(i, 0, tok[own_rows(i), :], first_gain_ref)
        pl.when(jnp.logical_and(outer, i == 1))(lambda: pl.semaphore_wait(free_sem, 1))
        pl.when(i > 0)(lambda: pass_on(i - 1))

    loop("norm", row_tiles, first_norm)
    drain([2], begins["terms"])
    for s in range(parts):
        terms_copy(0, s).wait_send()

    @pl.when(middle)
    def _():
        pl.semaphore_signal(free_sem, inc=1, device_id=targets[LINE], device_id_type=MESH)

    pass_on(row_tiles - 1)
    for i in range(row_tiles):
        ahead_of(begins["rows"] + i)
        norm_copy(i).wait_recv()
        pl.when(outer)(lambda i=i: far_copy(1 - tp, i).start())

    def units_at(left, buf, j):
        cols = pl.ds(pl.multiple_of(j * tile, tile), tile)
        gate = jnp.dot(left[...], buf[0, :, cols], preferred_element_type=jnp.float32)
        upward = jnp.dot(left[...], buf[1, :, cols], preferred_element_type=jnp.float32)
        return (gate * sigmoid(gate) * upward).astype(jnp.bfloat16)

    def in_middle(body):
        def asked(i):
            pl.when(middle)(lambda: body(i))

        return asked

    def first_step(j):
        @pl.when(j == 0)
        def _():
            for half in range(2):
                for i in range(row_tiles):
                    far_copy(half, i).wait_recv()

        to = pl.ds(pl.multiple_of(j * tile, tile), tile)
        hidden[:, to] = units_at(normed, buf_e, j)
        branch[:, to] = units_at(tok, buf_e, j)

    def far_step(s):
        left = branch[:, :first_units]
        keep(jnp.dot(left, buf_f[s], preferred_element_type=jnp.float32), s)
        pl.when(s > 0)(lambda: terms_copy(2, s - 1).start())

    def back_copy(s):
        return pltpu.make_async_remote_copy(
            src_ref=came.at[0, s],
            dst_ref=came.at[0, s],
            send_sem=back_send.at[s],
            recv_sem=back_recv.at[s],
            device_id=targets[LINE],
            device_id_type=MESH,
        )

    def back_step(s):
        pl.when(s == 0)(lambda: terms_copy(2, parts - 1).start())
        terms_copy(2, s).wait_recv()
        came[0, s] = (terms[tp, s].astype(jnp.float32) + came[0, s].astype(jnp.float32)).astype(jnp.bfloat16)
        pl.when(s > 0)(lambda: back_copy(s - 1).start())

    loop("first", first_tiles, in_middle(first_step))
    loop("far", parts, in_middle(far_step))
    loop("back", parts, in_middle(back_step))

    @pl.when(middle)
    def _():
        for s in range(parts):
            terms_copy(2, s).wait_send()
        back_copy(parts - 1).start()

    def hidden_step(j):
        to = pl.ds(pl.multiple_of(first_units + j * tile, tile), tile)
        hidden[:, to] = units_at(normed, buf_c, j)

    loop("hidden", other_tiles, hidden_step)

    order = [spots[side][k] for k, side in turn_of]

    def pick(j):
        at = order[0]
        for turn in range(1, parts):
            at = jnp.where(j == turn, order[turn], at)
        return at

    def down_step(j):
        at = pick(j)
        product = lambda: jnp.dot(hidden[:, first_units:], buf_d[at], preferred_element_type=jnp.float32)
        more = lambda: jnp.dot(hidden[:, :first_units], buf_f[at], preferred_element_type=jnp.float32)
        pl.when(outer)(lambda: keep(product(), at))
        pl.when(middle)(lambda: keep(product() + more(), at))
        pl.when(j > 0)(lambda: terms_copy(1, pick(j - 1)).start())

    loop("down", parts, down_step)
    drain(range(5), len(steps))
    terms_copy(1, order[-1]).start()
    drain(range(INPUTS), len(steps))
    for i in range(row_tiles):
        norm_copy(i).wait_send()

    @pl.when(outer)
    def _():
        for half in range(2):
            for i in range(row_tiles):
                far_copy(half, i).wait_send()
        for s in range(parts):
            back_copy(s).wait_recv()

    @pl.when(middle)
    def _():
        for s in range(parts):
            back_copy(s).wait_send()

    for s in order:
        terms_copy(1, s).wait_recv()

    def second_norm(i, _):
        here = pl.ds(pl.multiple_of(i * rows, rows), rows)
        out_ref[here, :] = norm_rows(i, 1, normed[own_rows(i), :], second_gain_ref)

    lax.fori_loop(0, row_tiles, second_norm, None)
    for s in range(parts):
        terms_copy(1, s).wait_send()


def whole_layer(
    tokens,
    recurrence_branch_weight,
    gate_branch_weight,
    convolution_kernel,
    recurrence_gate_blockwise,
    input_gate_blockwise,
    channel_decay_param,
    token_decay_shift,
    recurrence_output_weight,
    first_norm_gain,
    feedforward_gate_weight,
    feedforward_up_weight,
    feedforward_down_weight,
    second_norm_gain,
):
    length, model = tokens.shape
    parts = lax.axis_size("fs")
    share = length // lax.axis_size("tp")
    depth, channels = recurrence_branch_weight.shape
    units = feedforward_gate_weight.shape[1]
    first_units = units * 2 // 5 // 256 * 256
    columns = recurrence_output_weight.shape[1]
    hbm = pl.BlockSpec(memory_space=pl.ANY)
    vmem = pl.BlockSpec(memory_space=pltpu.VMEM)
    half = jnp.bfloat16
    packs = len(PACKS)
    row_tiles = share // min(64, share)
    return pl.pallas_call(
        layer_kernel,
        in_specs=[hbm, hbm, hbm, vmem, hbm, hbm, vmem, hbm, hbm, vmem, hbm, hbm, hbm, vmem],
        out_specs=vmem,
        out_shape=jax.ShapeDtypeStruct((share, model), half),
        scratch_shapes=[
            pltpu.VMEM((A_PARTS, 2, depth * parts, channels // A_PARTS), half),
            pltpu.VMEM((parts, channels, columns), half),
            pltpu.VMEM((2, depth * parts, first_units), half),
            pltpu.VMEM((parts, first_units, columns), half),
            pltpu.VMEM((2, depth * parts, units - first_units), half),
            pltpu.VMEM((parts, units - first_units, columns), half),
            pltpu.VMEM((length, model), half),
            pltpu.VMEM(recurrence_gate_blockwise.shape, half),
            pltpu.VMEM(input_gate_blockwise.shape, half),
            pltpu.VMEM((length, channels), jnp.float32),
            pltpu.VMEM((length, channels), half),
            pltpu.VMEM((2, parts, share, columns), half),
            pltpu.VMEM((2, parts, share, columns), half),
            pltpu.VMEM((length, model), half),
            pltpu.VMEM((length, units), half),
            pltpu.SemaphoreType.DMA((15,)),
            pltpu.SemaphoreType.DMA((packs, parts, 4)),
            pltpu.SemaphoreType.DMA((packs, 2, parts)),
            pltpu.SemaphoreType.DMA((3, parts)),
            pltpu.SemaphoreType.DMA((3, parts)),
            pltpu.SemaphoreType.DMA((row_tiles,)),
            pltpu.SemaphoreType.DMA((row_tiles,)),
            pltpu.SemaphoreType.DMA((2, row_tiles)),
            pltpu.SemaphoreType.DMA((2, row_tiles)),
            pltpu.SemaphoreType.DMA((parts,)),
            pltpu.SemaphoreType.DMA((parts,)),
            pltpu.SemaphoreType.REGULAR,
        ],
        cost_estimate=pl.CostEstimate(
            flops=2 * length * model * (2 * channels + 2 * units) + 2 * length * model * (channels + units),
            bytes_accessed=2 * model * (3 * channels + 3 * units),
            transcendentals=0,
        ),
        compiler_params=pltpu.CompilerParams(
            vmem_limit_bytes=LAYER_VMEM_BYTES, collective_id=0, has_side_effects=True
        ),
    )(
        tokens,
        recurrence_branch_weight,
        gate_branch_weight,
        convolution_kernel,
        recurrence_gate_blockwise,
        input_gate_blockwise,
        channel_decay_param[None, :],
        token_decay_shift,
        recurrence_output_weight,
        first_norm_gain[None, :],
        feedforward_gate_weight,
        feedforward_up_weight,
        feedforward_down_weight,
        second_norm_gain[None, :],
    )


def recurrence_kernel(count, meta, x_ref, taps_ref, rate_ref, inlet_ref, plus_ref, shift_ref, *refs):
    mine, other, out_ref = refs[:count], refs[count : 2 * count], refs[-1]
    first = split_product(meta, x_ref, mine)
    second = split_product(meta, x_ref, other)
    out_ref[...] = recur_core(
        first, second, taps_ref[...], rate_ref[0], inlet_ref[0], plus_ref[...], shift_ref[...]
    )


def recurrence(tokens, mine, other, meta, taps, rate_blocks, inlet_blocks, plus, shift):
    length, width = tokens.shape
    block = rate_blocks.shape[1]
    blocks = rate_blocks.shape[0]
    parts = [pl.BlockSpec((p.shape[0], block), lambda i: (0, i)) for p in [*mine, *other]]
    column = lambda rows: pl.BlockSpec((rows, block), lambda i: (0, i))
    square = pl.BlockSpec((1, block, block), lambda i: (i, 0, 0))
    return pl.pallas_call(
        functools.partial(recurrence_kernel, len(mine)),
        grid=(blocks,),
        in_specs=[
            pl.BlockSpec(memory_space=pltpu.SMEM),
            pl.BlockSpec((length, width), lambda i: (0, 0)),
            column(taps.shape[0]),
            square,
            square,
            column(1),
            column(length),
            *parts,
        ],
        out_specs=column(length),
        out_shape=jax.ShapeDtypeStruct((length, block * blocks), jnp.bfloat16),
        cost_estimate=pl.CostEstimate(
            flops=4 * length * width * block * blocks,
            bytes_accessed=4 * width * block * blocks + 8 * length * block * blocks,
            transcendentals=0,
        ),
        compiler_params=pltpu.CompilerParams(vmem_limit_bytes=VMEM_BYTES),
    )(meta, tokens, taps, rate_blocks, inlet_blocks, plus, shift, *mine, *other)


def hidden_kernel(count, meta, x_ref, *refs):
    mine, other, out_ref = refs[:count], refs[count : 2 * count], refs[-1]
    first = split_product(meta, x_ref, mine)
    second = split_product(meta, x_ref, other)
    swapped = meta[0] == 1
    gate = jnp.where(swapped, second, first)
    upward = jnp.where(swapped, first, second)
    out_ref[...] = (gate * sigmoid(gate) * upward).astype(jnp.bfloat16)


def hidden_units(normed, mine, other, meta):
    length, width = normed.shape
    units = mine[0].shape[1]
    tile = next(t for t in (512, 640, 256, 128, units) if units % t == 0)
    return pl.pallas_call(
        functools.partial(hidden_kernel, len(mine)),
        grid=(units // tile,),
        in_specs=[
            pl.BlockSpec(memory_space=pltpu.SMEM),
            pl.BlockSpec((length, width), lambda i: (0, 0)),
            *[pl.BlockSpec((p.shape[0], tile), lambda i: (0, i)) for p in [*mine, *other]],
        ],
        out_specs=pl.BlockSpec((length, tile), lambda i: (0, i)),
        out_shape=jax.ShapeDtypeStruct((length, units), jnp.bfloat16),
        cost_estimate=pl.CostEstimate(
            flops=4 * length * width * units, bytes_accessed=4 * width * units, transcendentals=0
        ),
        compiler_params=pltpu.CompilerParams(vmem_limit_bytes=VMEM_BYTES),
    )(meta, normed, *mine, *other)


def outward_kernel(count, meta, left_ref, *refs):
    mine, other, out_ref = refs[:count], refs[count : 2 * count], refs[-1]
    half = mine[0].shape[0]
    near = pl.ds(pl.multiple_of(meta[0] * half, 128), half)
    far = pl.ds(pl.multiple_of((1 - meta[0]) * half, 128), half)
    start = 0
    for at in range(count):
        total = jnp.dot(left_ref[:, near], mine[at][...], preferred_element_type=jnp.float32)
        total += jnp.dot(left_ref[:, far], other[at][...], preferred_element_type=jnp.float32)
        columns = mine[at].shape[1]
        out_ref[:, start : start + columns] = total.astype(jnp.bfloat16)
        start += columns


def outward(left, mine, other, meta):
    length, depth = left.shape
    width = sum(p.shape[1] for p in mine)
    rows = min(length, 256)
    whole = [pl.BlockSpec(p.shape, lambda i: (0, 0)) for p in [*mine, *other]]
    return pl.pallas_call(
        functools.partial(outward_kernel, len(mine)),
        grid=(length // rows,),
        in_specs=[
            pl.BlockSpec(memory_space=pltpu.SMEM),
            pl.BlockSpec((rows, depth), lambda i: (i, 0)),
            *whole,
        ],
        out_specs=pl.BlockSpec((rows, width), lambda i: (i, 0)),
        out_shape=jax.ShapeDtypeStruct((length, width), jnp.bfloat16),
        cost_estimate=pl.CostEstimate(
            flops=2 * length * width * depth, bytes_accessed=2 * width * depth, transcendentals=0
        ),
        compiler_params=pltpu.CompilerParams(vmem_limit_bytes=VMEM_BYTES),
    )(meta, left, *mine, *other)


def gathered_layer(
    tokens,
    recurrence_branch_weight,
    gate_branch_weight,
    convolution_kernel,
    recurrence_gate_blockwise,
    input_gate_blockwise,
    channel_decay_param,
    token_decay_shift,
    recurrence_output_weight,
    first_norm_gain,
    feedforward_gate_weight,
    feedforward_up_weight,
    feedforward_down_weight,
    second_norm_gain,
):
    share = tokens.shape[0] // lax.axis_size("tp")
    offset = lax.axis_index("tp") * share
    rows_of = lambda weight: [lax.all_gather(weight, "fs", axis=0, tiled=True)]

    def halves_of(weight):
        half = weight.shape[0] // 2
        return [[lax.all_gather(part, "fs", axis=1, tiled=True)] for part in (weight[:half], weight[half:])]

    meta = scalars([jnp.int32(0)], jnp.int32(0))
    branch = recurrence(
        tokens,
        rows_of(recurrence_branch_weight),
        rows_of(gate_branch_weight),
        meta,
        convolution_kernel,
        recurrence_gate_blockwise,
        input_gate_blockwise,
        jax.nn.softplus(-channel_decay_param)[None, :],
        token_decay_shift,
    )

    def grouped(left, weight):
        terms = outward(left, *halves_of(weight), meta)
        return lax.psum_scatter(terms, "tp", scatter_dimension=0, tiled=True).astype(jnp.float32)

    mix = grouped(branch, recurrence_output_weight)
    own_tokens = lax.dynamic_slice_in_dim(tokens, offset, share, 0)
    normed = layer_norm(
        residual_scale * own_tokens.astype(jnp.float32) + mix, first_norm_gain
    ).astype(jnp.bfloat16)
    rows = lax.all_gather(normed, "tp", axis=0, tiled=True)
    hidden = hidden_units(rows, rows_of(feedforward_gate_weight), rows_of(feedforward_up_weight), meta)
    ffn = grouped(hidden, feedforward_down_weight)
    return layer_norm(residual_scale * normed.astype(jnp.float32) + ffn, second_norm_gain).astype(
        jnp.bfloat16
    )


def solution(mesh):
    sizes = mesh.shape
    one_kernel = sizes["rep"] == 2 and sizes["tp"] == 2 and sizes["fs"] == 8
    return jax.shard_map(
        whole_layer if one_kernel else gathered_layer,
        mesh=mesh,
        in_specs=(
            P(("rep", "fs"), None),
            P("fs", "tp"),
            P("fs", "tp"),
            P(None, "tp"),
            P("tp", None, None),
            P("tp", None, None),
            P("tp"),
            P(("rep", "fs"), "tp"),
            P("tp", "fs"),
            P(),
            P("fs", "tp"),
            P("fs", "tp"),
            P("tp", "fs"),
            P(),
        ),
        out_specs=P(("rep", "fs", "tp"), None),
        check_vma=False,
    )
```

```python
import functools

import jax
import jax.numpy as jnp
from jax import lax
from jax.experimental import pallas as pl
from jax.experimental.pallas import tpu as pltpu
from jax.sharding import PartitionSpec as P

residual_scale = 1.4142135623730951

VMEM_BYTES = 60 * 1024 * 1024
LAYER_VMEM_BYTES = 67043328
MESH = pl.DeviceIdType.MESH


def layer_norm(values, gain):
    center = values - jnp.mean(values, axis=-1, keepdims=True)
    variance = jnp.mean(center * center, axis=-1, keepdims=True)
    return center * lax.rsqrt(variance + 1e-05) * gain


def scalars(owners, swapped):
    return jnp.stack([jnp.asarray(v, jnp.int32) for v in [swapped, *owners]])


def split_product(meta, left_ref, part_refs):
    total = None
    for at, part in enumerate(part_refs):
        depth = part.shape[0]
        columns = pl.ds(pl.multiple_of(meta[1 + at] * depth, depth), depth)
        term = jnp.dot(left_ref[:, columns], part[...], preferred_element_type=jnp.float32)
        total = term if total is None else total + term
    return total


def shifted(values, step, fill):
    rows = lax.broadcasted_iota(jnp.int32, values.shape, 0)
    return jnp.where(rows < step, fill, pltpu.roll(values, step, 0))


def sigmoid(values):
    return 1.0 / (1.0 + jnp.exp(-values))


def recur_core(value_in, gate_in, taps, rate_block, inlet_block, plus, shift):
    value_in = value_in.astype(jnp.bfloat16).astype(jnp.float32)
    gate_in = gate_in.astype(jnp.bfloat16).astype(jnp.float32)
    taps = taps.astype(jnp.float32)
    depth = taps.shape[0]
    conv = None
    for tap in range(depth):
        lag = depth - 1 - tap
        moved = value_in if lag == 0 else shifted(value_in, lag, 0.0)
        term = moved * taps[tap : tap + 1, :]
        conv = term if conv is None else conv + term
    conv = conv.astype(jnp.bfloat16)
    rate = sigmoid(jnp.dot(conv, rate_block, preferred_element_type=jnp.float32))
    inlet = sigmoid(jnp.dot(conv, inlet_block, preferred_element_type=jnp.float32))
    log_decay = -8.0 * rate * plus + shift
    decay = jnp.exp(log_decay)
    twice = 2.0 * log_decay
    series = jnp.ones_like(twice)
    for order in range(8, 1, -1):
        series = 1.0 + twice * series * (1.0 / order)
    lost = jnp.where(twice > -0.3, -twice * series, 1.0 - jnp.exp(twice))
    state = jnp.sqrt(lost) * inlet * conv.astype(jnp.float32)
    step = 1
    while step < state.shape[0]:
        state = state + decay * shifted(state, step, 0.0)
        if 2 * step < state.shape[0]:
            decay = decay * shifted(decay, step, 1.0)
        step *= 2
    gelu = 0.5 * gate_in * (
        1.0 + jnp.tanh(0.7978845608028654 * (gate_in + 0.044715 * gate_in * gate_in * gate_in))
    )
    return (state * gelu).astype(jnp.bfloat16)


LINE, OTHER, SIDE, CORE = 0, 1, 2, 3
INPUTS = 7
OWN, OWN_SIDE, FROM_SIDE, FROM_LINE, ON_SIDE, FROM_FAR_SIDE = range(6)
A_PARTS = 1
PACKS = ((0, 0, 1), (2, 0, 1), (3, 0, 1), (4, 0, 1), (5, 0, 2), (5, 1, 2), (6, 0, 1))
ALONG = ((6, 7), (4, 5), (2, 3), (7, 6), (5, 5), (4, 5), (2, 2))
PLANS = (
    (

        (130, 220, 323, 0, 10, 100, 20, 332, 200, 401, 40, 402, 403, 303, 301, 501, 302, 502, 110, 503, 311, 150, 230, 411, 210, 412, 50, 413, 512, 313, 511, 60, 250),
        (513, 312), (), (), (), (), (451, 433, 140, 30), (), (), (443, 160, 333), (), (), (), (461, 543, 551, 423),
        (), (442,), (), (462,), (452,), (533,), (521,), (562,), (542, 343), (453, 260), (541, 523), (), (), (342,),
        (), (), (361, 441), (), (), (331,), (), (531, 341, 353, 561, 240, 422), (), (351,), (), (532,),
        (552, 553, 421, 362, 352), (), (463,), (), (432, 120, 363), (), (563,), (), (), (), (), (321, 431), (322,),
        (), (522,),
    ),
    (
        (130, 0, 323, 451, 10, 220, 110, 100, 200, 332, 402, 502, 20, 303, 301, 40, 230, 403, 210),
        (503, 501, 411, 302, 311), (50, 413, 60, 313, 412, 150), (333,), (461,), (432, 160, 140), (),
        (513, 533, 512, 511, 30), (), (), (250, 312), (), (), (523,), (), (423,), (443,), (433,), (462,), (441,), (),
        (), (521,), (541, 442), (343, 452), (), (342,), (353, 453, 562), (), (240, 341, 361), (), (543, 561), (401,),
        (532,), (551,), (), (531, 422), (), (351,), (), (542,), (553, 552), (), (), (352,), (463, 362, 522), (120,),
        (), (363,), (), (), (), (260, 421), (431,), (322, 321, 563, 331),
    ),
    (

        (0, 120, 100, 10, 412, 462, 302, 301, 403, 150, 200, 303, 311, 421, 503, 312, 110, 501, 341, 502, 313, 321, 441, 413, 60, 210),
        (50, 511, 140, 40, 512, 513), (220, 362), (), (443, 323, 401), (531,), (452, 343), (20, 342), (352,), (422,),
        (130, 423), (), (), (), (), (521, 551), (351, 442, 522), (552, 543), (402, 240, 411), (),
        (322, 523, 331, 453, 250, 431, 353, 333, 230, 30, 160, 433), (332, 532, 533), (361,), (542,), (363, 553),
        (461,), (541,), (432,), (), (), (), (), (463,), (260,), (), (563,), (562,), (), (), (), (), (561,), (), (),
        (), (), (), (), (), (), (), (), (), (), (451,),
    ),
    (
        (422, 441, 0, 110, 302, 100, 462, 120, 130, 301, 303, 311, 403, 200, 10, 501, 313),
        (341, 502, 312, 413, 210, 412, 503, 150, 60, 50), (), (140, 421, 513), (), (), (220, 511), (443, 321),
        (343,), (), (), (512,), (), (362, 452), (40,), (), (461, 240, 401, 20, 402), (521, 543, 531), (351, 342), (),
        (423, 323, 331, 322, 552, 352), (551, 522, 250), (230, 353), (523, 411, 433, 442, 30), (361,), (160,), (),
        (542,), (561,), (), (363,), (432, 532, 453, 533), (431, 332), (333,), (260,), (), (), (), (562,), (), (), (),
        (553,), (), (463,), (), (541,), (), (), (), (), (), (), (), (563, 451),
    ),
)


def layer_kernel(
    tok_hbm,
    in_hbm,
    gate_hbm,
    taps_ref,
    rate_hbm,
    inlet_hbm,
    param_ref,
    shift_hbm,
    out_hbm,
    first_gain_ref,
    ffgate_hbm,
    ffup_hbm,
    down_hbm,
    second_gain_ref,
    out_ref,
    buf_a,
    buf_b,
    buf_e,
    buf_f,
    buf_c,
    buf_d,
    tok,
    rate_blocks,
    inlet_blocks,
    shift,
    branch,
    terms,
    came,
    normed,
    hidden,
    load_sem,
    send_sem,
    recv_sem,
    terms_send,
    terms_recv,
    norm_send,
    norm_recv,
    far_send,
    far_recv,
    back_send,
    back_recv,
    free_sem,
):
    core, fs, tp = lax.axis_index("rep"), lax.axis_index("fs"), lax.axis_index("tp")
    z, y = fs // 2, fs % 2
    zs = [z, z + 1 - 2 * (z % 2), 2 - z // 2, 3 - 3 * (z // 2)]
    middle = z * (3 - z) == 2
    role = core + z * (3 - z)
    roles = [role == at for at in range(4)]
    outer = jnp.logical_not(middle)
    spots = [[k * 2 + y for k in zs], [k * 2 + 1 - y for k in zs]]
    me = spots[0][0]
    targets = {
        LINE: (core, spots[0][1], tp),
        OTHER: (core, (3 - z) * 2 + y, tp),
        SIDE: (core, spots[1][0], tp),
        CORE: (1 - core, me, tp),
    }
    across = (core, me, 1 - tp)
    width = in_hbm.shape[0]
    parts = buf_b.shape[0]
    first_units, other_units = buf_e.shape[2], buf_c.shape[2]
    a_columns = buf_a.shape[3]
    mix_depth = buf_b.shape[1]
    share = out_ref.shape[0]
    block = rate_blocks.shape[1]
    blocks = rate_blocks.shape[0]
    tile = min(256, first_units)
    first_tiles, other_tiles = first_units // tile, other_units // tile
    rows = min(64, share)
    row_tiles = share // rows
    own_row = pl.multiple_of(tp * share, share)

    def run_of(base, part, count):
        return pl.ds(pl.multiple_of(base + part * count, count), count)

    def piece(pack, at, half):
        weight, part, count = PACKS[pack]
        by_row = run_of(at * width, part, width // count)
        by_depth = lambda depth: run_of(half * (depth // 2), part, depth // 2 // count)
        if weight < 2:
            return buf_a.at[weight, half, by_row, :]
        if weight == 2:
            return buf_b.at[at, by_depth(mix_depth), :]
        if weight == 3:
            return buf_e.at[half, by_row, :]
        if weight == 4:
            return buf_f.at[at, by_depth(first_units), :]
        if weight == 5:
            return buf_c.at[half, by_row, :]
        return buf_d.at[at, by_depth(other_units), :]

    def copy(pack, at, way, half=core):
        return pltpu.make_async_remote_copy(
            src_ref=piece(pack, at, half),
            dst_ref=piece(pack, at, half),
            send_sem=send_sem.at[pack, at, way],
            recv_sem=recv_sem.at[pack, half, at],
            device_id=targets[way],
            device_id_type=MESH,
        )

    own_rows_of = lambda ref, *at: ref.at[(*at, pl.ds(pl.multiple_of(me * width, width), width), slice(None))]
    a_part = lambda part: [
        (ref.at[:, pl.ds(part * a_columns, a_columns)], own_rows_of(buf_a, part, half))
        for half, ref in enumerate((in_hbm, gate_hbm))
    ]
    units_of = lambda start, count, buf: [
        (ref.at[:, pl.ds(start, count)], own_rows_of(buf, half)) for half, ref in enumerate((ffgate_hbm, ffup_hbm))
    ]
    loads = [
        a_part(0),
        a_part(1) if A_PARTS == 2 else [],
        [(out_hbm, buf_b.at[me])],
        units_of(0, first_units, buf_e),
        [(down_hbm.at[pl.ds(0, first_units), :], buf_f.at[me])],
        units_of(first_units, other_units, buf_c),
        [(down_hbm.at[pl.ds(first_units, other_units), :], buf_d.at[me])],
        [(tok_hbm, tok), (shift_hbm, shift), (rate_hbm, rate_blocks), (inlet_hbm, inlet_blocks)],
    ]
    count = 0
    for group in loads:
        for at, (source, target) in enumerate(group):
            group[at] = pltpu.make_async_copy(source, target, load_sem.at[count])
            count += 1

    steps = ["recur"] * blocks + ["mix"] * parts + ["terms"] + ["norm"] * row_tiles + ["rows"] * row_tiles
    steps += ["first"] * first_tiles + ["far"] * parts + ["back"] * parts
    steps += ["hidden"] * other_tiles + ["down"] * parts
    begins = {name: steps.index(name) for name in dict.fromkeys(steps)}
    turn_of = [(0, 0), (0, 1), (1, 0), (2, 0), (1, 1), (3, 0), (2, 1), (3, 1)]
    needs = {begins["recur"]: 0, begins["mix"]: 2, begins["first"]: 3, begins["far"]: 4, begins["hidden"]: 5}
    if A_PARTS == 2:
        needs[begins["recur"] + blocks // 2] = 1
    packs_of = [[p for p, (w, _, _) in enumerate(PACKS) if w == weight] for weight in range(INPUTS)]

    def actions(plan, in_middle, second):
        loaded, waited, sends, gaps = set(), set(), [], []

        def load(weight, out):
            if weight not in loaded:
                loaded.add(weight)
                out.append(("load", weight))

        def arrive(pack, k, side, out):
            if (k, side) == (0, 0):
                load(PACKS[pack][0], out)
            elif (pack, k, side) not in waited:
                waited.add((pack, k, side))
                out.append(("arrive", pack, k, side))

        def send(pack, k, side, way, out):
            arrive(pack, k, side, out)
            out.append(("send", pack, k, side, way))
            sends.append((pack, k, side, way, len(gaps)))

        for step, codes in enumerate(plan):
            out = []
            for code in codes:
                kind, pack, k = code // 100, code // 10 % 10, code % 10
                first = PACKS[pack][0] in (3, 4)
                to_end, to_middle, from_end = (ALONG[pack][second] & bit for bit in (1, 2, 4))
                if kind == OWN:
                    if not (first and in_middle):
                        send(pack, 0, 0, LINE, out)
                    if in_middle:
                        send(pack, 0, 0, OTHER, out)
                elif kind == OWN_SIDE:
                    if not first or in_middle or from_end:
                        send(pack, 0, 0, SIDE, out)
                elif kind == FROM_SIDE:
                    if in_middle and to_end and not first:
                        send(pack, 0, 1, LINE, out)
                    if in_middle and to_middle:
                        send(pack, 0, 1, OTHER, out)
                    if not in_middle and from_end:
                        send(pack, 0, 1, LINE, out)
                    if not first or in_middle:
                        send(pack, 0, 1, CORE, out)
                elif first and not in_middle:
                    pass
                elif kind == FROM_LINE:
                    if in_middle and (k == 1 or not first):
                        send(pack, k, 0, OTHER if k == 1 else LINE, out)
                    send(pack, k, 0, CORE, out)
                elif kind == ON_SIDE:
                    comes_along = {1: from_end if in_middle else to_end, 2: in_middle and to_middle, 3: False}
                    if not comes_along[k]:
                        send(pack, k, 0, SIDE, out)
                else:
                    send(pack, k, 1, CORE, out)
            if step in needs:
                weight = needs[step]
                load(weight, out)
                if step == 0:
                    load(INPUTS, out)
                for pack in packs_of[weight] if in_middle or weight not in (3, 4) else []:
                    for turn in turn_of[1:]:
                        arrive(pack, *turn, out)
                        out.append(("handed", pack, *turn))
            if begins["down"] <= step:
                turn = turn_of[step - begins["down"]]
                for pack in packs_of[6]:
                    arrive(pack, *turn, out)
                    if turn != (0, 0):
                        out.append(("handed", pack, *turn))
            gaps.append(out)
        return gaps, sends

    programs = [actions(plan, at >= 2, at % 2) for at, plan in enumerate(PLANS)]

    def act(todo):
        for kind, *rest in todo:
            if kind == "load":
                for one in loads[rest[0]]:
                    one.wait()
                continue
            at = spots[rest[2]][rest[1]]
            if kind == "arrive":
                copy(rest[0], at, CORE).wait_recv()
            elif kind == "handed":
                copy(rest[0], at, CORE, 1 - core).wait_recv()
            elif kind == "send":
                copy(rest[0], at, rest[3]).start()
            else:
                copy(rest[0], at, rest[3]).wait_send()

    def ahead_of(step, index=None):
        for mine, (gaps, _) in zip(roles, programs):
            if gaps[step]:
                asked = mine if index is None else jnp.logical_and(mine, index == step - begins[steps[step]])
                pl.when(asked)(functools.partial(act, gaps[step]))

    def loop(name, length, body):
        def whole(index, _):
            for step in range(begins[name], begins[name] + length):
                ahead_of(step, index)
            body(index)

        lax.fori_loop(0, length, whole, None)

    drained = [set() for _ in programs]

    def drain(weights, before):
        for mine, (_, sends), gone in zip(roles, programs, drained):
            now = [one for one in sends if PACKS[one[0]][0] in weights and one[-1] < before and one not in gone]
            gone.update(now)
            pl.when(mine)(functools.partial(act, [("sent", *one) for one in now]))

    for group in loads:
        for one in group:
            one.start()
    barrier = pltpu.get_barrier_semaphore()
    for target in [targets[LINE], targets[SIDE], targets[CORE], across]:
        pl.semaphore_signal(barrier, inc=1, device_id=target, device_id_type=MESH)

    @pl.when(middle)
    def _():
        pl.semaphore_signal(barrier, inc=1, device_id=targets[OTHER], device_id_type=MESH)

    pl.semaphore_wait(barrier, 4 + z * (3 - z) // 2)

    def recur_step(i):
        cols = pl.ds(pl.multiple_of(i * block, block), block)
        part, place = (i * block) // a_columns, pl.ds(pl.multiple_of(i * block % a_columns, block), block)
        value_in = jnp.dot(tok[...], buf_a[part, 0, :, place], preferred_element_type=jnp.float32)
        gate_in = jnp.dot(tok[...], buf_a[part, 1, :, place], preferred_element_type=jnp.float32)
        param = -param_ref[:, cols]
        plus = jnp.maximum(param, 0.0) + jnp.log1p(jnp.exp(-jnp.abs(param)))
        branch[:, cols] = recur_core(
            value_in, gate_in, taps_ref[:, cols], rate_blocks[i], inlet_blocks[i], plus, shift[:, cols]
        )

    loop("recur", blocks, recur_step)

    def terms_copy(phase, at):
        return pltpu.make_async_remote_copy(
            src_ref=terms.at[1 - tp, at],
            dst_ref=came.at[phase % 2, at],
            send_sem=terms_send.at[phase, at],
            recv_sem=terms_recv.at[phase, at],
            device_id=across,
            device_id_type=MESH,
        )

    def keep(product, at):
        product = product.astype(jnp.bfloat16)
        for row in range(2):
            terms[row, at] = product[row * share : (row + 1) * share]

    def mix_step(s):
        keep(jnp.dot(branch[...], buf_b[s], preferred_element_type=jnp.float32), s)
        pl.when(s > 0)(lambda: terms_copy(0, s - 1).start())

    loop("mix", parts, mix_step)
    drain([0, 1], begins["recur"] + 1)
    terms_copy(0, parts - 1).start()
    ahead_of(begins["terms"])
    for s in range(parts):
        terms_copy(0, s).wait_recv()

    def norm_rows(i, phase, residual, gain_ref):
        here = pl.ds(pl.multiple_of(i * rows, rows), rows)

        def total(s):
            value = terms[tp, s, here, :].astype(jnp.float32) + came[phase, s, here, :].astype(jnp.float32)
            return value if phase == 0 else value + jnp.where(outer, came[0, s, here, :].astype(jnp.float32), 0.0)

        value = jnp.concatenate([total(s) for s in range(parts)], axis=1)
        return layer_norm(residual_scale * residual.astype(jnp.float32) + value, gain_ref[...]).astype(jnp.bfloat16)

    def own_rows(i):
        return pl.ds(pl.multiple_of(own_row + i * rows, rows), rows)

    def norm_copy(i):
        return pltpu.make_async_remote_copy(
            src_ref=normed.at[own_rows(i), :],
            dst_ref=normed.at[own_rows(i), :],
            send_sem=norm_send.at[i],
            recv_sem=norm_recv.at[i],
            device_id=across,
            device_id_type=MESH,
        )

    def far_copy(half, i):
        here = pl.ds(pl.multiple_of(half * share + i * rows, rows), rows)
        return pltpu.make_async_remote_copy(
            src_ref=normed.at[here, :],
            dst_ref=tok.at[here, :],
            send_sem=far_send.at[half, i],
            recv_sem=far_recv.at[half, i],
            device_id=targets[LINE],
            device_id_type=MESH,
        )

    def pass_on(i):
        norm_copy(i).start()
        pl.when(outer)(lambda: far_copy(tp, i).start())

    def first_norm(i):
        normed[own_rows(i), :] = norm_rows(i, 0, tok[own_rows(i), :], first_gain_ref)
        pl.when(jnp.logical_and(outer, i == 1))(lambda: pl.semaphore_wait(free_sem, 1))
        pl.when(i > 0)(lambda: pass_on(i - 1))

    loop("norm", row_tiles, first_norm)
    drain([2], begins["terms"])
    for s in range(parts):
        terms_copy(0, s).wait_send()

    @pl.when(middle)
    def _():
        pl.semaphore_signal(free_sem, inc=1, device_id=targets[LINE], device_id_type=MESH)

    pass_on(row_tiles - 1)
    for i in range(row_tiles):
        ahead_of(begins["rows"] + i)
        norm_copy(i).wait_recv()
        pl.when(outer)(lambda i=i: far_copy(1 - tp, i).start())

    def units_at(left, buf, j):
        cols = pl.ds(pl.multiple_of(j * tile, tile), tile)
        gate = jnp.dot(left[...], buf[0, :, cols], preferred_element_type=jnp.float32)
        upward = jnp.dot(left[...], buf[1, :, cols], preferred_element_type=jnp.float32)
        return (gate * sigmoid(gate) * upward).astype(jnp.bfloat16)

    def in_middle(body):
        def asked(i):
            pl.when(middle)(lambda: body(i))

        return asked

    def first_step(j):
        @pl.when(j == 0)
        def _():
            for half in range(2):
                for i in range(row_tiles):
                    far_copy(half, i).wait_recv()

        to = pl.ds(pl.multiple_of(j * tile, tile), tile)
        hidden[:, to] = units_at(normed, buf_e, j)
        branch[:, to] = units_at(tok, buf_e, j)

    def far_step(s):
        left = branch[:, :first_units]
        keep(jnp.dot(left, buf_f[s], preferred_element_type=jnp.float32), s)
        pl.when(s > 0)(lambda: terms_copy(2, s - 1).start())

    def back_copy(s):
        return pltpu.make_async_remote_copy(
            src_ref=came.at[0, s],
            dst_ref=came.at[0, s],
            send_sem=back_send.at[s],
            recv_sem=back_recv.at[s],
            device_id=targets[LINE],
            device_id_type=MESH,
        )

    def back_step(s):
        pl.when(s == 0)(lambda: terms_copy(2, parts - 1).start())
        terms_copy(2, s).wait_recv()
        came[0, s] = (terms[tp, s].astype(jnp.float32) + came[0, s].astype(jnp.float32)).astype(jnp.bfloat16)
        pl.when(s > 0)(lambda: back_copy(s - 1).start())

    loop("first", first_tiles, in_middle(first_step))
    loop("far", parts, in_middle(far_step))
    loop("back", parts, in_middle(back_step))

    @pl.when(middle)
    def _():
        for s in range(parts):
            terms_copy(2, s).wait_send()
        back_copy(parts - 1).start()

    def hidden_step(j):
        to = pl.ds(pl.multiple_of(first_units + j * tile, tile), tile)
        hidden[:, to] = units_at(normed, buf_c, j)

    loop("hidden", other_tiles, hidden_step)

    order = [spots[side][k] for k, side in turn_of]

    def pick(j):
        at = order[0]
        for turn in range(1, parts):
            at = jnp.where(j == turn, order[turn], at)
        return at

    def down_step(j):
        at = pick(j)
        product = lambda: jnp.dot(hidden[:, first_units:], buf_d[at], preferred_element_type=jnp.float32)
        more = lambda: jnp.dot(hidden[:, :first_units], buf_f[at], preferred_element_type=jnp.float32)
        pl.when(outer)(lambda: keep(product(), at))
        pl.when(middle)(lambda: keep(product() + more(), at))
        pl.when(j > 0)(lambda: terms_copy(1, pick(j - 1)).start())

    loop("down", parts, down_step)
    drain(range(5), len(steps))
    terms_copy(1, order[-1]).start()
    drain(range(INPUTS), len(steps))
    for i in range(row_tiles):
        norm_copy(i).wait_send()

    @pl.when(outer)
    def _():
        for half in range(2):
            for i in range(row_tiles):
                far_copy(half, i).wait_send()
        for s in range(parts):
            back_copy(s).wait_recv()

    @pl.when(middle)
    def _():
        for s in range(parts):
            back_copy(s).wait_send()

    for s in order:
        terms_copy(1, s).wait_recv()

    def second_norm(i, _):
        here = pl.ds(pl.multiple_of(i * rows, rows), rows)
        out_ref[here, :] = norm_rows(i, 1, normed[own_rows(i), :], second_gain_ref)

    lax.fori_loop(0, row_tiles, second_norm, None)
    for s in range(parts):
        terms_copy(1, s).wait_send()


def whole_layer(
    tokens,
    recurrence_branch_weight,
    gate_branch_weight,
    convolution_kernel,
    recurrence_gate_blockwise,
    input_gate_blockwise,
    channel_decay_param,
    token_decay_shift,
    recurrence_output_weight,
    first_norm_gain,
    feedforward_gate_weight,
    feedforward_up_weight,
    feedforward_down_weight,
    second_norm_gain,
):
    length, model = tokens.shape
    parts = lax.axis_size("fs")
    share = length // lax.axis_size("tp")
    depth, channels = recurrence_branch_weight.shape
    units = feedforward_gate_weight.shape[1]
    first_units = units * 2 // 5 // 256 * 256
    columns = recurrence_output_weight.shape[1]
    hbm = pl.BlockSpec(memory_space=pl.ANY)
    vmem = pl.BlockSpec(memory_space=pltpu.VMEM)
    half = jnp.bfloat16
    packs = len(PACKS)
    row_tiles = share // min(64, share)
    return pl.pallas_call(
        layer_kernel,
        in_specs=[hbm, hbm, hbm, vmem, hbm, hbm, vmem, hbm, hbm, vmem, hbm, hbm, hbm, vmem],
        out_specs=vmem,
        out_shape=jax.ShapeDtypeStruct((share, model), half),
        scratch_shapes=[
            pltpu.VMEM((A_PARTS, 2, depth * parts, channels // A_PARTS), half),
            pltpu.VMEM((parts, channels, columns), half),
            pltpu.VMEM((2, depth * parts, first_units), half),
            pltpu.VMEM((parts, first_units, columns), half),
            pltpu.VMEM((2, depth * parts, units - first_units), half),
            pltpu.VMEM((parts, units - first_units, columns), half),
            pltpu.VMEM((length, model), half),
            pltpu.VMEM(recurrence_gate_blockwise.shape, half),
            pltpu.VMEM(input_gate_blockwise.shape, half),
            pltpu.VMEM((length, channels), jnp.float32),
            pltpu.VMEM((length, channels), half),
            pltpu.VMEM((2, parts, share, columns), half),
            pltpu.VMEM((2, parts, share, columns), half),
            pltpu.VMEM((length, model), half),
            pltpu.VMEM((length, units), half),
            pltpu.SemaphoreType.DMA((15,)),
            pltpu.SemaphoreType.DMA((packs, parts, 4)),
            pltpu.SemaphoreType.DMA((packs, 2, parts)),
            pltpu.SemaphoreType.DMA((3, parts)),
            pltpu.SemaphoreType.DMA((3, parts)),
            pltpu.SemaphoreType.DMA((row_tiles,)),
            pltpu.SemaphoreType.DMA((row_tiles,)),
            pltpu.SemaphoreType.DMA((2, row_tiles)),
            pltpu.SemaphoreType.DMA((2, row_tiles)),
            pltpu.SemaphoreType.DMA((parts,)),
            pltpu.SemaphoreType.DMA((parts,)),
            pltpu.SemaphoreType.REGULAR,
        ],
        cost_estimate=pl.CostEstimate(
            flops=2 * length * model * (2 * channels + 2 * units) + 2 * length * model * (channels + units),
            bytes_accessed=2 * model * (3 * channels + 3 * units),
            transcendentals=0,
        ),
        compiler_params=pltpu.CompilerParams(
            vmem_limit_bytes=LAYER_VMEM_BYTES, collective_id=0, has_side_effects=True
        ),
    )(
        tokens,
        recurrence_branch_weight,
        gate_branch_weight,
        convolution_kernel,
        recurrence_gate_blockwise,
        input_gate_blockwise,
        channel_decay_param[None, :],
        token_decay_shift,
        recurrence_output_weight,
        first_norm_gain[None, :],
        feedforward_gate_weight,
        feedforward_up_weight,
        feedforward_down_weight,
        second_norm_gain[None, :],
    )


def recurrence_kernel(count, meta, x_ref, taps_ref, rate_ref, inlet_ref, plus_ref, shift_ref, *refs):
    mine, other, out_ref = refs[:count], refs[count : 2 * count], refs[-1]
    first = split_product(meta, x_ref, mine)
    second = split_product(meta, x_ref, other)
    out_ref[...] = recur_core(
        first, second, taps_ref[...], rate_ref[0], inlet_ref[0], plus_ref[...], shift_ref[...]
    )


def recurrence(tokens, mine, other, meta, taps, rate_blocks, inlet_blocks, plus, shift):
    length, width = tokens.shape
    block = rate_blocks.shape[1]
    blocks = rate_blocks.shape[0]
    parts = [pl.BlockSpec((p.shape[0], block), lambda i: (0, i)) for p in [*mine, *other]]
    column = lambda rows: pl.BlockSpec((rows, block), lambda i: (0, i))
    square = pl.BlockSpec((1, block, block), lambda i: (i, 0, 0))
    return pl.pallas_call(
        functools.partial(recurrence_kernel, len(mine)),
        grid=(blocks,),
        in_specs=[
            pl.BlockSpec(memory_space=pltpu.SMEM),
            pl.BlockSpec((length, width), lambda i: (0, 0)),
            column(taps.shape[0]),
            square,
            square,
            column(1),
            column(length),
            *parts,
        ],
        out_specs=column(length),
        out_shape=jax.ShapeDtypeStruct((length, block * blocks), jnp.bfloat16),
        cost_estimate=pl.CostEstimate(
            flops=4 * length * width * block * blocks,
            bytes_accessed=4 * width * block * blocks + 8 * length * block * blocks,
            transcendentals=0,
        ),
        compiler_params=pltpu.CompilerParams(vmem_limit_bytes=VMEM_BYTES),
    )(meta, tokens, taps, rate_blocks, inlet_blocks, plus, shift, *mine, *other)


def hidden_kernel(count, meta, x_ref, *refs):
    mine, other, out_ref = refs[:count], refs[count : 2 * count], refs[-1]
    first = split_product(meta, x_ref, mine)
    second = split_product(meta, x_ref, other)
    swapped = meta[0] == 1
    gate = jnp.where(swapped, second, first)
    upward = jnp.where(swapped, first, second)
    out_ref[...] = (gate * sigmoid(gate) * upward).astype(jnp.bfloat16)


def hidden_units(normed, mine, other, meta):
    length, width = normed.shape
    units = mine[0].shape[1]
    tile = next(t for t in (512, 640, 256, 128, units) if units % t == 0)
    return pl.pallas_call(
        functools.partial(hidden_kernel, len(mine)),
        grid=(units // tile,),
        in_specs=[
            pl.BlockSpec(memory_space=pltpu.SMEM),
            pl.BlockSpec((length, width), lambda i: (0, 0)),
            *[pl.BlockSpec((p.shape[0], tile), lambda i: (0, i)) for p in [*mine, *other]],
        ],
        out_specs=pl.BlockSpec((length, tile), lambda i: (0, i)),
        out_shape=jax.ShapeDtypeStruct((length, units), jnp.bfloat16),
        cost_estimate=pl.CostEstimate(
            flops=4 * length * width * units, bytes_accessed=4 * width * units, transcendentals=0
        ),
        compiler_params=pltpu.CompilerParams(vmem_limit_bytes=VMEM_BYTES),
    )(meta, normed, *mine, *other)


def outward_kernel(count, meta, left_ref, *refs):
    mine, other, out_ref = refs[:count], refs[count : 2 * count], refs[-1]
    half = mine[0].shape[0]
    near = pl.ds(pl.multiple_of(meta[0] * half, 128), half)
    far = pl.ds(pl.multiple_of((1 - meta[0]) * half, 128), half)
    start = 0
    for at in range(count):
        total = jnp.dot(left_ref[:, near], mine[at][...], preferred_element_type=jnp.float32)
        total += jnp.dot(left_ref[:, far], other[at][...], preferred_element_type=jnp.float32)
        columns = mine[at].shape[1]
        out_ref[:, start : start + columns] = total.astype(jnp.bfloat16)
        start += columns


def outward(left, mine, other, meta):
    length, depth = left.shape
    width = sum(p.shape[1] for p in mine)
    rows = min(length, 256)
    whole = [pl.BlockSpec(p.shape, lambda i: (0, 0)) for p in [*mine, *other]]
    return pl.pallas_call(
        functools.partial(outward_kernel, len(mine)),
        grid=(length // rows,),
        in_specs=[
            pl.BlockSpec(memory_space=pltpu.SMEM),
            pl.BlockSpec((rows, depth), lambda i: (i, 0)),
            *whole,
        ],
        out_specs=pl.BlockSpec((rows, width), lambda i: (i, 0)),
        out_shape=jax.ShapeDtypeStruct((length, width), jnp.bfloat16),
        cost_estimate=pl.CostEstimate(
            flops=2 * length * width * depth, bytes_accessed=2 * width * depth, transcendentals=0
        ),
        compiler_params=pltpu.CompilerParams(vmem_limit_bytes=VMEM_BYTES),
    )(meta, left, *mine, *other)


def gathered_layer(
    tokens,
    recurrence_branch_weight,
    gate_branch_weight,
    convolution_kernel,
    recurrence_gate_blockwise,
    input_gate_blockwise,
    channel_decay_param,
    token_decay_shift,
    recurrence_output_weight,
    first_norm_gain,
    feedforward_gate_weight,
    feedforward_up_weight,
    feedforward_down_weight,
    second_norm_gain,
):
    share = tokens.shape[0] // lax.axis_size("tp")
    offset = lax.axis_index("tp") * share
    rows_of = lambda weight: [lax.all_gather(weight, "fs", axis=0, tiled=True)]

    def halves_of(weight):
        half = weight.shape[0] // 2
        return [[lax.all_gather(part, "fs", axis=1, tiled=True)] for part in (weight[:half], weight[half:])]

    meta = scalars([jnp.int32(0)], jnp.int32(0))
    branch = recurrence(
        tokens,
        rows_of(recurrence_branch_weight),
        rows_of(gate_branch_weight),
        meta,
        convolution_kernel,
        recurrence_gate_blockwise,
        input_gate_blockwise,
        jax.nn.softplus(-channel_decay_param)[None, :],
        token_decay_shift,
    )

    def grouped(left, weight):
        terms = outward(left, *halves_of(weight), meta)
        return lax.psum_scatter(terms, "tp", scatter_dimension=0, tiled=True).astype(jnp.float32)

    mix = grouped(branch, recurrence_output_weight)
    own_tokens = lax.dynamic_slice_in_dim(tokens, offset, share, 0)
    normed = layer_norm(
        residual_scale * own_tokens.astype(jnp.float32) + mix, first_norm_gain
    ).astype(jnp.bfloat16)
    rows = lax.all_gather(normed, "tp", axis=0, tiled=True)
    hidden = hidden_units(rows, rows_of(feedforward_gate_weight), rows_of(feedforward_up_weight), meta)
    ffn = grouped(hidden, feedforward_down_weight)
    return layer_norm(residual_scale * normed.astype(jnp.float32) + ffn, second_norm_gain).astype(
        jnp.bfloat16
    )


def solution(mesh):
    sizes = mesh.shape
    one_kernel = sizes["rep"] == 2 and sizes["tp"] == 2 and sizes["fs"] == 8
    return jax.shard_map(
        whole_layer if one_kernel else gathered_layer,
        mesh=mesh,
        in_specs=(
            P(("rep", "fs"), None),
            P("fs", "tp"),
            P("fs", "tp"),
            P(None, "tp"),
            P("tp", None, None),
            P("tp", None, None),
            P("tp"),
            P(("rep", "fs"), "tp"),
            P("tp", "fs"),
            P(),
            P("fs", "tp"),
            P("fs", "tp"),
            P("tp", "fs"),
            P(),
        ),
        out_specs=P(("rep", "fs", "tp"), None),
        check_vma=False,
    )
```

```python
import functools

import jax
import jax.numpy as jnp
from jax import lax
from jax.experimental import pallas as pl
from jax.experimental.pallas import tpu as pltpu
from jax.sharding import PartitionSpec as P

residual_scale = 1.4142135623730951

VMEM_BYTES = 60 * 1024 * 1024
LAYER_VMEM_BYTES = 67043328
MESH = pl.DeviceIdType.MESH


def layer_norm(values, gain):
    center = values - jnp.mean(values, axis=-1, keepdims=True)
    variance = jnp.mean(center * center, axis=-1, keepdims=True)
    return center * lax.rsqrt(variance + 1e-05) * gain


def scalars(owners, swapped):
    return jnp.stack([jnp.asarray(v, jnp.int32) for v in [swapped, *owners]])


def split_product(meta, left_ref, part_refs):
    total = None
    for at, part in enumerate(part_refs):
        depth = part.shape[0]
        columns = pl.ds(pl.multiple_of(meta[1 + at] * depth, depth), depth)
        term = jnp.dot(left_ref[:, columns], part[...], preferred_element_type=jnp.float32)
        total = term if total is None else total + term
    return total


def shifted(values, step, fill):
    rows = lax.broadcasted_iota(jnp.int32, values.shape, 0)
    return jnp.where(rows < step, fill, pltpu.roll(values, step, 0))


def sigmoid(values):
    return 1.0 / (1.0 + jnp.exp(-values))


def recur_core(value_in, gate_in, taps, rate_block, inlet_block, plus, shift):
    value_in = value_in.astype(jnp.bfloat16).astype(jnp.float32)
    gate_in = gate_in.astype(jnp.bfloat16).astype(jnp.float32)
    taps = taps.astype(jnp.float32)
    depth = taps.shape[0]
    conv = None
    for tap in range(depth):
        lag = depth - 1 - tap
        moved = value_in if lag == 0 else shifted(value_in, lag, 0.0)
        term = moved * taps[tap : tap + 1, :]
        conv = term if conv is None else conv + term
    conv = conv.astype(jnp.bfloat16)
    rate = sigmoid(jnp.dot(conv, rate_block, preferred_element_type=jnp.float32))
    inlet = sigmoid(jnp.dot(conv, inlet_block, preferred_element_type=jnp.float32))
    log_decay = -8.0 * rate * plus + shift
    decay = jnp.exp(log_decay)
    twice = 2.0 * log_decay
    series = jnp.ones_like(twice)
    for order in range(8, 1, -1):
        series = 1.0 + twice * series * (1.0 / order)
    lost = jnp.where(twice > -0.3, -twice * series, 1.0 - jnp.exp(twice))
    state = jnp.sqrt(lost) * inlet * conv.astype(jnp.float32)
    step = 1
    while step < state.shape[0]:
        state = state + decay * shifted(state, step, 0.0)
        if 2 * step < state.shape[0]:
            decay = decay * shifted(decay, step, 1.0)
        step *= 2
    gelu = 0.5 * gate_in * (
        1.0 + jnp.tanh(0.7978845608028654 * (gate_in + 0.044715 * gate_in * gate_in * gate_in))
    )
    return (state * gelu).astype(jnp.bfloat16)


LINE, OTHER, SIDE, CORE = 0, 1, 2, 3
INPUTS = 7
OWN, OWN_SIDE, FROM_SIDE, FROM_LINE, ON_SIDE, FROM_FAR_SIDE = range(6)
A_PARTS = 1
PACKS = ((0, 0, 1), (2, 0, 1), (3, 0, 1), (4, 0, 1), (5, 0, 1), (6, 0, 2), (6, 1, 2))
ALONG = ((4, 5), (7, 7), (0, 1), (2, 3), (6, 7), (6, 3), (6, 3))
PLANS = (
    (

        (100, 0, 130, 110, 120, 301, 10, 200, 402, 433, 302, 210, 20, 30, 511, 401, 50, 403, 311, 501, 502, 503, 303, 423, 322, 40, 413),
        (513, 412, 140, 323), (312, 313, 512), (160, 240), (), (), (), (), (), (), (533, 432, 332, 441), (), (),
        (150,), (421,), (), (), (), (341, 342), (442, 541, 521), (), (351, 443, 343, 451), (532, 260), (), (),
        (352,), (250,), (), (), (), (453, 542, 361, 461), (452, 60), (220, 462), (543, 353), (331,), (561,), (),
        (531,), (333, 230), (), (), (562, 553), (), (463, 362), (), (), (431,), (552, 411, 551), (523, 363, 563), (),
        (321,), (), (422,), (), (522,),
    ),
    (
        (10, 140, 120, 110, 100, 0, 20, 433, 210, 302, 402, 200, 30, 403, 502, 40, 301, 303, 501, 413, 503),
        (240, 412, 50, 311, 423), (), (), (), (323, 401, 312, 130, 322), (512,), (), (511, 160, 313), (), (),
        (533, 532, 432, 260, 332, 60, 513), (), (442,), (), (), (), (), (341, 521, 351, 150, 421), (), (), (),
        (343,), (443, 543), (), (), (342,), (), (352, 441), (), (), (), (361,), (461, 542, 541, 451, 220), (462,),
        (353, 452, 531, 331), (453,), (), (561,), (), (), (230, 333, 362), (), (463,), (), (411,), (), (),
        (431, 553, 562), (552,), (), (551, 523), (), (563,), (321, 422, 363, 250, 522),
    ),
    (

        (0, 110, 301, 302, 402, 311, 462, 100, 10, 210, 502, 403, 20, 130, 303, 501, 200, 413, 442, 503, 452, 512, 421, 120, 313, 513, 422, 511, 312, 331),
        (), (), (), (), (322,), (522,), (), (140,), (), (220, 40, 321, 351, 341), (60,), (431, 432), (50, 240),
        (423,), (), (353,), (412, 433, 333, 323), (541, 342), (), (343, 523, 521, 230, 533),
        (443, 542, 401, 30, 352, 362, 332, 160, 531, 532), (543,), (461,), (361,), (), (453, 561), (150,),
        (463, 363, 551), (), (), (), (), (), (260, 441, 250), (), (), (563, 553, 552, 562, 411), (), (), (), (), (),
        (), (), (), (), (), (), (), (), (), (), (451,), (),
    ),
    (
        (10, 0, 100, 110, 462, 130, 311, 402, 302, 301, 403, 313, 303, 442, 20, 200, 502, 413, 230, 312, 60),
        (503, 513, 511, 331, 210, 40), (501, 431), (), (512, 321), (), (140,), (432, 532), (421,), (120, 342),
        (341, 531), (), (422, 541), (50, 333), (362, 323), (), (), (343,), (412, 322, 401, 352, 522, 423, 433),
        (523,), (), (361,), (160,), (443, 30, 220, 521), (351, 533, 240), (), (), (461,), (), (332,), (),
        (260, 353, 150), (363,), (), (543,), (542,), (), (250,), (), (), (), (), (552,), (453,), (), (), (), (), (),
        (451, 562, 441, 553), (463,), (), (411,), (), (452, 563, 551, 561),
    ),
)


def layer_kernel(
    tok_hbm,
    in_hbm,
    gate_hbm,
    taps_ref,
    rate_hbm,
    inlet_hbm,
    param_ref,
    shift_hbm,
    out_hbm,
    first_gain_ref,
    ffgate_hbm,
    ffup_hbm,
    down_hbm,
    second_gain_ref,
    out_ref,
    buf_a,
    buf_b,
    buf_e,
    buf_f,
    buf_c,
    buf_d,
    tok,
    rate_blocks,
    inlet_blocks,
    shift,
    branch,
    terms,
    came,
    normed,
    hidden,
    load_sem,
    send_sem,
    recv_sem,
    terms_send,
    terms_recv,
    norm_send,
    norm_recv,
    far_send,
    far_recv,
    back_send,
    back_recv,
    free_sem,
):
    core, fs, tp = lax.axis_index("rep"), lax.axis_index("fs"), lax.axis_index("tp")
    z, y = fs // 2, fs % 2
    zs = [z, z + 1 - 2 * (z % 2), 2 - z // 2, 3 - 3 * (z // 2)]
    middle = z * (3 - z) == 2
    role = core + z * (3 - z)
    roles = [role == at for at in range(4)]
    outer = jnp.logical_not(middle)
    spots = [[k * 2 + y for k in zs], [k * 2 + 1 - y for k in zs]]
    me = spots[0][0]
    targets = {
        LINE: (core, spots[0][1], tp),
        OTHER: (core, (3 - z) * 2 + y, tp),
        SIDE: (core, spots[1][0], tp),
        CORE: (1 - core, me, tp),
    }
    across = (core, me, 1 - tp)
    width = in_hbm.shape[0]
    parts = buf_b.shape[0]
    first_units, other_units = buf_e.shape[2], buf_c.shape[2]
    a_columns = buf_a.shape[3]
    mix_depth = buf_b.shape[1]
    share = out_ref.shape[0]
    block = rate_blocks.shape[1]
    blocks = rate_blocks.shape[0]
    tile = min(256, first_units)
    first_tiles, other_tiles = first_units // tile, other_units // tile
    rows = min(64, share)
    row_tiles = share // rows
    own_row = pl.multiple_of(tp * share, share)

    def run_of(base, part, count):
        return pl.ds(pl.multiple_of(base + part * count, count), count)

    def piece(pack, at, half):
        weight, part, count = PACKS[pack]
        by_row = run_of(at * width, part, width // count)
        by_depth = lambda depth: run_of(half * (depth // 2), part, depth // 2 // count)
        if weight < 2:
            return buf_a.at[weight, half, by_row, :]
        if weight == 2:
            return buf_b.at[at, by_depth(mix_depth), :]
        if weight == 3:
            return buf_e.at[half, by_row, :]
        if weight == 4:
            return buf_f.at[at, by_depth(first_units), :]
        if weight == 5:
            return buf_c.at[half, by_row, :]
        return buf_d.at[at, by_depth(other_units), :]

    def copy(pack, at, way, half=core):
        return pltpu.make_async_remote_copy(
            src_ref=piece(pack, at, half),
            dst_ref=piece(pack, at, half),
            send_sem=send_sem.at[pack, at, way],
            recv_sem=recv_sem.at[pack, half, at],
            device_id=targets[way],
            device_id_type=MESH,
        )

    own_rows_of = lambda ref, *at: ref.at[(*at, pl.ds(pl.multiple_of(me * width, width), width), slice(None))]
    a_part = lambda part: [
        (ref.at[:, pl.ds(part * a_columns, a_columns)], own_rows_of(buf_a, part, half))
        for half, ref in enumerate((in_hbm, gate_hbm))
    ]
    units_of = lambda start, count, buf: [
        (ref.at[:, pl.ds(start, count)], own_rows_of(buf, half)) for half, ref in enumerate((ffgate_hbm, ffup_hbm))
    ]
    loads = [
        a_part(0),
        a_part(1) if A_PARTS == 2 else [],
        [(out_hbm, buf_b.at[me])],
        units_of(0, first_units, buf_e),
        [(down_hbm.at[pl.ds(0, first_units), :], buf_f.at[me])],
        units_of(first_units, other_units, buf_c),
        [(down_hbm.at[pl.ds(first_units, other_units), :], buf_d.at[me])],
        [(tok_hbm, tok), (shift_hbm, shift), (rate_hbm, rate_blocks), (inlet_hbm, inlet_blocks)],
    ]
    count = 0
    for group in loads:
        for at, (source, target) in enumerate(group):
            group[at] = pltpu.make_async_copy(source, target, load_sem.at[count])
            count += 1

    steps = ["recur"] * blocks + ["mix"] * parts + ["terms"] + ["norm"] * row_tiles + ["rows"] * row_tiles
    steps += ["first"] * first_tiles + ["far"] * parts + ["hidden"] * other_tiles
    steps += ["back"] * parts + ["down"] * parts
    begins = {name: steps.index(name) for name in dict.fromkeys(steps)}
    turn_of = [(0, 0), (0, 1), (1, 0), (2, 0), (1, 1), (3, 0), (2, 1), (3, 1)]
    needs = {begins["recur"]: 0, begins["mix"]: 2, begins["first"]: 3, begins["far"]: 4, begins["hidden"]: 5}
    if A_PARTS == 2:
        needs[begins["recur"] + blocks // 2] = 1
    packs_of = [[p for p, (w, _, _) in enumerate(PACKS) if w == weight] for weight in range(INPUTS)]

    def actions(plan, in_middle, second):
        loaded, waited, sends, gaps = set(), set(), [], []

        def load(weight, out):
            if weight not in loaded:
                loaded.add(weight)
                out.append(("load", weight))

        def arrive(pack, k, side, out):
            if (k, side) == (0, 0):
                load(PACKS[pack][0], out)
            elif (pack, k, side) not in waited:
                waited.add((pack, k, side))
                out.append(("arrive", pack, k, side))

        def send(pack, k, side, way, out):
            arrive(pack, k, side, out)
            out.append(("send", pack, k, side, way))
            sends.append((pack, k, side, way, len(gaps)))

        for step, codes in enumerate(plan):
            out = []
            for code in codes:
                kind, pack, k = code // 100, code // 10 % 10, code % 10
                first = PACKS[pack][0] in (3, 4)
                to_end, to_middle, from_end = (ALONG[pack][second] & bit for bit in (1, 2, 4))
                if kind == OWN:
                    if not (first and in_middle):
                        send(pack, 0, 0, LINE, out)
                    if in_middle:
                        send(pack, 0, 0, OTHER, out)
                elif kind == OWN_SIDE:
                    if not first or in_middle or from_end:
                        send(pack, 0, 0, SIDE, out)
                elif kind == FROM_SIDE:
                    if in_middle and to_end and not first:
                        send(pack, 0, 1, LINE, out)
                    if in_middle and to_middle:
                        send(pack, 0, 1, OTHER, out)
                    if not in_middle and from_end:
                        send(pack, 0, 1, LINE, out)
                    if not first or in_middle:
                        send(pack, 0, 1, CORE, out)
                elif first and not in_middle:
                    pass
                elif kind == FROM_LINE:
                    if in_middle and (k == 1 or not first):
                        send(pack, k, 0, OTHER if k == 1 else LINE, out)
                    send(pack, k, 0, CORE, out)
                elif kind == ON_SIDE:
                    comes_along = {1: from_end if in_middle else to_end, 2: in_middle and to_middle, 3: False}
                    if not comes_along[k]:
                        send(pack, k, 0, SIDE, out)
                else:
                    send(pack, k, 1, CORE, out)
            if step in needs:
                weight = needs[step]
                load(weight, out)
                if step == 0:
                    load(INPUTS, out)
                for pack in packs_of[weight] if in_middle or weight not in (3, 4) else []:
                    for turn in turn_of[1:]:
                        arrive(pack, *turn, out)
                        out.append(("handed", pack, *turn))
            if begins["down"] <= step:
                turn = turn_of[step - begins["down"]]
                for pack in packs_of[6]:
                    arrive(pack, *turn, out)
                    if turn != (0, 0):
                        out.append(("handed", pack, *turn))
            gaps.append(out)
        return gaps, sends

    programs = [actions(plan, at >= 2, at % 2) for at, plan in enumerate(PLANS)]

    def act(todo):
        for kind, *rest in todo:
            if kind == "load":
                for one in loads[rest[0]]:
                    one.wait()
                continue
            at = spots[rest[2]][rest[1]]
            if kind == "arrive":
                copy(rest[0], at, CORE).wait_recv()
            elif kind == "handed":
                copy(rest[0], at, CORE, 1 - core).wait_recv()
            elif kind == "send":
                copy(rest[0], at, rest[3]).start()
            else:
                copy(rest[0], at, rest[3]).wait_send()

    def ahead_of(step, index=None):
        for mine, (gaps, _) in zip(roles, programs):
            if gaps[step]:
                asked = mine if index is None else jnp.logical_and(mine, index == step - begins[steps[step]])
                pl.when(asked)(functools.partial(act, gaps[step]))

    def loop(name, length, body):
        def whole(index, _):
            for step in range(begins[name], begins[name] + length):
                ahead_of(step, index)
            body(index)

        lax.fori_loop(0, length, whole, None)

    drained = [set() for _ in programs]

    def drain(weights, before):
        for mine, (_, sends), gone in zip(roles, programs, drained):
            now = [one for one in sends if PACKS[one[0]][0] in weights and one[-1] < before and one not in gone]
            gone.update(now)
            pl.when(mine)(functools.partial(act, [("sent", *one) for one in now]))

    for group in loads:
        for one in group:
            one.start()
    barrier = pltpu.get_barrier_semaphore()
    for target in [targets[LINE], targets[SIDE], targets[CORE], across]:
        pl.semaphore_signal(barrier, inc=1, device_id=target, device_id_type=MESH)

    @pl.when(middle)
    def _():
        pl.semaphore_signal(barrier, inc=1, device_id=targets[OTHER], device_id_type=MESH)

    pl.semaphore_wait(barrier, 4 + z * (3 - z) // 2)

    def recur_step(i):
        cols = pl.ds(pl.multiple_of(i * block, block), block)
        part, place = (i * block) // a_columns, pl.ds(pl.multiple_of(i * block % a_columns, block), block)
        value_in = jnp.dot(tok[...], buf_a[part, 0, :, place], preferred_element_type=jnp.float32)
        gate_in = jnp.dot(tok[...], buf_a[part, 1, :, place], preferred_element_type=jnp.float32)
        param = -param_ref[:, cols]
        plus = jnp.maximum(param, 0.0) + jnp.log1p(jnp.exp(-jnp.abs(param)))
        branch[:, cols] = recur_core(
            value_in, gate_in, taps_ref[:, cols], rate_blocks[i], inlet_blocks[i], plus, shift[:, cols]
        )

    loop("recur", blocks, recur_step)

    def terms_copy(phase, at):
        return pltpu.make_async_remote_copy(
            src_ref=terms.at[1 - tp, at],
            dst_ref=came.at[phase % 2, at],
            send_sem=terms_send.at[phase, at],
            recv_sem=terms_recv.at[phase, at],
            device_id=across,
            device_id_type=MESH,
        )

    def keep(product, at):
        product = product.astype(jnp.bfloat16)
        for row in range(2):
            terms[row, at] = product[row * share : (row + 1) * share]

    def mix_step(s):
        keep(jnp.dot(branch[...], buf_b[s], preferred_element_type=jnp.float32), s)
        pl.when(s > 0)(lambda: terms_copy(0, s - 1).start())

    loop("mix", parts, mix_step)
    drain([0, 1], begins["recur"] + 1)
    terms_copy(0, parts - 1).start()
    ahead_of(begins["terms"])
    for s in range(parts):
        terms_copy(0, s).wait_recv()

    def norm_rows(i, phase, residual, gain_ref):
        here = pl.ds(pl.multiple_of(i * rows, rows), rows)

        def total(s):
            value = terms[tp, s, here, :].astype(jnp.float32) + came[phase, s, here, :].astype(jnp.float32)
            return value if phase == 0 else value + jnp.where(outer, came[0, s, here, :].astype(jnp.float32), 0.0)

        value = jnp.concatenate([total(s) for s in range(parts)], axis=1)
        return layer_norm(residual_scale * residual.astype(jnp.float32) + value, gain_ref[...]).astype(jnp.bfloat16)

    def own_rows(i):
        return pl.ds(pl.multiple_of(own_row + i * rows, rows), rows)

    def norm_copy(i):
        return pltpu.make_async_remote_copy(
            src_ref=normed.at[own_rows(i), :],
            dst_ref=normed.at[own_rows(i), :],
            send_sem=norm_send.at[i],
            recv_sem=norm_recv.at[i],
            device_id=across,
            device_id_type=MESH,
        )

    def far_copy(half, i):
        here = pl.ds(pl.multiple_of(half * share + i * rows, rows), rows)
        return pltpu.make_async_remote_copy(
            src_ref=normed.at[here, :],
            dst_ref=tok.at[here, :],
            send_sem=far_send.at[half, i],
            recv_sem=far_recv.at[half, i],
            device_id=targets[LINE],
            device_id_type=MESH,
        )

    def pass_on(i):
        norm_copy(i).start()
        pl.when(outer)(lambda: far_copy(tp, i).start())

    def first_norm(i):
        normed[own_rows(i), :] = norm_rows(i, 0, tok[own_rows(i), :], first_gain_ref)
        pl.when(jnp.logical_and(outer, i == 1))(lambda: pl.semaphore_wait(free_sem, 1))
        pl.when(i > 0)(lambda: pass_on(i - 1))

    loop("norm", row_tiles, first_norm)
    drain([2], begins["terms"])
    for s in range(parts):
        terms_copy(0, s).wait_send()

    @pl.when(middle)
    def _():
        pl.semaphore_signal(free_sem, inc=1, device_id=targets[LINE], device_id_type=MESH)

    pass_on(row_tiles - 1)
    for i in range(row_tiles):
        ahead_of(begins["rows"] + i)
        norm_copy(i).wait_recv()
        pl.when(outer)(lambda i=i: far_copy(1 - tp, i).start())

    def units_at(left, buf, j):
        cols = pl.ds(pl.multiple_of(j * tile, tile), tile)
        gate = jnp.dot(left[...], buf[0, :, cols], preferred_element_type=jnp.float32)
        upward = jnp.dot(left[...], buf[1, :, cols], preferred_element_type=jnp.float32)
        return (gate * sigmoid(gate) * upward).astype(jnp.bfloat16)

    def in_middle(body):
        def asked(i):
            pl.when(middle)(lambda: body(i))

        return asked

    def first_step(j):
        @pl.when(j == 0)
        def _():
            for half in range(2):
                for i in range(row_tiles):
                    far_copy(half, i).wait_recv()

        to = pl.ds(pl.multiple_of(j * tile, tile), tile)
        hidden[:, to] = units_at(normed, buf_e, j)
        branch[:, to] = units_at(tok, buf_e, j)

    def far_step(s):
        left = branch[:, :first_units]
        keep(jnp.dot(left, buf_f[s], preferred_element_type=jnp.float32), s)
        pl.when(s > 0)(lambda: terms_copy(2, s - 1).start())

    def back_copy(s):
        return pltpu.make_async_remote_copy(
            src_ref=came.at[0, s],
            dst_ref=came.at[0, s],
            send_sem=back_send.at[s],
            recv_sem=back_recv.at[s],
            device_id=targets[LINE],
            device_id_type=MESH,
        )

    def back_step(s):
        terms_copy(2, s).wait_recv()
        came[0, s] = (terms[tp, s].astype(jnp.float32) + came[0, s].astype(jnp.float32)).astype(jnp.bfloat16)
        pl.when(s > 0)(lambda: back_copy(s - 1).start())

    loop("first", first_tiles, in_middle(first_step))
    loop("far", parts, in_middle(far_step))
    def hidden_step(j):
        to = pl.ds(pl.multiple_of(first_units + j * tile, tile), tile)
        hidden[:, to] = units_at(normed, buf_c, j)
        pl.when(jnp.logical_and(middle, j == 0))(lambda: terms_copy(2, parts - 1).start())

    loop("hidden", other_tiles, hidden_step)
    loop("back", parts, in_middle(back_step))

    @pl.when(middle)
    def _():
        for s in range(parts):
            terms_copy(2, s).wait_send()
        back_copy(parts - 1).start()

    order = [spots[side][k] for k, side in turn_of]

    def pick(j):
        at = order[0]
        for turn in range(1, parts):
            at = jnp.where(j == turn, order[turn], at)
        return at

    def down_step(j):
        at = pick(j)
        product = lambda: jnp.dot(hidden[:, first_units:], buf_d[at], preferred_element_type=jnp.float32)
        more = lambda: jnp.dot(hidden[:, :first_units], buf_f[at], preferred_element_type=jnp.float32)
        pl.when(outer)(lambda: keep(product(), at))
        pl.when(middle)(lambda: keep(product() + more(), at))
        pl.when(j > 0)(lambda: terms_copy(1, pick(j - 1)).start())

    loop("down", parts, down_step)
    drain(range(5), len(steps))
    terms_copy(1, order[-1]).start()
    drain(range(INPUTS), len(steps))
    for i in range(row_tiles):
        norm_copy(i).wait_send()

    @pl.when(outer)
    def _():
        for half in range(2):
            for i in range(row_tiles):
                far_copy(half, i).wait_send()
        for s in range(parts):
            back_copy(s).wait_recv()

    @pl.when(middle)
    def _():
        for s in range(parts):
            back_copy(s).wait_send()

    for s in order:
        terms_copy(1, s).wait_recv()

    def second_norm(i, _):
        here = pl.ds(pl.multiple_of(i * rows, rows), rows)
        out_ref[here, :] = norm_rows(i, 1, normed[own_rows(i), :], second_gain_ref)

    lax.fori_loop(0, row_tiles, second_norm, None)
    for s in range(parts):
        terms_copy(1, s).wait_send()


def whole_layer(
    tokens,
    recurrence_branch_weight,
    gate_branch_weight,
    convolution_kernel,
    recurrence_gate_blockwise,
    input_gate_blockwise,
    channel_decay_param,
    token_decay_shift,
    recurrence_output_weight,
    first_norm_gain,
    feedforward_gate_weight,
    feedforward_up_weight,
    feedforward_down_weight,
    second_norm_gain,
):
    length, model = tokens.shape
    parts = lax.axis_size("fs")
    share = length // lax.axis_size("tp")
    depth, channels = recurrence_branch_weight.shape
    units = feedforward_gate_weight.shape[1]
    first_units = units * 2 // 5 // 256 * 256
    columns = recurrence_output_weight.shape[1]
    hbm = pl.BlockSpec(memory_space=pl.ANY)
    vmem = pl.BlockSpec(memory_space=pltpu.VMEM)
    half = jnp.bfloat16
    packs = len(PACKS)
    row_tiles = share // min(64, share)
    return pl.pallas_call(
        layer_kernel,
        in_specs=[hbm, hbm, hbm, vmem, hbm, hbm, vmem, hbm, hbm, vmem, hbm, hbm, hbm, vmem],
        out_specs=vmem,
        out_shape=jax.ShapeDtypeStruct((share, model), half),
        scratch_shapes=[
            pltpu.VMEM((A_PARTS, 2, depth * parts, channels // A_PARTS), half),
            pltpu.VMEM((parts, channels, columns), half),
            pltpu.VMEM((2, depth * parts, first_units), half),
            pltpu.VMEM((parts, first_units, columns), half),
            pltpu.VMEM((2, depth * parts, units - first_units), half),
            pltpu.VMEM((parts, units - first_units, columns), half),
            pltpu.VMEM((length, model), half),
            pltpu.VMEM(recurrence_gate_blockwise.shape, half),
            pltpu.VMEM(input_gate_blockwise.shape, half),
            pltpu.VMEM((length, channels), jnp.float32),
            pltpu.VMEM((length, channels), half),
            pltpu.VMEM((2, parts, share, columns), half),
            pltpu.VMEM((2, parts, share, columns), half),
            pltpu.VMEM((length, model), half),
            pltpu.VMEM((length, units), half),
            pltpu.SemaphoreType.DMA((15,)),
            pltpu.SemaphoreType.DMA((packs, parts, 4)),
            pltpu.SemaphoreType.DMA((packs, 2, parts)),
            pltpu.SemaphoreType.DMA((3, parts)),
            pltpu.SemaphoreType.DMA((3, parts)),
            pltpu.SemaphoreType.DMA((row_tiles,)),
            pltpu.SemaphoreType.DMA((row_tiles,)),
            pltpu.SemaphoreType.DMA((2, row_tiles)),
            pltpu.SemaphoreType.DMA((2, row_tiles)),
            pltpu.SemaphoreType.DMA((parts,)),
            pltpu.SemaphoreType.DMA((parts,)),
            pltpu.SemaphoreType.REGULAR,
        ],
        cost_estimate=pl.CostEstimate(
            flops=2 * length * model * (2 * channels + 2 * units) + 2 * length * model * (channels + units),
            bytes_accessed=2 * model * (3 * channels + 3 * units),
            transcendentals=0,
        ),
        compiler_params=pltpu.CompilerParams(
            vmem_limit_bytes=LAYER_VMEM_BYTES, collective_id=0, has_side_effects=True
        ),
    )(
        tokens,
        recurrence_branch_weight,
        gate_branch_weight,
        convolution_kernel,
        recurrence_gate_blockwise,
        input_gate_blockwise,
        channel_decay_param[None, :],
        token_decay_shift,
        recurrence_output_weight,
        first_norm_gain[None, :],
        feedforward_gate_weight,
        feedforward_up_weight,
        feedforward_down_weight,
        second_norm_gain[None, :],
    )


def recurrence_kernel(count, meta, x_ref, taps_ref, rate_ref, inlet_ref, plus_ref, shift_ref, *refs):
    mine, other, out_ref = refs[:count], refs[count : 2 * count], refs[-1]
    first = split_product(meta, x_ref, mine)
    second = split_product(meta, x_ref, other)
    out_ref[...] = recur_core(
        first, second, taps_ref[...], rate_ref[0], inlet_ref[0], plus_ref[...], shift_ref[...]
    )


def recurrence(tokens, mine, other, meta, taps, rate_blocks, inlet_blocks, plus, shift):
    length, width = tokens.shape
    block = rate_blocks.shape[1]
    blocks = rate_blocks.shape[0]
    parts = [pl.BlockSpec((p.shape[0], block), lambda i: (0, i)) for p in [*mine, *other]]
    column = lambda rows: pl.BlockSpec((rows, block), lambda i: (0, i))
    square = pl.BlockSpec((1, block, block), lambda i: (i, 0, 0))
    return pl.pallas_call(
        functools.partial(recurrence_kernel, len(mine)),
        grid=(blocks,),
        in_specs=[
            pl.BlockSpec(memory_space=pltpu.SMEM),
            pl.BlockSpec((length, width), lambda i: (0, 0)),
            column(taps.shape[0]),
            square,
            square,
            column(1),
            column(length),
            *parts,
        ],
        out_specs=column(length),
        out_shape=jax.ShapeDtypeStruct((length, block * blocks), jnp.bfloat16),
        cost_estimate=pl.CostEstimate(
            flops=4 * length * width * block * blocks,
            bytes_accessed=4 * width * block * blocks + 8 * length * block * blocks,
            transcendentals=0,
        ),
        compiler_params=pltpu.CompilerParams(vmem_limit_bytes=VMEM_BYTES),
    )(meta, tokens, taps, rate_blocks, inlet_blocks, plus, shift, *mine, *other)


def hidden_kernel(count, meta, x_ref, *refs):
    mine, other, out_ref = refs[:count], refs[count : 2 * count], refs[-1]
    first = split_product(meta, x_ref, mine)
    second = split_product(meta, x_ref, other)
    swapped = meta[0] == 1
    gate = jnp.where(swapped, second, first)
    upward = jnp.where(swapped, first, second)
    out_ref[...] = (gate * sigmoid(gate) * upward).astype(jnp.bfloat16)


def hidden_units(normed, mine, other, meta):
    length, width = normed.shape
    units = mine[0].shape[1]
    tile = next(t for t in (512, 640, 256, 128, units) if units % t == 0)
    return pl.pallas_call(
        functools.partial(hidden_kernel, len(mine)),
        grid=(units // tile,),
        in_specs=[
            pl.BlockSpec(memory_space=pltpu.SMEM),
            pl.BlockSpec((length, width), lambda i: (0, 0)),
            *[pl.BlockSpec((p.shape[0], tile), lambda i: (0, i)) for p in [*mine, *other]],
        ],
        out_specs=pl.BlockSpec((length, tile), lambda i: (0, i)),
        out_shape=jax.ShapeDtypeStruct((length, units), jnp.bfloat16),
        cost_estimate=pl.CostEstimate(
            flops=4 * length * width * units, bytes_accessed=4 * width * units, transcendentals=0
        ),
        compiler_params=pltpu.CompilerParams(vmem_limit_bytes=VMEM_BYTES),
    )(meta, normed, *mine, *other)


def outward_kernel(count, meta, left_ref, *refs):
    mine, other, out_ref = refs[:count], refs[count : 2 * count], refs[-1]
    half = mine[0].shape[0]
    near = pl.ds(pl.multiple_of(meta[0] * half, 128), half)
    far = pl.ds(pl.multiple_of((1 - meta[0]) * half, 128), half)
    start = 0
    for at in range(count):
        total = jnp.dot(left_ref[:, near], mine[at][...], preferred_element_type=jnp.float32)
        total += jnp.dot(left_ref[:, far], other[at][...], preferred_element_type=jnp.float32)
        columns = mine[at].shape[1]
        out_ref[:, start : start + columns] = total.astype(jnp.bfloat16)
        start += columns


def outward(left, mine, other, meta):
    length, depth = left.shape
    width = sum(p.shape[1] for p in mine)
    rows = min(length, 256)
    whole = [pl.BlockSpec(p.shape, lambda i: (0, 0)) for p in [*mine, *other]]
    return pl.pallas_call(
        functools.partial(outward_kernel, len(mine)),
        grid=(length // rows,),
        in_specs=[
            pl.BlockSpec(memory_space=pltpu.SMEM),
            pl.BlockSpec((rows, depth), lambda i: (i, 0)),
            *whole,
        ],
        out_specs=pl.BlockSpec((rows, width), lambda i: (i, 0)),
        out_shape=jax.ShapeDtypeStruct((length, width), jnp.bfloat16),
        cost_estimate=pl.CostEstimate(
            flops=2 * length * width * depth, bytes_accessed=2 * width * depth, transcendentals=0
        ),
        compiler_params=pltpu.CompilerParams(vmem_limit_bytes=VMEM_BYTES),
    )(meta, left, *mine, *other)


def gathered_layer(
    tokens,
    recurrence_branch_weight,
    gate_branch_weight,
    convolution_kernel,
    recurrence_gate_blockwise,
    input_gate_blockwise,
    channel_decay_param,
    token_decay_shift,
    recurrence_output_weight,
    first_norm_gain,
    feedforward_gate_weight,
    feedforward_up_weight,
    feedforward_down_weight,
    second_norm_gain,
):
    share = tokens.shape[0] // lax.axis_size("tp")
    offset = lax.axis_index("tp") * share
    rows_of = lambda weight: [lax.all_gather(weight, "fs", axis=0, tiled=True)]

    def halves_of(weight):
        half = weight.shape[0] // 2
        return [[lax.all_gather(part, "fs", axis=1, tiled=True)] for part in (weight[:half], weight[half:])]

    meta = scalars([jnp.int32(0)], jnp.int32(0))
    branch = recurrence(
        tokens,
        rows_of(recurrence_branch_weight),
        rows_of(gate_branch_weight),
        meta,
        convolution_kernel,
        recurrence_gate_blockwise,
        input_gate_blockwise,
        jax.nn.softplus(-channel_decay_param)[None, :],
        token_decay_shift,
    )

    def grouped(left, weight):
        terms = outward(left, *halves_of(weight), meta)
        return lax.psum_scatter(terms, "tp", scatter_dimension=0, tiled=True).astype(jnp.float32)

    mix = grouped(branch, recurrence_output_weight)
    own_tokens = lax.dynamic_slice_in_dim(tokens, offset, share, 0)
    normed = layer_norm(
        residual_scale * own_tokens.astype(jnp.float32) + mix, first_norm_gain
    ).astype(jnp.bfloat16)
    rows = lax.all_gather(normed, "tp", axis=0, tiled=True)
    hidden = hidden_units(rows, rows_of(feedforward_gate_weight), rows_of(feedforward_up_weight), meta)
    ffn = grouped(hidden, feedforward_down_weight)
    return layer_norm(residual_scale * normed.astype(jnp.float32) + ffn, second_norm_gain).astype(
        jnp.bfloat16
    )


def solution(mesh):
    sizes = mesh.shape
    one_kernel = sizes["rep"] == 2 and sizes["tp"] == 2 and sizes["fs"] == 8
    return jax.shard_map(
        whole_layer if one_kernel else gathered_layer,
        mesh=mesh,
        in_specs=(
            P(("rep", "fs"), None),
            P("fs", "tp"),
            P("fs", "tp"),
            P(None, "tp"),
            P("tp", None, None),
            P("tp", None, None),
            P("tp"),
            P(("rep", "fs"), "tp"),
            P("tp", "fs"),
            P(),
            P("fs", "tp"),
            P("fs", "tp"),
            P("tp", "fs"),
            P(),
        ),
        out_specs=P(("rep", "fs", "tp"), None),
        check_vma=False,
    )
```

```python
import functools

import jax
import jax.numpy as jnp
from jax import lax
from jax.experimental import pallas as pl
from jax.experimental.pallas import tpu as pltpu
from jax.sharding import PartitionSpec as P

residual_scale = 1.4142135623730951

VMEM_BYTES = 60 * 1024 * 1024
LAYER_VMEM_BYTES = 67043328
MESH = pl.DeviceIdType.MESH


def layer_norm(values, gain):
    center = values - jnp.mean(values, axis=-1, keepdims=True)
    variance = jnp.mean(center * center, axis=-1, keepdims=True)
    return center * lax.rsqrt(variance + 1e-05) * gain


def scalars(owners, swapped):
    return jnp.stack([jnp.asarray(v, jnp.int32) for v in [swapped, *owners]])


def split_product(meta, left_ref, part_refs):
    total = None
    for at, part in enumerate(part_refs):
        depth = part.shape[0]
        columns = pl.ds(pl.multiple_of(meta[1 + at] * depth, depth), depth)
        term = jnp.dot(left_ref[:, columns], part[...], preferred_element_type=jnp.float32)
        total = term if total is None else total + term
    return total


def shifted(values, step, fill):
    rows = lax.broadcasted_iota(jnp.int32, values.shape, 0)
    return jnp.where(rows < step, fill, pltpu.roll(values, step, 0))


def sigmoid(values):
    return 1.0 / (1.0 + jnp.exp(-values))


def recur_core(value_in, gate_in, taps, rate_block, inlet_block, plus, shift):
    value_in = value_in.astype(jnp.bfloat16).astype(jnp.float32)
    gate_in = gate_in.astype(jnp.bfloat16).astype(jnp.float32)
    taps = taps.astype(jnp.float32)
    depth = taps.shape[0]
    conv = None
    for tap in range(depth):
        lag = depth - 1 - tap
        moved = value_in if lag == 0 else shifted(value_in, lag, 0.0)
        term = moved * taps[tap : tap + 1, :]
        conv = term if conv is None else conv + term
    conv = conv.astype(jnp.bfloat16)
    rate = sigmoid(jnp.dot(conv, rate_block, preferred_element_type=jnp.float32))
    inlet = sigmoid(jnp.dot(conv, inlet_block, preferred_element_type=jnp.float32))
    log_decay = -8.0 * rate * plus + shift
    decay = jnp.exp(log_decay)
    twice = 2.0 * log_decay
    series = jnp.ones_like(twice)
    for order in range(8, 1, -1):
        series = 1.0 + twice * series * (1.0 / order)
    lost = jnp.where(twice > -0.3, -twice * series, 1.0 - jnp.exp(twice))
    state = jnp.sqrt(lost) * inlet * conv.astype(jnp.float32)
    step = 1
    while step < state.shape[0]:
        state = state + decay * shifted(state, step, 0.0)
        if 2 * step < state.shape[0]:
            decay = decay * shifted(decay, step, 1.0)
        step *= 2
    gelu = 0.5 * gate_in * (
        1.0 + jnp.tanh(0.7978845608028654 * (gate_in + 0.044715 * gate_in * gate_in * gate_in))
    )
    return (state * gelu).astype(jnp.bfloat16)


LINE, OTHER, SIDE, CORE = 0, 1, 2, 3
INPUTS = 7
OWN, OWN_SIDE, FROM_SIDE, FROM_LINE, ON_SIDE, FROM_FAR_SIDE = range(6)
A_PARTS = 1
PACKS = ((0, 0, 1), (2, 0, 1), (3, 0, 1), (4, 0, 1), (5, 0, 1), (6, 0, 2), (6, 1, 2))
ALONG = ((4, 5), (7, 7), (0, 1), (2, 3), (6, 7), (6, 3), (6, 3))
PLANS = (
    (

        (100, 0, 130, 110, 120, 301, 10, 200, 402, 433, 302, 210, 20, 30, 511, 401, 50, 403, 311, 501, 502, 503, 303, 423, 322, 40, 413),
        (513, 412, 140, 323), (312, 313, 512), (160, 240), (), (), (), (), (), (), (533, 432, 332, 441), (), (),
        (150,), (421,), (), (), (), (341, 342), (442, 541, 521), (), (351, 443, 343, 451), (532, 260), (), (),
        (352,), (250,), (), (), (), (453, 542, 361, 461), (452, 60), (220, 462), (543, 353), (331,), (561,), (),
        (531,), (333, 230), (), (), (562, 553), (), (463, 362), (), (), (431,), (552, 411, 551), (523, 363, 563), (),
        (321,), (), (422,), (), (522,),
    ),
    (
        (10, 140, 120, 110, 100, 0, 20, 433, 210, 302, 402, 200, 30, 403, 502, 40, 301, 303, 501, 413, 503),
        (240, 412, 50, 311, 423), (), (), (), (323, 401, 312, 130, 322), (512,), (), (511, 160, 313), (), (),
        (533, 532, 432, 260, 332, 60, 513), (), (442,), (), (), (), (), (341, 521, 351, 150, 421), (), (), (),
        (343,), (443, 543), (), (), (342,), (), (352, 441), (), (), (), (361,), (461, 542, 541, 451, 220), (462,),
        (353, 452, 531, 331), (453,), (), (561,), (), (), (230, 333, 362), (), (463,), (), (411,), (), (),
        (431, 553, 562), (552,), (), (551, 523), (), (563,), (321, 422, 363, 250, 522),
    ),
    (

        (0, 110, 301, 302, 402, 311, 462, 100, 10, 210, 502, 403, 20, 130, 303, 501, 200, 413, 442, 503, 452, 512, 421, 120, 313, 513, 422, 511, 312, 331),
        (), (), (), (), (322,), (522,), (), (140,), (), (220, 40, 321, 351, 341), (60,), (431, 432), (50, 240),
        (423,), (), (353,), (412, 433, 333, 323), (541, 342), (), (343, 523, 521, 230, 533),
        (443, 542, 401, 30, 352, 362, 332, 160, 531, 532), (543,), (461,), (361,), (), (453, 561), (150,),
        (463, 363, 551), (), (), (), (), (), (260, 441, 250), (), (), (563, 553, 552, 562, 411), (), (), (), (), (),
        (), (), (), (), (), (), (), (), (), (), (451,), (),
    ),
    (
        (10, 0, 100, 110, 462, 130, 311, 402, 302, 301, 403, 313, 303, 442, 20, 200, 502, 413, 230, 312, 60),
        (503, 513, 511, 331, 210, 40), (501, 431), (), (512, 321), (), (140,), (432, 532), (421,), (120, 342),
        (341, 531), (), (422, 541), (50, 333), (362, 323), (), (), (343,), (412, 322, 401, 352, 522, 423, 433),
        (523,), (), (361,), (160,), (443, 30, 220, 521), (351, 533, 240), (), (), (461,), (), (332,), (),
        (260, 353, 150), (363,), (), (543,), (542,), (), (250,), (), (), (), (), (552,), (453,), (), (), (), (), (),
        (451, 562, 441, 553), (463,), (), (411,), (), (452, 563, 551, 561),
    ),
)


def layer_kernel(
    tok_hbm,
    in_hbm,
    gate_hbm,
    taps_ref,
    rate_hbm,
    inlet_hbm,
    param_ref,
    shift_hbm,
    out_hbm,
    first_gain_ref,
    ffgate_hbm,
    ffup_hbm,
    down_hbm,
    second_gain_ref,
    out_ref,
    buf_a,
    buf_b,
    buf_e,
    buf_f,
    buf_c,
    buf_d,
    tok,
    rate_blocks,
    inlet_blocks,
    shift,
    branch,
    terms,
    came,
    normed,
    hidden,
    load_sem,
    send_sem,
    recv_sem,
    terms_send,
    terms_recv,
    norm_send,
    norm_recv,
    far_send,
    far_recv,
    back_send,
    back_recv,
    free_sem,
):
    core, fs, tp = lax.axis_index("rep"), lax.axis_index("fs"), lax.axis_index("tp")
    z, y = fs // 2, fs % 2
    zs = [z, z + 1 - 2 * (z % 2), 2 - z // 2, 3 - 3 * (z // 2)]
    middle = z * (3 - z) == 2
    role = core + z * (3 - z)
    roles = [role == at for at in range(4)]
    outer = jnp.logical_not(middle)
    spots = [[k * 2 + y for k in zs], [k * 2 + 1 - y for k in zs]]
    me = spots[0][0]
    targets = {
        LINE: (core, spots[0][1], tp),
        OTHER: (core, (3 - z) * 2 + y, tp),
        SIDE: (core, spots[1][0], tp),
        CORE: (1 - core, me, tp),
    }
    across = (core, me, 1 - tp)
    width = in_hbm.shape[0]
    parts = buf_b.shape[0]
    first_units, other_units = buf_e.shape[2], buf_c.shape[2]
    a_columns = buf_a.shape[3]
    mix_depth = buf_b.shape[1]
    share = out_ref.shape[0]
    block = rate_blocks.shape[1]
    blocks = rate_blocks.shape[0]
    tile = min(256, first_units)
    first_tiles, other_tiles = first_units // tile, other_units // tile
    rows = min(64, share)
    row_tiles = share // rows
    own_row = pl.multiple_of(tp * share, share)

    def run_of(base, part, count):
        return pl.ds(pl.multiple_of(base + part * count, count), count)

    def piece(pack, at, half):
        weight, part, count = PACKS[pack]
        by_row = run_of(at * width, part, width // count)
        by_depth = lambda depth: run_of(half * (depth // 2), part, depth // 2 // count)
        if weight < 2:
            return buf_a.at[weight, half, by_row, :]
        if weight == 2:
            return buf_b.at[at, by_depth(mix_depth), :]
        if weight == 3:
            return buf_e.at[half, by_row, :]
        if weight == 4:
            return buf_f.at[at, by_depth(first_units), :]
        if weight == 5:
            return buf_c.at[half, by_row, :]
        return buf_d.at[at, by_depth(other_units), :]

    def copy(pack, at, way, half=core):
        return pltpu.make_async_remote_copy(
            src_ref=piece(pack, at, half),
            dst_ref=piece(pack, at, half),
            send_sem=send_sem.at[pack, at, way],
            recv_sem=recv_sem.at[pack, half, at],
            device_id=targets[way],
            device_id_type=MESH,
        )

    own_rows_of = lambda ref, *at: ref.at[(*at, pl.ds(pl.multiple_of(me * width, width), width), slice(None))]
    a_part = lambda part: [
        (ref.at[:, pl.ds(part * a_columns, a_columns)], own_rows_of(buf_a, part, half))
        for half, ref in enumerate((in_hbm, gate_hbm))
    ]
    units_of = lambda start, count, buf: [
        (ref.at[:, pl.ds(start, count)], own_rows_of(buf, half)) for half, ref in enumerate((ffgate_hbm, ffup_hbm))
    ]
    loads = [
        a_part(0),
        a_part(1) if A_PARTS == 2 else [],
        [(out_hbm, buf_b.at[me])],
        units_of(0, first_units, buf_e),
        [(down_hbm.at[pl.ds(0, first_units), :], buf_f.at[me])],
        units_of(first_units, other_units, buf_c),
        [(down_hbm.at[pl.ds(first_units, other_units), :], buf_d.at[me])],
        [(tok_hbm, tok), (shift_hbm, shift), (rate_hbm, rate_blocks), (inlet_hbm, inlet_blocks)],
    ]
    count = 0
    for group in loads:
        for at, (source, target) in enumerate(group):
            group[at] = pltpu.make_async_copy(source, target, load_sem.at[count])
            count += 1

    steps = ["recur"] * blocks + ["mix"] * parts + ["terms"] + ["norm"] * row_tiles + ["rows"] * row_tiles
    steps += ["first"] * first_tiles + ["far"] * parts + ["hidden"] * other_tiles
    steps += ["back"] * parts + ["down"] * parts
    begins = {name: steps.index(name) for name in dict.fromkeys(steps)}
    turn_of = [(0, 0), (0, 1), (1, 0), (2, 0), (1, 1), (3, 0), (2, 1), (3, 1)]
    needs = {begins["recur"]: 0, begins["mix"]: 2, begins["first"]: 3, begins["far"]: 4, begins["hidden"]: 5}
    if A_PARTS == 2:
        needs[begins["recur"] + blocks // 2] = 1
    packs_of = [[p for p, (w, _, _) in enumerate(PACKS) if w == weight] for weight in range(INPUTS)]

    def actions(plan, in_middle, second):
        loaded, waited, sends, gaps = set(), set(), [], []

        def load(weight, out):
            if weight not in loaded:
                loaded.add(weight)
                out.append(("load", weight))

        def arrive(pack, k, side, out):
            if (k, side) == (0, 0):
                load(PACKS[pack][0], out)
            elif (pack, k, side) not in waited:
                waited.add((pack, k, side))
                out.append(("arrive", pack, k, side))

        def send(pack, k, side, way, out):
            arrive(pack, k, side, out)
            out.append(("send", pack, k, side, way))
            sends.append((pack, k, side, way, len(gaps)))

        for step, codes in enumerate(plan):
            out = []
            for code in codes:
                kind, pack, k = code // 100, code // 10 % 10, code % 10
                first = PACKS[pack][0] in (3, 4)
                to_end, to_middle, from_end = (ALONG[pack][second] & bit for bit in (1, 2, 4))
                if kind == OWN:
                    if not (first and in_middle):
                        send(pack, 0, 0, LINE, out)
                    if in_middle:
                        send(pack, 0, 0, OTHER, out)
                elif kind == OWN_SIDE:
                    if not first or in_middle or from_end:
                        send(pack, 0, 0, SIDE, out)
                elif kind == FROM_SIDE:
                    if in_middle and to_end and not first:
                        send(pack, 0, 1, LINE, out)
                    if in_middle and to_middle:
                        send(pack, 0, 1, OTHER, out)
                    if not in_middle and from_end:
                        send(pack, 0, 1, LINE, out)
                    if not first or in_middle:
                        send(pack, 0, 1, CORE, out)
                elif first and not in_middle:
                    pass
                elif kind == FROM_LINE:
                    if in_middle and (k == 1 or not first):
                        send(pack, k, 0, OTHER if k == 1 else LINE, out)
                    send(pack, k, 0, CORE, out)
                elif kind == ON_SIDE:
                    comes_along = {1: from_end if in_middle else to_end, 2: in_middle and to_middle, 3: False}
                    if not comes_along[k]:
                        send(pack, k, 0, SIDE, out)
                else:
                    send(pack, k, 1, CORE, out)
            if step in needs:
                weight = needs[step]
                load(weight, out)
                if step == 0:
                    load(INPUTS, out)
                for pack in packs_of[weight] if in_middle or weight not in (3, 4) else []:
                    for turn in turn_of[1:]:
                        arrive(pack, *turn, out)
                        out.append(("handed", pack, *turn))
            if begins["down"] <= step:
                turn = turn_of[step - begins["down"]]
                for pack in packs_of[6]:
                    arrive(pack, *turn, out)
                    if turn != (0, 0):
                        out.append(("handed", pack, *turn))
            gaps.append(out)
        return gaps, sends

    programs = [actions(plan, at >= 2, at % 2) for at, plan in enumerate(PLANS)]

    def act(todo):
        for kind, *rest in todo:
            if kind == "load":
                for one in loads[rest[0]]:
                    one.wait()
                continue
            at = spots[rest[2]][rest[1]]
            if kind == "arrive":
                copy(rest[0], at, CORE).wait_recv()
            elif kind == "handed":
                copy(rest[0], at, CORE, 1 - core).wait_recv()
            elif kind == "send":
                copy(rest[0], at, rest[3]).start()
            else:
                copy(rest[0], at, rest[3]).wait_send()

    def ahead_of(step, index=None):
        for mine, (gaps, _) in zip(roles, programs):
            if gaps[step]:
                asked = mine if index is None else jnp.logical_and(mine, index == step - begins[steps[step]])
                pl.when(asked)(functools.partial(act, gaps[step]))

    def loop(name, length, body):
        def whole(index, _):
            for step in range(begins[name], begins[name] + length):
                ahead_of(step, index)
            body(index)

        lax.fori_loop(0, length, whole, None)

    drained = [set() for _ in programs]

    def drain(weights, before):
        for mine, (_, sends), gone in zip(roles, programs, drained):
            now = [one for one in sends if PACKS[one[0]][0] in weights and one[-1] < before and one not in gone]
            gone.update(now)
            pl.when(mine)(functools.partial(act, [("sent", *one) for one in now]))

    def begin(groups):
        for group in groups:
            for one in group:
                one.start()

    begin(loads[:A_PARTS])
    barrier = pltpu.get_barrier_semaphore()
    for target in [targets[LINE], targets[SIDE], targets[CORE], across]:
        pl.semaphore_signal(barrier, inc=1, device_id=target, device_id_type=MESH)

    @pl.when(middle)
    def _():
        pl.semaphore_signal(barrier, inc=1, device_id=targets[OTHER], device_id_type=MESH)

    pl.semaphore_wait(barrier, 4 + z * (3 - z) // 2)
    begin(loads[A_PARTS:])

    def recur_step(i):
        cols = pl.ds(pl.multiple_of(i * block, block), block)
        part, place = (i * block) // a_columns, pl.ds(pl.multiple_of(i * block % a_columns, block), block)
        value_in = jnp.dot(tok[...], buf_a[part, 0, :, place], preferred_element_type=jnp.float32)
        gate_in = jnp.dot(tok[...], buf_a[part, 1, :, place], preferred_element_type=jnp.float32)
        param = -param_ref[:, cols]
        plus = jnp.maximum(param, 0.0) + jnp.log1p(jnp.exp(-jnp.abs(param)))
        branch[:, cols] = recur_core(
            value_in, gate_in, taps_ref[:, cols], rate_blocks[i], inlet_blocks[i], plus, shift[:, cols]
        )

    loop("recur", blocks, recur_step)

    def terms_copy(phase, at):
        return pltpu.make_async_remote_copy(
            src_ref=terms.at[1 - tp, at],
            dst_ref=came.at[phase % 2, at],
            send_sem=terms_send.at[phase, at],
            recv_sem=terms_recv.at[phase, at],
            device_id=across,
            device_id_type=MESH,
        )

    def keep(product, at):
        product = product.astype(jnp.bfloat16)
        for row in range(2):
            terms[row, at] = product[row * share : (row + 1) * share]

    def mix_step(s):
        keep(jnp.dot(branch[...], buf_b[s], preferred_element_type=jnp.float32), s)
        pl.when(s > 0)(lambda: terms_copy(0, s - 1).start())

    loop("mix", parts, mix_step)
    drain([0, 1], begins["recur"] + 1)
    terms_copy(0, parts - 1).start()
    ahead_of(begins["terms"])
    for s in range(parts):
        terms_copy(0, s).wait_recv()

    def norm_rows(i, phase, residual, gain_ref):
        here = pl.ds(pl.multiple_of(i * rows, rows), rows)

        def total(s):
            value = terms[tp, s, here, :].astype(jnp.float32) + came[phase, s, here, :].astype(jnp.float32)
            return value if phase == 0 else value + jnp.where(outer, came[0, s, here, :].astype(jnp.float32), 0.0)

        value = jnp.concatenate([total(s) for s in range(parts)], axis=1)
        return layer_norm(residual_scale * residual.astype(jnp.float32) + value, gain_ref[...]).astype(jnp.bfloat16)

    def own_rows(i):
        return pl.ds(pl.multiple_of(own_row + i * rows, rows), rows)

    def norm_copy(i):
        return pltpu.make_async_remote_copy(
            src_ref=normed.at[own_rows(i), :],
            dst_ref=normed.at[own_rows(i), :],
            send_sem=norm_send.at[i],
            recv_sem=norm_recv.at[i],
            device_id=across,
            device_id_type=MESH,
        )

    def far_copy(half, i):
        here = pl.ds(pl.multiple_of(half * share + i * rows, rows), rows)
        return pltpu.make_async_remote_copy(
            src_ref=normed.at[here, :],
            dst_ref=tok.at[here, :],
            send_sem=far_send.at[half, i],
            recv_sem=far_recv.at[half, i],
            device_id=targets[LINE],
            device_id_type=MESH,
        )

    def pass_on(i):
        norm_copy(i).start()
        pl.when(outer)(lambda: far_copy(tp, i).start())

    def first_norm(i):
        normed[own_rows(i), :] = norm_rows(i, 0, tok[own_rows(i), :], first_gain_ref)
        pl.when(jnp.logical_and(outer, i == 1))(lambda: pl.semaphore_wait(free_sem, 1))
        pl.when(i > 0)(lambda: pass_on(i - 1))

    loop("norm", row_tiles, first_norm)
    drain([2], begins["terms"])
    for s in range(parts):
        terms_copy(0, s).wait_send()

    @pl.when(middle)
    def _():
        pl.semaphore_signal(free_sem, inc=1, device_id=targets[LINE], device_id_type=MESH)

    pass_on(row_tiles - 1)
    for i in range(row_tiles):
        ahead_of(begins["rows"] + i)
        norm_copy(i).wait_recv()
        pl.when(outer)(lambda i=i: far_copy(1 - tp, i).start())

    def units_at(left, buf, j):
        cols = pl.ds(pl.multiple_of(j * tile, tile), tile)
        gate = jnp.dot(left[...], buf[0, :, cols], preferred_element_type=jnp.float32)
        upward = jnp.dot(left[...], buf[1, :, cols], preferred_element_type=jnp.float32)
        return (gate * sigmoid(gate) * upward).astype(jnp.bfloat16)

    def in_middle(body):
        def asked(i):
            pl.when(middle)(lambda: body(i))

        return asked

    def first_step(j):
        @pl.when(j == 0)
        def _():
            for half in range(2):
                for i in range(row_tiles):
                    far_copy(half, i).wait_recv()

        to = pl.ds(pl.multiple_of(j * tile, tile), tile)
        hidden[:, to] = units_at(normed, buf_e, j)
        branch[:, to] = units_at(tok, buf_e, j)

    def far_step(s):
        left = branch[:, :first_units]
        keep(jnp.dot(left, buf_f[s], preferred_element_type=jnp.float32), s)
        pl.when(s > 0)(lambda: terms_copy(2, s - 1).start())

    def back_copy(s):
        return pltpu.make_async_remote_copy(
            src_ref=came.at[0, s],
            dst_ref=came.at[0, s],
            send_sem=back_send.at[s],
            recv_sem=back_recv.at[s],
            device_id=targets[LINE],
            device_id_type=MESH,
        )

    def back_step(s):
        terms_copy(2, s).wait_recv()
        came[0, s] = (terms[tp, s].astype(jnp.float32) + came[0, s].astype(jnp.float32)).astype(jnp.bfloat16)
        pl.when(s > 0)(lambda: back_copy(s - 1).start())

    loop("first", first_tiles, in_middle(first_step))
    loop("far", parts, in_middle(far_step))
    def hidden_step(j):
        to = pl.ds(pl.multiple_of(first_units + j * tile, tile), tile)
        hidden[:, to] = units_at(normed, buf_c, j)
        pl.when(jnp.logical_and(middle, j == 0))(lambda: terms_copy(2, parts - 1).start())

    loop("hidden", other_tiles, hidden_step)
    loop("back", parts, in_middle(back_step))

    @pl.when(middle)
    def _():
        for s in range(parts):
            terms_copy(2, s).wait_send()
        back_copy(parts - 1).start()

    order = [spots[side][k] for k, side in turn_of]

    def pick(j):
        at = order[0]
        for turn in range(1, parts):
            at = jnp.where(j == turn, order[turn], at)
        return at

    def down_step(j):
        at = pick(j)
        product = lambda: jnp.dot(hidden[:, first_units:], buf_d[at], preferred_element_type=jnp.float32)
        more = lambda: jnp.dot(hidden[:, :first_units], buf_f[at], preferred_element_type=jnp.float32)
        pl.when(outer)(lambda: keep(product(), at))
        pl.when(middle)(lambda: keep(product() + more(), at))
        pl.when(j > 0)(lambda: terms_copy(1, pick(j - 1)).start())

    loop("down", parts, down_step)
    drain(range(3), len(steps))
    terms_copy(1, order[-1]).start()
    drain(range(INPUTS), len(steps))
    for i in range(row_tiles):
        norm_copy(i).wait_send()

    @pl.when(outer)
    def _():
        for half in range(2):
            for i in range(row_tiles):
                far_copy(half, i).wait_send()
        for s in range(parts):
            back_copy(s).wait_recv()

    @pl.when(middle)
    def _():
        for s in range(parts):
            back_copy(s).wait_send()

    for s in order:
        terms_copy(1, s).wait_recv()

    def second_norm(i, _):
        here = pl.ds(pl.multiple_of(i * rows, rows), rows)
        out_ref[here, :] = norm_rows(i, 1, normed[own_rows(i), :], second_gain_ref)

    lax.fori_loop(0, row_tiles, second_norm, None)
    for s in range(parts):
        terms_copy(1, s).wait_send()


def whole_layer(
    tokens,
    recurrence_branch_weight,
    gate_branch_weight,
    convolution_kernel,
    recurrence_gate_blockwise,
    input_gate_blockwise,
    channel_decay_param,
    token_decay_shift,
    recurrence_output_weight,
    first_norm_gain,
    feedforward_gate_weight,
    feedforward_up_weight,
    feedforward_down_weight,
    second_norm_gain,
):
    length, model = tokens.shape
    parts = lax.axis_size("fs")
    share = length // lax.axis_size("tp")
    depth, channels = recurrence_branch_weight.shape
    units = feedforward_gate_weight.shape[1]
    first_units = units * 2 // 5 // 256 * 256
    columns = recurrence_output_weight.shape[1]
    hbm = pl.BlockSpec(memory_space=pl.ANY)
    vmem = pl.BlockSpec(memory_space=pltpu.VMEM)
    half = jnp.bfloat16
    packs = len(PACKS)
    row_tiles = share // min(64, share)
    return pl.pallas_call(
        layer_kernel,
        in_specs=[hbm, hbm, hbm, vmem, hbm, hbm, vmem, hbm, hbm, vmem, hbm, hbm, hbm, vmem],
        out_specs=vmem,
        out_shape=jax.ShapeDtypeStruct((share, model), half),
        scratch_shapes=[
            pltpu.VMEM((A_PARTS, 2, depth * parts, channels // A_PARTS), half),
            pltpu.VMEM((parts, channels, columns), half),
            pltpu.VMEM((2, depth * parts, first_units), half),
            pltpu.VMEM((parts, first_units, columns), half),
            pltpu.VMEM((2, depth * parts, units - first_units), half),
            pltpu.VMEM((parts, units - first_units, columns), half),
            pltpu.VMEM((length, model), half),
            pltpu.VMEM(recurrence_gate_blockwise.shape, half),
            pltpu.VMEM(input_gate_blockwise.shape, half),
            pltpu.VMEM((length, channels), jnp.float32),
            pltpu.VMEM((length, channels), half),
            pltpu.VMEM((2, parts, share, columns), half),
            pltpu.VMEM((2, parts, share, columns), half),
            pltpu.VMEM((length, model), half),
            pltpu.VMEM((length, units), half),
            pltpu.SemaphoreType.DMA((15,)),
            pltpu.SemaphoreType.DMA((packs, parts, 4)),
            pltpu.SemaphoreType.DMA((packs, 2, parts)),
            pltpu.SemaphoreType.DMA((3, parts)),
            pltpu.SemaphoreType.DMA((3, parts)),
            pltpu.SemaphoreType.DMA((row_tiles,)),
            pltpu.SemaphoreType.DMA((row_tiles,)),
            pltpu.SemaphoreType.DMA((2, row_tiles)),
            pltpu.SemaphoreType.DMA((2, row_tiles)),
            pltpu.SemaphoreType.DMA((parts,)),
            pltpu.SemaphoreType.DMA((parts,)),
            pltpu.SemaphoreType.REGULAR,
        ],
        cost_estimate=pl.CostEstimate(
            flops=2 * length * model * (2 * channels + 2 * units) + 2 * length * model * (channels + units),
            bytes_accessed=2 * model * (3 * channels + 3 * units),
            transcendentals=0,
        ),
        compiler_params=pltpu.CompilerParams(
            vmem_limit_bytes=LAYER_VMEM_BYTES, collective_id=0, has_side_effects=True
        ),
    )(
        tokens,
        recurrence_branch_weight,
        gate_branch_weight,
        convolution_kernel,
        recurrence_gate_blockwise,
        input_gate_blockwise,
        channel_decay_param[None, :],
        token_decay_shift,
        recurrence_output_weight,
        first_norm_gain[None, :],
        feedforward_gate_weight,
        feedforward_up_weight,
        feedforward_down_weight,
        second_norm_gain[None, :],
    )


def recurrence_kernel(count, meta, x_ref, taps_ref, rate_ref, inlet_ref, plus_ref, shift_ref, *refs):
    mine, other, out_ref = refs[:count], refs[count : 2 * count], refs[-1]
    first = split_product(meta, x_ref, mine)
    second = split_product(meta, x_ref, other)
    out_ref[...] = recur_core(
        first, second, taps_ref[...], rate_ref[0], inlet_ref[0], plus_ref[...], shift_ref[...]
    )


def recurrence(tokens, mine, other, meta, taps, rate_blocks, inlet_blocks, plus, shift):
    length, width = tokens.shape
    block = rate_blocks.shape[1]
    blocks = rate_blocks.shape[0]
    parts = [pl.BlockSpec((p.shape[0], block), lambda i: (0, i)) for p in [*mine, *other]]
    column = lambda rows: pl.BlockSpec((rows, block), lambda i: (0, i))
    square = pl.BlockSpec((1, block, block), lambda i: (i, 0, 0))
    return pl.pallas_call(
        functools.partial(recurrence_kernel, len(mine)),
        grid=(blocks,),
        in_specs=[
            pl.BlockSpec(memory_space=pltpu.SMEM),
            pl.BlockSpec((length, width), lambda i: (0, 0)),
            column(taps.shape[0]),
            square,
            square,
            column(1),
            column(length),
            *parts,
        ],
        out_specs=column(length),
        out_shape=jax.ShapeDtypeStruct((length, block * blocks), jnp.bfloat16),
        cost_estimate=pl.CostEstimate(
            flops=4 * length * width * block * blocks,
            bytes_accessed=4 * width * block * blocks + 8 * length * block * blocks,
            transcendentals=0,
        ),
        compiler_params=pltpu.CompilerParams(vmem_limit_bytes=VMEM_BYTES),
    )(meta, tokens, taps, rate_blocks, inlet_blocks, plus, shift, *mine, *other)


def hidden_kernel(count, meta, x_ref, *refs):
    mine, other, out_ref = refs[:count], refs[count : 2 * count], refs[-1]
    first = split_product(meta, x_ref, mine)
    second = split_product(meta, x_ref, other)
    swapped = meta[0] == 1
    gate = jnp.where(swapped, second, first)
    upward = jnp.where(swapped, first, second)
    out_ref[...] = (gate * sigmoid(gate) * upward).astype(jnp.bfloat16)


def hidden_units(normed, mine, other, meta):
    length, width = normed.shape
    units = mine[0].shape[1]
    tile = next(t for t in (512, 640, 256, 128, units) if units % t == 0)
    return pl.pallas_call(
        functools.partial(hidden_kernel, len(mine)),
        grid=(units // tile,),
        in_specs=[
            pl.BlockSpec(memory_space=pltpu.SMEM),
            pl.BlockSpec((length, width), lambda i: (0, 0)),
            *[pl.BlockSpec((p.shape[0], tile), lambda i: (0, i)) for p in [*mine, *other]],
        ],
        out_specs=pl.BlockSpec((length, tile), lambda i: (0, i)),
        out_shape=jax.ShapeDtypeStruct((length, units), jnp.bfloat16),
        cost_estimate=pl.CostEstimate(
            flops=4 * length * width * units, bytes_accessed=4 * width * units, transcendentals=0
        ),
        compiler_params=pltpu.CompilerParams(vmem_limit_bytes=VMEM_BYTES),
    )(meta, normed, *mine, *other)


def outward_kernel(count, meta, left_ref, *refs):
    mine, other, out_ref = refs[:count], refs[count : 2 * count], refs[-1]
    half = mine[0].shape[0]
    near = pl.ds(pl.multiple_of(meta[0] * half, 128), half)
    far = pl.ds(pl.multiple_of((1 - meta[0]) * half, 128), half)
    start = 0
    for at in range(count):
        total = jnp.dot(left_ref[:, near], mine[at][...], preferred_element_type=jnp.float32)
        total += jnp.dot(left_ref[:, far], other[at][...], preferred_element_type=jnp.float32)
        columns = mine[at].shape[1]
        out_ref[:, start : start + columns] = total.astype(jnp.bfloat16)
        start += columns


def outward(left, mine, other, meta):
    length, depth = left.shape
    width = sum(p.shape[1] for p in mine)
    rows = min(length, 256)
    whole = [pl.BlockSpec(p.shape, lambda i: (0, 0)) for p in [*mine, *other]]
    return pl.pallas_call(
        functools.partial(outward_kernel, len(mine)),
        grid=(length // rows,),
        in_specs=[
            pl.BlockSpec(memory_space=pltpu.SMEM),
            pl.BlockSpec((rows, depth), lambda i: (i, 0)),
            *whole,
        ],
        out_specs=pl.BlockSpec((rows, width), lambda i: (i, 0)),
        out_shape=jax.ShapeDtypeStruct((length, width), jnp.bfloat16),
        cost_estimate=pl.CostEstimate(
            flops=2 * length * width * depth, bytes_accessed=2 * width * depth, transcendentals=0
        ),
        compiler_params=pltpu.CompilerParams(vmem_limit_bytes=VMEM_BYTES),
    )(meta, left, *mine, *other)


def gathered_layer(
    tokens,
    recurrence_branch_weight,
    gate_branch_weight,
    convolution_kernel,
    recurrence_gate_blockwise,
    input_gate_blockwise,
    channel_decay_param,
    token_decay_shift,
    recurrence_output_weight,
    first_norm_gain,
    feedforward_gate_weight,
    feedforward_up_weight,
    feedforward_down_weight,
    second_norm_gain,
):
    share = tokens.shape[0] // lax.axis_size("tp")
    offset = lax.axis_index("tp") * share
    rows_of = lambda weight: [lax.all_gather(weight, "fs", axis=0, tiled=True)]

    def halves_of(weight):
        half = weight.shape[0] // 2
        return [[lax.all_gather(part, "fs", axis=1, tiled=True)] for part in (weight[:half], weight[half:])]

    meta = scalars([jnp.int32(0)], jnp.int32(0))
    branch = recurrence(
        tokens,
        rows_of(recurrence_branch_weight),
        rows_of(gate_branch_weight),
        meta,
        convolution_kernel,
        recurrence_gate_blockwise,
        input_gate_blockwise,
        jax.nn.softplus(-channel_decay_param)[None, :],
        token_decay_shift,
    )

    def grouped(left, weight):
        terms = outward(left, *halves_of(weight), meta)
        return lax.psum_scatter(terms, "tp", scatter_dimension=0, tiled=True).astype(jnp.float32)

    mix = grouped(branch, recurrence_output_weight)
    own_tokens = lax.dynamic_slice_in_dim(tokens, offset, share, 0)
    normed = layer_norm(
        residual_scale * own_tokens.astype(jnp.float32) + mix, first_norm_gain
    ).astype(jnp.bfloat16)
    rows = lax.all_gather(normed, "tp", axis=0, tiled=True)
    hidden = hidden_units(rows, rows_of(feedforward_gate_weight), rows_of(feedforward_up_weight), meta)
    ffn = grouped(hidden, feedforward_down_weight)
    return layer_norm(residual_scale * normed.astype(jnp.float32) + ffn, second_norm_gain).astype(
        jnp.bfloat16
    )


def solution(mesh):
    sizes = mesh.shape
    one_kernel = sizes["rep"] == 2 and sizes["tp"] == 2 and sizes["fs"] == 8
    return jax.shard_map(
        whole_layer if one_kernel else gathered_layer,
        mesh=mesh,
        in_specs=(
            P(("rep", "fs"), None),
            P("fs", "tp"),
            P("fs", "tp"),
            P(None, "tp"),
            P("tp", None, None),
            P("tp", None, None),
            P("tp"),
            P(("rep", "fs"), "tp"),
            P("tp", "fs"),
            P(),
            P("fs", "tp"),
            P("fs", "tp"),
            P("tp", "fs"),
            P(),
        ),
        out_specs=P(("rep", "fs", "tp"), None),
        check_vma=False,
    )
```
